128 devices in a mesh: sp: 16 (over z, x), fs: 4 (over y), tp: 2 (over core).
Axes of the slice: x: 4, y: 4, z: 4, core: 2. Of those that a mesh axis runs over, the one named last changes fastest.
Arguments:
- tokens: bfloat16 [4, 4096, 2048], P('fs', 'sp', 'tp'), may hold values from -6 to 6
- norm_gain: float32 [2048], replicated, may hold values from 0.1 to 1.9
- query_weight: bfloat16 [2048, 1024], P('fs', 'tp'), may hold values from -1 to 1
- key_weight: bfloat16 [2048, 1024], P('fs', 'tp'), may hold values from -4 to 4
- value_weight: bfloat16 [2048, 1024], P('fs', 'tp'), may hold values from -0.125 to 0.125
- state_query: bfloat16 [2048, 1024], P('fs', 'tp'), may hold values from -0.125 to 0.125
- state_key: bfloat16 [2048, 1024], P('fs', 'tp'), may hold values from -0.125 to 0.125
- state_value: bfloat16 [2048, 1024], P('fs', 'tp'), may hold values from -0.125 to 0.125
- map_lambda: float32 [8], P('tp'), may hold values from 0.3 to 0.8
- diff_gain: float32 [1024], P('tp'), may hold values from 0.1 to 1.9
- decay_rate: float32 [8], P('tp'), may hold values from 0 to 0.04
- state_gain: float32 [1024], P('tp'), may hold values from 0.1 to 1.9
- out_weight: bfloat16 [2048, 2048], replicated, may hold values from -0.125 to 0.125
Outputs:
- mixed: bfloat16 [4, 4096, 2048], P('fs', ('sp', 'tp'))
The draws below stay inside these ranges and needn't reach their ends.
All inputs are finite; a program needn't handle non-finite values.
Results may differ from the reference program's by a relative error of at most 0.015.
Values may be sent and summed in bfloat16 or wider, within the bound.
A program may use at most 128 MiB of HBM per device.

```python
import math
import jax
import jax.numpy as jnp
from jax import lax

D = 2048
HD = 8
DK = 64
DV = 128
HR = 8
DR = 128
TOK_DEV = 256
LENGTH = 4096
SEQS = 4


def query_base(key):
    return jax.random.normal(jax.random.fold_in(key, 101), (D, HD * 2 * DK), jnp.float32) * (2.0 / D) ** 0.5


def draw_query_weight(key, part):
    return jnp.clip(query_base(key), -1.0, 1.0).astype(jnp.bfloat16)


def draw_key_weight(key, part):
    fresh = jax.random.normal(jax.random.fold_in(key, 202), (D, HD * 2 * DK), jnp.float32) * (2.0 / D) ** 0.5
    result = fresh
    return jnp.clip(result, -4.0, 4.0).astype(jnp.bfloat16)


def draw_decay_rate(key, part):
    pick = jax.random.uniform(jax.random.fold_in(key, 404), (HR,), jnp.float32)
    share = 0.5
    slow_rate = jnp.exp(jax.random.uniform(jax.random.fold_in(key, 505), (HR,), jnp.float32, math.log(0.1), math.log(2.0))) / LENGTH
    fast_rate = jnp.exp(jax.random.uniform(jax.random.fold_in(key, 606), (HR,), jnp.float32, math.log(0.01), math.log(0.033)))
    return jnp.where(pick < share, slow_rate, fast_rate)


def shard_levels(key, shape, pieces, smallest, high):
    level, own = 1.0, jax.random.fold_in(key, 6)
    for dim, blocks in pieces:
        steps = jnp.exp(jax.random.uniform(jax.random.fold_in(own, dim), (blocks,), jnp.float32, smallest / len(pieces), high / len(pieces)))
        level = level * jnp.repeat(steps, shape[dim] // blocks).reshape([-1 if axis == dim else 1 for axis in range(len(shape))])
    return level


def scatter_about(rng, dims, width, most, shards=(), held_as=jnp.bfloat16):
    drawn = width * jax.random.normal(rng, dims, jnp.float32)
    if shards:
        drawn = drawn * shard_levels(rng, dims, shards, -0.22, 0.18)
    return jnp.clip(drawn, -most, most).astype(held_as)


def setup_inputs(seed: int = 0) -> dict:
    key_list = jax.random.split(jax.random.key(seed), 14)
    return {
        "tokens": scatter_about(key_list[0], (SEQS, LENGTH, D), 1.0, 6.0, ((0, 4), (1, 16), (2, 2))),
        "norm_gain": jnp.clip(1.0 + 0.18 * jax.random.normal(key_list[1], (D,), jnp.float32), 0.1, 1.9),
        "query_weight": draw_query_weight(jax.random.fold_in(key_list[13], 71), 0),
        "key_weight": draw_key_weight(jax.random.fold_in(key_list[13], 71), 0),
        "value_weight": scatter_about(key_list[4], (D, HD * DV), D ** -0.5, 0.125, ((0, 4), (1, 2))),
        "state_query": scatter_about(key_list[5], (D, HR * DR), D ** -0.5, 0.125, ((0, 4), (1, 2))),
        "state_key": scatter_about(key_list[6], (D, HR * DR), D ** -0.5, 0.125, ((0, 4), (1, 2))),
        "state_value": scatter_about(key_list[7], (D, HR * DR), D ** -0.5, 0.125, ((0, 4), (1, 2))),
        "map_lambda": jnp.clip(0.3 + 0.5 * jax.random.uniform(key_list[8], (HD,), jnp.float32) ** shard_levels(key_list[8], (HD,), ((0, 2),), -0.2, 0.2), 0.3, 0.8),
        "diff_gain": jnp.clip(1.0 + 0.18 * jax.random.normal(key_list[9], (HD * DV,), jnp.float32), 0.1, 1.9),
        "decay_rate": draw_decay_rate(jax.random.fold_in(key_list[13], 71), 0),
        "state_gain": jnp.clip(1.0 + 0.18 * jax.random.normal(key_list[11], (HR * DR,), jnp.float32), 0.1, 1.9),
        "out_weight": scatter_about(key_list[12], (HD * DV + HR * DR, D), (HD * DV + HR * DR) ** -0.5, 0.125),
    }


epsilon = 1e-05
branch_scale = 0.8
masked_score = -1e+30

def normalize(values, gain):
    meansq = lax.optimization_barrier(jnp.mean(values * values, axis=-1, keepdims=True))
    return values * lax.rsqrt(meansq + epsilon) * gain

def rounded(values):
    return lax.optimization_barrier(values.astype(jnp.bfloat16)).astype(jnp.float32)

def differential(att_query, att_keys, att_values, map_lambda, diff_gain):
    length = att_query.shape[0]
    blocks = length // TOK_DEV
    query_float = att_query.reshape(blocks, TOK_DEV, HD, 2, DK).astype(jnp.float32)
    key_float = att_keys.reshape(length, HD, 2, DK).astype(jnp.float32)
    value_float = att_values.reshape(length, HD, DV).astype(jnp.float32)
    key_place = jnp.arange(length)

    def one_block(inputs):
        block_index, query_block = inputs
        query_place = block_index * TOK_DEV + jnp.arange(TOK_DEV)
        scores = jnp.einsum('qhmd,khmd->mhqk', query_block, key_float) * DK ** (-0.5)
        causal = key_place[None, :] <= query_place[:, None]
        row_peak = lax.optimization_barrier(jnp.max(jnp.where(causal, scores, masked_score), axis=-1, keepdims=True))
        weights = jnp.where(causal, jnp.exp(scores - row_peak), 0.0)
        totals = lax.optimization_barrier(jnp.sum(weights, axis=-1, keepdims=True))
        averaged = jnp.einsum('mhqk,khv->mhqv', rounded(weights), value_float) / totals
        differ = averaged[0] - map_lambda[:, None, None] * averaged[1]
        normed = normalize(differ, diff_gain.reshape(HD, 1, DV)) * branch_scale
        return normed.transpose(1, 0, 2).reshape(TOK_DEV, HD * DV).astype(jnp.bfloat16)
    outputs = lax.map(one_block, (jnp.arange(blocks), query_float))
    return outputs.reshape(length, HD * DV)

def retention(ret_query, ret_keys, ret_values, decay_rate, state_gain):
    length = ret_query.shape[0]
    blocks = length // TOK_DEV

    def to_blocks(array):
        return array.reshape(blocks, TOK_DEV, HR, DR)
    position = jnp.arange(TOK_DEV).astype(jnp.float32)
    distance = position[:, None] - position[None, :]
    decay_col = decay_rate[:, None, None]
    within = jnp.where(distance >= 0, jnp.exp(-decay_col * jnp.maximum(distance, 0.0)), 0.0)
    query_decay = jnp.exp(-decay_col * (position + 1.0)[None, :, None])
    key_decay = jnp.exp(-decay_rate[None, :, None] * (TOK_DEV - 1.0 - position)[:, None, None])
    block_decay = jnp.exp(-decay_rate * TOK_DEV)[:, None, None]

    def advance(carry_state, inputs):
        query_block, key_block, value_block = (member.astype(jnp.float32) for member in inputs)
        local_scores = jnp.einsum('qhd,khd->hqk', query_block, key_block) * within
        intra_out = jnp.einsum('hqk,khv->hqv', rounded(local_scores), value_block)
        carried = jnp.einsum('qhd,hdv->hqv', query_block, carry_state, precision=lax.Precision.HIGHEST) * query_decay
        carry_state = carry_state * block_decay + jnp.einsum('khd,khv->hdv', key_block * key_decay, value_block, precision=lax.Precision.HIGHEST)
        normed = normalize(intra_out + carried, state_gain.reshape(HR, 1, DR))
        return (carry_state, normed.transpose(1, 0, 2).reshape(TOK_DEV, HR * DR).astype(jnp.bfloat16))
    initial = jnp.zeros((HR, DR, DR), jnp.float32)
    _, outputs = lax.scan(advance, initial, (to_blocks(ret_query), to_blocks(ret_keys), to_blocks(ret_values)))
    return outputs.reshape(length, HR * DR)

def reference(tokens, norm_gain, query_weight, key_weight, value_weight, state_query, state_key, state_value, map_lambda, diff_gain, decay_rate, state_gain, out_weight):

    def one_sequence(sequence):
        tok_float = sequence.astype(jnp.float32)
        normed = normalize(tok_float, norm_gain).astype(jnp.bfloat16)

        def project(weight):
            return jnp.dot(normed, weight, preferred_element_type=jnp.float32).astype(jnp.bfloat16)
        attended = differential(project(query_weight), project(key_weight), project(value_weight), map_lambda, diff_gain)
        retained = retention(project(state_query), project(state_key), project(state_value), decay_rate, state_gain)
        joined = jnp.concatenate([attended, retained], axis=1)
        return jnp.dot(joined, out_weight, preferred_element_type=jnp.float32).astype(jnp.bfloat16)
    return lax.map(one_sequence, tokens)
```

```python
import jax
import jax.numpy as jnp
from jax import lax
from jax.experimental import pallas as pl
from jax.experimental.pallas import tpu as pltpu
from jax.sharding import Mesh
from jax.sharding import PartitionSpec as P

BF16 = jnp.bfloat16
F32 = jnp.float32
MESH = pl.DeviceIdType.MESH
SP = ("sp_0", "sp_1")
SP_TP = ("sp_0", "sp_1", "tp")
FEATURES = 2048
epsilon = 1e-05
branch_scale = 0.8
masked_score = -1e30

DMA = pltpu.SemaphoreType.DMA


def nt_dot(a, b):
    return lax.dot_general(a, b, (((1,), (1,)), ((), ())), preferred_element_type=F32)


def tn_dot(a, b):
    return lax.dot_general(a, b, (((0,), (0,)), ((), ())), preferred_element_type=F32)


def remote(src, dst, send, recv, device):
    return pltpu.make_async_remote_copy(
        src_ref=src, dst_ref=dst, send_sem=send, recv_sem=recv, device_id=device, device_id_type=MESH
    )


def arrival(ref, sem):
    pltpu.make_async_copy(ref, ref, sem).wait()


def kernel(
    tok_hbm, gain, par, wq, wk, wv, sq, sk, sv, ow_hbm, out,
    tok, ss, gl, xs, wa, wb, qkv, kv, qb, ob, join, ow, stat, rs, ps, sin, uu, rb,
    loc, g_s, g_r, w1_s, w1_r, s1_s, s1_r, s1f_s, s1f_r, s2_s, s2_r, s2f_s, s2f_r,
    x_s, x_r, xf_s, xf_r, p_s, p_r, a_s, q_s, kv_r, q_r, f_s, f_r,
    st_s, st_r, pt_s, pt_r, ja_s, jr_s, j_r,
):
    z, x, f, t = (lax.axis_index(a) for a in ("sp_0", "sp_1", "fs", "tp"))
    s = z * 4 + x
    partner = (z, x, f, 1 - t)
    up, down = lax.rem(f + 1, 4), lax.rem(f + 3, 4)

    tok_copy = pltpu.make_async_copy(tok_hbm.at[0], tok, loc.at[0])
    tok_copy.start()
    cols = pl.ds(pl.multiple_of(f * 128, 128), 128)
    own = []
    for g, (w, group) in enumerate(((wa, (wq, wk, wv)), (wb, (sq, sk, sv)))):
        for i, source in enumerate(group):
            c = pltpu.make_async_copy(source.at[:, cols], w.at[0, :, pl.ds(i * 128, 128)], loc.at[1 + g])
            c.start()
    ow_copy = pltpu.make_async_copy(ow_hbm, ow, loc.at[3])
    ow_copy.start()

    srow = pl.ds(pl.multiple_of(s * 32, 32), 32)
    for g, (w, group) in enumerate(((wa, (wq, wk, wv)), (wb, (sq, sk, sv)))):
        for k in range(1, 4):
            fd = lax.rem(f + k, 4)
            for i, source in enumerate(group):
                remote(
                    source.at[srow, pl.ds(pl.multiple_of(fd * 128, 128), 128)],
                    w.at[4 - k, srow, pl.ds(i * 128, 128)],
                    w1_s.at[g], w1_r.at[g], (z, x, fd, t),
                ).start()

    gl_copy = remote(par.at[pl.ds(0, 8), :], gl.at[t], g_s.at[0], g_r.at[0], partner)
    gl_copy.start()
    gl[t] = par[0:8, :]

    tok_copy.wait()

    @pl.loop(0, 8)
    def _(b):
        rows = pl.ds(pl.multiple_of(b * 32, 32), 32)
        v = tok[rows, :].astype(F32)
        v = v * v
        total = v[:, 0:128]
        for k in range(1, 8):
            total = total + v[:, k * 128 : (k + 1) * 128]
        ss[0, rows, :] = total

    ss_copy = remote(ss.at[0], ss.at[1], g_s.at[1], g_r.at[1], partner)
    ss_copy.start()
    ss_copy.wait_recv()

    @pl.loop(0, 8)
    def _(b):
        rows = pl.ds(pl.multiple_of(b * 32, 32), 32)
        total = jnp.sum(ss[0, rows, :] + ss[1, rows, :], axis=-1, keepdims=True)
        r = lax.rsqrt(total * (1.0 / FEATURES) + epsilon)
        v = tok[rows, :].astype(F32) * r * gain[pl.ds(t, 1), :]
        v = v.astype(BF16)
        xs[f, 2 * t, rows, :] = v[:, 0:512]
        xs[f, 2 * t + 1, rows, :] = v[:, 512:1024]

    sends = [gl_copy, ss_copy]

    def xref(e, half):
        return xs.at[lax.rem(f + e, 4), pl.ds(2 * t, 2), pl.ds(half * 128, 128), :]

    def xsend(e, half, target, send, recv):
        c = remote(xref(e, half), xref(e, half), send, recv, (z, x, target, t))
        c.start()
        sends.append(c)

    def xpair(e, half):
        c = remote(xref(e, half), xref(e, half), p_s.at[e, half], p_r.at[e, half], partner)
        c.start()
        sends.append(c)

    xsend(0, 0, up, x_s.at[0, 0], x_r.at[0, 0])
    xsend(0, 1, down, x_s.at[1, 1], x_r.at[1, 1])
    xsend(0, 1, up, x_s.at[0, 1], x_r.at[0, 1])
    xsend(0, 0, down, x_s.at[1, 0], x_r.at[1, 0])
    xpair(0, 0)
    xpair(0, 1)

    ws = (wa, wb)

    def place(g, c1, c2):
        return (c2, c1) if g == 0 else (c1, c2)

    def coords(g):
        return (x, z) if g == 0 else (z, x)

    def share(g, e1, e2, half=None):
        c1, c2 = coords(g)
        pz, px = place(g, lax.rem(c1 + e1, 4), lax.rem(c2 + e2, 4))
        start = (pz * 4 + px) * 32
        if half is None:
            return ws[g].at[pl.ds(1, 3), pl.ds(pl.multiple_of(start, 32), 32), :]
        return ws[g].at[pl.ds(1, 3), pl.ds(pl.multiple_of(start + half * 16, 16), 16), :]

    def wsend(g, ref, d1, d2, send, recv):
        c1, c2 = coords(g)
        pz, px = place(g, lax.rem(c1 + d1, 4), lax.rem(c2 + d2, 4))
        c = remote(ref, ref, send, recv, (pz, px, f, t))
        c.start()
        sends.append(c)

    step = (1, 3)
    origin = (3, 1)

    def second(g, j):
        for d in range(2):
            wsend(g, share(g, j, 0), 0, step[d], s2_s.at[g, j, d], s2_r.at[g, j, d])

    def second_forward(g, j):
        for d in range(2):
            arrival(share(g, j, origin[d]), s2_r.at[g, j, d])
            wsend(g, share(g, j, origin[d], d), 0, step[d], s2f_s.at[g, j, d], s2f_r.at[g, j, d])

    for g in range(2):
        arrival(share(g, 0, 0), w1_r.at[g])
        for d in range(2):
            wsend(g, share(g, 0, 0), step[d], 0, s1_s.at[g, d], s1_r.at[g, d])
        second(g, 0)
    for g in range(2):
        for d in range(2):
            arrival(share(g, origin[d], 0), s1_r.at[g, d])
            wsend(g, share(g, origin[d], 0, d), step[d], 0, s1f_s.at[g, d], s1f_r.at[g, d])
            second(g, origin[d])
    for g in range(2):
        second_forward(g, 0)

    arrival(xref(3, 0), x_r.at[0, 0])
    xsend(3, 0, up, xf_s.at[0], xf_r.at[0])
    xpair(3, 0)
    arrival(xref(1, 1), x_r.at[1, 1])
    xsend(1, 1, down, xf_s.at[1], xf_r.at[1])
    xpair(1, 1)

    for g in range(2):
        for d in range(2):
            arrival(share(g, 2, 0, d), s1f_r.at[g, d])
        second(g, 2)
    for j in (3, 1):
        for g in range(2):
            second_forward(g, j)
    arrival(xref(3, 1), x_r.at[0, 1])
    xpair(3, 1)
    arrival(xref(1, 0), x_r.at[1, 0])
    xpair(1, 0)
    for g in range(2):
        second_forward(g, 2)
    for j in (0, 3, 1, 2):
        for g in range(2):
            for d in range(2):
                arrival(share(g, j, 2, d), s2f_r.at[g, j, d])
    for g in range(2):
        pltpu.make_async_copy(ws[g].at[0], ws[g].at[0], loc.at[1 + g]).wait()

    def arrived_from_partner(e, half):
        q = lax.rem(f + e, 4)
        arrival(xs.at[q, pl.ds(2 * (1 - t), 2), pl.ds(half * 128, 128), :], p_r.at[e, half])

    for e in (0, 3, 1):
        for half in range(2):
            arrived_from_partner(e, half)

    late = jnp.where(s >= 11, 1, 0)

    def att_copies(q):
        found = []
        for c in range(2):
            for h in range(2):
                wanted = (s <= 10) if h == 0 else (s >= 0)
                mine = (q == z) & (2 * t + h == x) & (t == c)
                found.append((
                    remote(qkv.at[q, 1 + c], kv.at[c, s], a_s.at[q, 2 * c + h], kv_r.at[s], (q, 2 * t + h, f, c)),
                    wanted, mine,
                ))
        queries = []
        for c in range(2):
            mine = (q == z) & (2 * t + late == x) & (t == c)
            queries.append((
                remote(
                    qkv.at[q, 0, pl.ds(c * 128, 128), :], qb.at[s], q_s.at[q, c], q_r.at[s],
                    (q, 2 * t + late, f, c),
                ),
                mine,
            ))
        return found, queries

    decay = par[pl.ds(12 + f, 1), :]
    place_rows = lax.broadcasted_iota(jnp.int32, (256, 128), 0).astype(F32)
    key_decay = jnp.exp(-decay * (255.0 - place_rows))

    @pl.loop(0, 4)
    def _(k):
        e = k + (k // 2) * (1 - 2 * lax.rem(k, 2))
        q = lax.rem(f + e, 4)

        @pl.when(k == 3)
        def _():
            for half, up_down in ((0, up), (1, down)):
                arrival(xref(2, half), xf_r.at[half])
                remote(xref(2, half), xref(2, half), p_s.at[2, half], p_r.at[2, half], partner).start()
            for half in range(2):
                arrived_from_partner(2, half)

        for g in range(2):
            total = None
            for d in range(4):
                piece = jnp.dot(xs[q, lax.rem(f + d, 4)], ws[g][d], preferred_element_type=F32)
                total = piece if total is None else total + piece
            total = total.astype(BF16)
            for i in range(3):
                qkv[q, 3 * g + i] = total[:, i * 128 : (i + 1) * 128]

        found, queries = att_copies(q)
        for copy, wanted, mine in found:
            @pl.when(wanted & jnp.logical_not(mine))
            def _():
                copy.start()
        for copy, mine in queries:
            @pl.when(jnp.logical_not(mine))
            def _():
                copy.start()

        @pl.when((q == z) & ((x == 2 * t) & (s <= 10) | (x == 2 * t + 1)))
        def _():
            kv[t, s] = qkv[q, 1 + t]

        @pl.when((q == z) & (x == 2 * t + late))
        def _():
            qb[s] = qkv[q, 0, pl.ds(pl.multiple_of(t * 128, 128), 128), :]

        decayed = (qkv[q, 4].astype(F32) * key_decay).astype(BF16)
        stat[pl.ds(pl.multiple_of(q * 128, 128), 128), :] = tn_dot(decayed, qkv[q, 5]).astype(BF16)

    def st_copy(i):
        return remote(
            stat.at[pl.ds(pl.multiple_of(i * 32, 32), 32), :], rs.at[s], st_s.at[i], st_r.at[s],
            (i // 4, lax.rem(i, 4), f, t),
        )

    def pt_copy(i):
        return remote(
            ps.at[i], sin.at[pl.ds(pl.multiple_of(s * 32, 32), 32), :], pt_s.at[i], pt_r.at[s],
            (i // 4, lax.rem(i, 4), f, t),
        )

    @pl.loop(0, 16)
    def _(i):
        @pl.when(i != s)
        def _():
            st_copy(i).start()

    rs[s] = stat[srow, :]

    decay_square = jnp.broadcast_to(decay[:, 0:1], (256, 256))
    apart = (
        lax.broadcasted_iota(jnp.int32, (256, 256), 0) - lax.broadcasted_iota(jnp.int32, (256, 256), 1)
    ).astype(F32)
    within = jnp.where(apart >= 0, jnp.exp(-decay_square * jnp.maximum(apart, 0.0)), 0.0)

    @pl.loop(0, 4)
    def _(q):
        scores = nt_dot(qkv[q, 3], qkv[q, 4]) * within
        uu[q] = jnp.dot(scores.astype(BF16), qkv[q, 5], preferred_element_type=F32)

    @pl.loop(0, 16)
    def _(i):
        @pl.when(i != s)
        def _():
            arrival(rs.at[i], st_r.at[i])

    block_decay = jnp.exp(-decay * 256.0)
    carry = jnp.zeros((32, 128), F32)
    for i in range(16):
        ps[i] = carry.astype(BF16)
        if i < 15:
            carry = carry * block_decay + rs[i].astype(F32)

    @pl.loop(0, 16)
    def _(i):
        @pl.when(i != s)
        def _():
            pt_copy(i).start()

    sin[srow, :] = ps[s]

    side = lax.rem(x, 2)
    high = x // 2
    head = 4 * high + f
    key_blocks = 11 + 5 * side

    def forward_copy(i):
        return remote(kv.at[t, i], kv.at[t, i], f_s.at[i], f_r.at[i], partner)

    @pl.loop(0, key_blocks)
    def _(i):
        @pl.when(jnp.logical_not((i == s) & (high == t)))
        def _():
            arrival(kv.at[t, i], kv_r.at[i])
        forward_copy(i).start()

    arrival(gl.at[1 - t], g_r.at[0])

    @pl.loop(0, key_blocks)
    def _(i):
        arrival(kv.at[1 - t, i], f_r.at[i])

    lam = gl[high, pl.ds(4 + f, 1), :]
    att_gain = gl[high, pl.ds(f, 1), :] * branch_scale
    lane = lax.broadcasted_iota(jnp.int32, (128, 128), 1)

    def att_out(i):
        return remote(
            ob.at[i], join.at[:, pl.ds(pl.multiple_of(head * 128, 128), 128)], ja_s.at[i], j_r.at[head],
            (i // 4, lax.rem(i, 4), z, t),
        )

    def att_self(i):
        return (i == s) & (z == f)

    first_block = 11 * side

    @pl.loop(first_block, key_blocks)
    def _(i):
        @pl.when(jnp.logical_not((i == s) & (high == t)))
        def _():
            arrival(qb.at[i], q_r.at[i])

        query = qb[i].astype(F32) * 0.125
        stacked = jnp.concatenate(
            [jnp.where(lane < 64, query, 0.0), jnp.where(lane >= 64, query, 0.0)], axis=0
        ).astype(BF16)

        def absorb(j, running, masked):
            peak, total, summed = running
            scores = nt_dot(stacked, kv[0, j])
            if masked:
                row = lax.rem(lax.broadcasted_iota(jnp.int32, (256, 256), 0), 128) + 128 * t
                column = lax.broadcasted_iota(jnp.int32, (256, 256), 1)
                causal = column <= row
                scores = jnp.where(causal, scores, masked_score)
            new_peak = jnp.maximum(peak, jnp.max(scores, axis=-1, keepdims=True))
            weights = jnp.exp(scores - new_peak)
            if masked:
                weights = jnp.where(causal, weights, 0.0)
            factor = jnp.exp(peak - new_peak)
            total = total * factor + jnp.sum(weights, axis=-1, keepdims=True)
            summed = summed * factor + jnp.dot(
                weights.astype(BF16), kv[1, j], preferred_element_type=F32
            )
            return new_peak, total, summed

        running = (
            jnp.full((256, 1), masked_score, F32), jnp.zeros((256, 1), F32), jnp.zeros((256, 128), F32)
        )
        running = lax.fori_loop(0, i, lambda j, r: absorb(j, r, False), running)
        _, total, summed = absorb(i, running, True)
        averaged = summed / total
        differ = averaged[0:128] - lam * averaged[128:256]
        normed = differ * lax.rsqrt(jnp.mean(differ * differ, axis=-1, keepdims=True) + epsilon)
        result = (normed * att_gain).astype(BF16)
        ob[i] = result

        @pl.when(jnp.logical_not(att_self(i)))
        def _():
            att_out(i).start()

        @pl.when(att_self(i))
        def _():
            join[:, pl.ds(pl.multiple_of(head * 128, 128), 128)] = result

    @pl.loop(0, 16)
    def _(i):
        @pl.when(i != s)
        def _():
            arrival(sin.at[pl.ds(pl.multiple_of(i * 32, 32), 32), :], pt_r.at[i])

    ret_head = 8 + 4 * t + f
    ret_cols = pl.ds(pl.multiple_of(ret_head * 128, 128), 128)
    query_decay = jnp.exp(-decay * (place_rows + 1.0))
    state_gain = par[pl.ds(8 + f, 1), :]

    def ret_out(q, c):
        return remote(
            rb.at[q, pl.ds(c * 128, 128), :], join.at[:, ret_cols], jr_s.at[q, c], j_r.at[ret_head], (z, x, q, c)
        )

    def ret_self(q, c):
        return (q == f) & (t == c)

    @pl.loop(0, 4)
    def _(q):
        state = sin[pl.ds(pl.multiple_of(q * 128, 128), 128), :]
        u = uu[q] + jnp.dot(qkv[q, 3], state, preferred_element_type=F32) * query_decay
        normed = u * lax.rsqrt(jnp.mean(u * u, axis=-1, keepdims=True) + epsilon)
        rb[q] = (normed * state_gain).astype(BF16)
        for c in range(2):
            @pl.when(jnp.logical_not(ret_self(q, c)))
            def _():
                ret_out(q, c).start()

            @pl.when(ret_self(q, c))
            def _():
                join[:, ret_cols] = rb[q, c * 128 : (c + 1) * 128, :]

    @pl.loop(0, 8)
    def _(h):
        @pl.when(jnp.logical_not((lax.rem(h, 4) == f) & (z == f) & (x == 2 * (h // 4) + late)))
        def _():
            arrival(ob.at[0], j_r.at[h])

        @pl.when(h != 4 * t + f)
        def _():
            arrival(ob.at[0], j_r.at[8 + h])

    ow_copy.wait()

    @pl.loop(0, 4)
    def _(n):
        span = pl.ds(pl.multiple_of(n * 512, 512), 512)
        out[:, span] = jnp.dot(join[...], ow[:, span], preferred_element_type=F32).astype(BF16)

    for g in range(2):
        arrival(share(g, 0, 0), w1_s.at[g])
    for c in sends:
        c.wait_send()
    for half in range(2):
        remote(xref(2, half), xref(2, half), p_s.at[2, half], p_r.at[2, half], partner).wait_send()

    @pl.loop(0, 4)
    def _(q):
        found, queries = att_copies(q)
        for copy, wanted, mine in found:
            @pl.when(wanted & jnp.logical_not(mine))
            def _():
                copy.wait_send()
        for copy, mine in queries:
            @pl.when(jnp.logical_not(mine))
            def _():
                copy.wait_send()
        for c in range(2):
            @pl.when(jnp.logical_not(ret_self(q, c)))
            def _():
                ret_out(q, c).wait_send()

    @pl.loop(0, 16)
    def _(i):
        @pl.when(i != s)
        def _():
            st_copy(i).wait_send()
            pt_copy(i).wait_send()

    @pl.loop(0, key_blocks)
    def _(i):
        forward_copy(i).wait_send()

    @pl.loop(first_block, key_blocks)
    def _(i):
        @pl.when(jnp.logical_not(att_self(i)))
        def _():
            att_out(i).wait_send()


def body(
    tokens, norm_gain, query_weight, key_weight, value_weight, state_query, state_key, state_value,
    map_lambda, diff_gain, decay_rate, state_gain, out_weight,
):
    wide = lambda v: jnp.broadcast_to(v[:, None], (4, 128))
    params = jnp.concatenate(
        [diff_gain.reshape(4, 128), wide(map_lambda), state_gain.reshape(4, 128), wide(decay_rate)], axis=0
    )
    hbm = pl.BlockSpec(memory_space=pl.ANY)
    vmem = pl.BlockSpec(memory_space=pltpu.VMEM)
    out = pl.pallas_call(
        kernel,
        out_shape=jax.ShapeDtypeStruct((128, FEATURES), BF16),
        in_specs=[hbm, vmem, vmem] + [hbm] * 7,
        out_specs=vmem,
        scratch_shapes=[
            pltpu.VMEM((256, 1024), BF16),
            pltpu.VMEM((2, 256, 128), F32),
            pltpu.VMEM((2, 8, 128), F32),
            pltpu.VMEM((4, 4, 256, 512), BF16),
            pltpu.VMEM((4, 512, 384), BF16),
            pltpu.VMEM((4, 512, 384), BF16),
            pltpu.VMEM((4, 6, 256, 128), BF16),
            pltpu.VMEM((2, 16, 256, 128), BF16),
            pltpu.VMEM((16, 128, 128), BF16),
            pltpu.VMEM((16, 128, 128), BF16),
            pltpu.VMEM((128, FEATURES), BF16),
            pltpu.VMEM((FEATURES, FEATURES), BF16),
            pltpu.VMEM((512, 128), BF16),
            pltpu.VMEM((16, 32, 128), BF16),
            pltpu.VMEM((16, 32, 128), BF16),
            pltpu.VMEM((512, 128), BF16),
            pltpu.VMEM((4, 256, 128), F32),
            pltpu.VMEM((4, 256, 128), BF16),
            DMA((4,)), DMA((2,)), DMA((2,)), DMA((2,)), DMA((2,)),
            DMA((2, 2)), DMA((2, 2)), DMA((2, 2)), DMA((2, 2)),
            DMA((2, 4, 2)), DMA((2, 4, 2)), DMA((2, 4, 2)), DMA((2, 4, 2)),
            DMA((2, 2)), DMA((2, 2)), DMA((2,)), DMA((2,)), DMA((4, 2)), DMA((4, 2)),
            DMA((4, 4)), DMA((4, 2)), DMA((16,)), DMA((16,)), DMA((16,)), DMA((16,)),
            DMA((16,)), DMA((16,)), DMA((16,)), DMA((16,)),
            DMA((16,)), DMA((4, 2)), DMA((16,)),
        ],
        compiler_params=pltpu.CompilerParams(has_side_effects=True, vmem_limit_bytes=60 * 1024 * 1024),
        name="layer",
    )(
        tokens, norm_gain.reshape(2, FEATURES // 2), params,
        query_weight, key_weight, value_weight, state_query, state_key, state_value, out_weight,
    )
    return out[None]


def solution(mesh):
    torus = Mesh(
        mesh.devices.reshape(4, 4, mesh.shape["fs"], mesh.shape["tp"]), ("sp_0", "sp_1", "fs", "tp")
    )
    return jax.shard_map(
        body,
        mesh=torus,
        in_specs=(
            P("fs", SP, "tp"), P(), P("fs", "tp"), P("fs", "tp"), P("fs", "tp"), P("fs", "tp"), P("fs", "tp"),
            P("fs", "tp"), P("tp"), P("tp"), P("tp"), P("tp"), P(),
        ),
        out_specs=P("fs", SP_TP, None),
        check_vma=False,
    )
```

```python
import jax
import jax.numpy as jnp
from jax import lax
from jax.experimental import pallas as pl
from jax.experimental.pallas import tpu as pltpu
from jax.sharding import Mesh
from jax.sharding import PartitionSpec as P

BF16 = jnp.bfloat16
F32 = jnp.float32
MESH = pl.DeviceIdType.MESH
SP = ("sp_0", "sp_1")
SP_TP = ("sp_0", "sp_1", "tp")
FEATURES = 2048
epsilon = 1e-05
branch_scale = 0.8
masked_score = -1e30

DMA = pltpu.SemaphoreType.DMA


def nt_dot(a, b):
    return lax.dot_general(a, b, (((1,), (1,)), ((), ())), preferred_element_type=F32)


def tn_dot(a, b):
    return lax.dot_general(a, b, (((0,), (0,)), ((), ())), preferred_element_type=F32)


def remote(src, dst, send, recv, device):
    return pltpu.make_async_remote_copy(
        src_ref=src, dst_ref=dst, send_sem=send, recv_sem=recv, device_id=device, device_id_type=MESH
    )


def arrival(ref, sem):
    pltpu.make_async_copy(ref, ref, sem).wait()


def kernel(
    tok_hbm, norm_gain, diff_gain, state_gain, lambda_hbm, decay_hbm, wq, wk, wv, sq, sk, sv, join,
    map_lambda, decay_rate, tok, gain, rows, ss, gl, xs, wa, wb, qkv, kk, vv, qb, qs, peaks, sums, ob, stat, rs, ps, sin, uu, rb,
    loc, g_s, g_r, w1_s, w1_r, s1_s, s1_r, s1f_s, s1f_r, s2_s, s2_r, s2f_s, s2f_r,
    x_s, x_r, xf_s, xf_r, p_s, p_r, a_s, q_s, kv_r, q_r, f_s, f_r,
    st_s, st_r, pt_s, pt_r, ja_s, jr_s, j_r,
):
    z, x, f, t = (lax.axis_index(a) for a in ("sp_0", "sp_1", "fs", "tp"))
    s = z * 4 + x
    partner = (z, x, f, 1 - t)
    up, down = lax.rem(f + 1, 4), lax.rem(f + 3, 4)
    side = lax.rem(x, 2)
    high = x // 2

    barrier = pltpu.get_barrier_semaphore()
    peers = [partner]
    for k in (1, 3):
        peers += [(z, lax.rem(x + k, 4), f, t), (lax.rem(z + k, 4), x, f, t)]
    for k in (1, 2, 3):
        peers.append((z, x, lax.rem(f + k, 4), t))
    for peer in peers:
        pl.semaphore_signal(barrier, inc=1, device_id=peer, device_id_type=MESH)

    tok_copy = pltpu.make_async_copy(tok_hbm.at[0], tok, loc.at[0])
    tok_copy.start()
    cols = pl.ds(pl.multiple_of(f * 128, 128), 128)
    small = [
        pltpu.make_async_copy(norm_gain.at[pl.ds(pl.multiple_of(t * 1024, 1024), 1024)], gain.at[0], loc.at[3]),
        pltpu.make_async_copy(diff_gain.at[cols], rows.at[0], loc.at[4]),
        pltpu.make_async_copy(state_gain.at[cols], rows.at[2], loc.at[5]),
        pltpu.make_async_copy(lambda_hbm, map_lambda, loc.at[6]),
        pltpu.make_async_copy(decay_hbm, decay_rate, loc.at[7]),
    ]
    for c in small:
        c.start()
    groups = tuple(enumerate(((wa, (wq, wk, wv)), (wb, (sq, sk, sv)))))
    for g, (w, group) in groups:
        for i, source in enumerate(group):
            pltpu.make_async_copy(
                source.at[:, cols], w.at[0, :, pl.ds(i * 128, 128)], loc.at[1 + g]
            ).start()

    tok_copy.wait()

    @pl.loop(0, 8)
    def _(b):
        block = pl.ds(pl.multiple_of(b * 32, 32), 32)
        v = tok[block, :].astype(F32)
        v = v * v
        total = v[:, 0:128]
        for k in range(1, 8):
            total = total + v[:, k * 128 : (k + 1) * 128]
        ss[0, block, :] = total

    for c in small:
        c.wait()
    rows[1] = jnp.full((128,), map_lambda[f], F32)

    pl.semaphore_wait(barrier, len(peers))

    ss_copy = remote(ss.at[0], ss.at[1], g_s.at[1], g_r.at[1], partner)
    ss_copy.start()

    srow = pl.ds(pl.multiple_of(s * 32, 32), 32)
    for g, (w, group) in groups:
        for k in range(1, 4):
            fd = lax.rem(f + k, 4)
            for i, source in enumerate(group):
                remote(
                    source.at[srow, pl.ds(pl.multiple_of(fd * 128, 128), 128)],
                    w.at[4 - k, srow, pl.ds(i * 128, 128)],
                    w1_s.at[g], w1_r.at[g], (z, x, fd, t),
                ).start()

    gl_copy = remote(rows, gl.at[t], g_s.at[0], g_r.at[0], partner)
    gl_copy.start()
    gl[t] = rows[...]
    vv[:, :, 128:256] = jnp.ones((16, 256, 128), BF16)

    @pl.when(side == 0)
    def _():
        kk[11] = jnp.zeros((256, 128), BF16)
        vv[11, :, 0:128] = jnp.zeros((256, 128), BF16)

    ss_copy.wait_recv()

    @pl.loop(0, 8)
    def _(b):
        block = pl.ds(pl.multiple_of(b * 32, 32), 32)
        total = jnp.sum(ss[0, block, :] + ss[1, block, :], axis=-1, keepdims=True)
        r = lax.rsqrt(total * (1.0 / FEATURES) + epsilon)
        v = tok[block, :].astype(F32) * r * gain[...]
        v = v.astype(BF16)
        xs[f, 2 * t, block, :] = v[:, 0:512]
        xs[f, 2 * t + 1, block, :] = v[:, 512:1024]

    sends = [gl_copy, ss_copy]

    def xref(e, half):
        return xs.at[lax.rem(f + e, 4), pl.ds(2 * t, 2), pl.ds(half * 128, 128), :]

    def xsend(e, half, target, send, recv):
        c = remote(xref(e, half), xref(e, half), send, recv, (z, x, target, t))
        c.start()
        sends.append(c)

    def xpair(e, half):
        c = remote(xref(e, half), xref(e, half), p_s.at[e, half], p_r.at[e, half], partner)
        c.start()
        sends.append(c)

    xsend(0, 0, up, x_s.at[0, 0], x_r.at[0, 0])
    xsend(0, 1, down, x_s.at[1, 1], x_r.at[1, 1])
    xsend(0, 1, up, x_s.at[0, 1], x_r.at[0, 1])
    xsend(0, 0, down, x_s.at[1, 0], x_r.at[1, 0])
    xpair(0, 0)
    xpair(0, 1)

    ws = (wa, wb)

    def place(g, c1, c2):
        return (c2, c1) if g == 0 else (c1, c2)

    def coords(g):
        return (x, z) if g == 0 else (z, x)

    def share(g, e1, e2, half=None):
        c1, c2 = coords(g)
        pz, px = place(g, lax.rem(c1 + e1, 4), lax.rem(c2 + e2, 4))
        start = (pz * 4 + px) * 32
        if half is None:
            return ws[g].at[pl.ds(1, 3), pl.ds(pl.multiple_of(start, 32), 32), :]
        return ws[g].at[pl.ds(1, 3), pl.ds(pl.multiple_of(start + half * 16, 16), 16), :]

    def wsend(g, ref, d1, d2, send, recv):
        c1, c2 = coords(g)
        pz, px = place(g, lax.rem(c1 + d1, 4), lax.rem(c2 + d2, 4))
        c = remote(ref, ref, send, recv, (pz, px, f, t))
        c.start()
        sends.append(c)

    step = (1, 3)
    origin = (3, 1)

    def second(g, j):
        for d in range(2):
            wsend(g, share(g, j, 0), 0, step[d], s2_s.at[g, j, d], s2_r.at[g, j, d])

    def second_forward(g, j):
        for d in range(2):
            arrival(share(g, j, origin[d]), s2_r.at[g, j, d])
            wsend(g, share(g, j, origin[d], d), 0, step[d], s2f_s.at[g, j, d], s2f_r.at[g, j, d])

    for g in range(2):
        arrival(share(g, 0, 0), w1_r.at[g])
        for d in range(2):
            wsend(g, share(g, 0, 0), step[d], 0, s1_s.at[g, d], s1_r.at[g, d])
        second(g, 0)
    for g in range(2):
        for d in range(2):
            arrival(share(g, origin[d], 0), s1_r.at[g, d])
            wsend(g, share(g, origin[d], 0, d), step[d], 0, s1f_s.at[g, d], s1f_r.at[g, d])
            second(g, origin[d])
    for g in range(2):
        second_forward(g, 0)

    arrival(xref(3, 0), x_r.at[0, 0])
    xsend(3, 0, up, xf_s.at[0], xf_r.at[0])
    xpair(3, 0)
    arrival(xref(1, 1), x_r.at[1, 1])
    xsend(1, 1, down, xf_s.at[1], xf_r.at[1])
    xpair(1, 1)

    for g in range(2):
        for d in range(2):
            arrival(share(g, 2, 0, d), s1f_r.at[g, d])
        second(g, 2)
    for j in (3, 1):
        for g in range(2):
            second_forward(g, j)
    arrival(xref(3, 1), x_r.at[0, 1])
    xpair(3, 1)
    arrival(xref(1, 0), x_r.at[1, 0])
    xpair(1, 0)
    for g in range(2):
        second_forward(g, 2)
    for j in (0, 3, 1, 2):
        for g in range(2):
            for d in range(2):
                arrival(share(g, j, 2, d), s2f_r.at[g, j, d])
    for g in range(2):
        pltpu.make_async_copy(ws[g].at[0], ws[g].at[0], loc.at[1 + g]).wait()

    def arrived_from_partner(e, half):
        q = lax.rem(f + e, 4)
        arrival(xs.at[q, pl.ds(2 * (1 - t), 2), pl.ds(half * 128, 128), :], p_r.at[e, half])

    for e in (0, 3, 1):
        for half in range(2):
            arrived_from_partner(e, half)

    late = jnp.where(s >= 11, 1, 0)

    def owner(q, u, c):
        return (lax.rem(q + u, 4), u, f, c)

    def att_copies(q):
        my_sequence = q == lax.rem(z + 4 - x, 4)
        found = []
        for h in (1, 0):
            u = 2 * t + h
            for c in range(2):
                target = kk.at[s] if c == 0 else vv.at[s, :, pl.ds(0, 128)]
                copy = remote(qkv.at[q, 1 + c], target, a_s.at[q, 2 * c + h], kv_r.at[s], owner(q, u, c))
                elsewhere = jnp.logical_not(my_sequence & (x == u) & (t == c))
                found.append((copy, elsewhere if h == 1 else elsewhere & (s <= 10)))
        u = 2 * t + late
        for c in range(2):
            copy = remote(
                qkv.at[q, 0, pl.ds(c * 128, 128), :], qb.at[s], q_s.at[q, c], q_r.at[s], owner(q, u, c)
            )
            found.append((copy, jnp.logical_not(my_sequence & (x == u) & (t == c))))
        return found

    decay = jnp.full((1, 128), decay_rate[f], F32)
    place_rows = lax.broadcasted_iota(jnp.int32, (256, 128), 0).astype(F32)
    key_decay = jnp.exp(-decay * (255.0 - place_rows))

    @pl.loop(0, 4)
    def _(k):
        e = k + (k // 2) * (1 - 2 * lax.rem(k, 2))
        q = lax.rem(f + e, 4)

        @pl.when(k == 3)
        def _():
            for half, up_down in ((0, up), (1, down)):
                arrival(xref(2, half), xf_r.at[half])
                remote(xref(2, half), xref(2, half), p_s.at[2, half], p_r.at[2, half], partner).start()
            for half in range(2):
                arrived_from_partner(2, half)

        for g in range(2):
            total = None
            for d in range(4):
                piece = jnp.dot(xs[q, lax.rem(f + d, 4)], ws[g][d], preferred_element_type=F32)
                total = piece if total is None else total + piece
            total = total.astype(BF16)
            for i in range(3):
                qkv[q, 3 * g + i] = total[:, i * 128 : (i + 1) * 128]

        for copy, condition in att_copies(q):
            @pl.when(condition)
            def _():
                copy.start()

        kept = (q == lax.rem(z + 4 - x, 4)) & (high == t)

        @pl.when(kept & ((side == 1) | (s <= 10)))
        def _():
            @pl.when(t == 0)
            def _():
                kk[s] = qkv[q, 1]

            @pl.when(t == 1)
            def _():
                vv[s, :, 0:128] = qkv[q, 2]

        @pl.when(kept & (side == late))
        def _():
            qb[s] = qkv[q, 0, pl.ds(pl.multiple_of(t * 128, 128), 128), :]

        decayed = (qkv[q, 4].astype(F32) * key_decay).astype(BF16)
        stat[pl.ds(pl.multiple_of(q * 128, 128), 128), :] = tn_dot(decayed, qkv[q, 5]).astype(BF16)

    def st_copy(i):
        return remote(
            stat.at[pl.ds(pl.multiple_of(i * 32, 32), 32), :], rs.at[s], st_s.at[i], st_r.at[s],
            (i // 4, lax.rem(i, 4), f, t),
        )

    def pt_copy(i):
        return remote(
            ps.at[i], sin.at[pl.ds(pl.multiple_of(s * 32, 32), 32), :], pt_s.at[i], pt_r.at[s],
            (i // 4, lax.rem(i, 4), f, t),
        )

    @pl.loop(0, 16)
    def _(i):
        @pl.when(i != s)
        def _():
            st_copy(i).start()

    rs[s] = stat[srow, :]

    decay_square = jnp.broadcast_to(decay[:, 0:1], (256, 256))
    apart = (
        lax.broadcasted_iota(jnp.int32, (256, 256), 0) - lax.broadcasted_iota(jnp.int32, (256, 256), 1)
    ).astype(F32)
    within = jnp.where(apart >= 0, jnp.exp(-decay_square * jnp.maximum(apart, 0.0)), 0.0)

    @pl.loop(0, 4)
    def _(q):
        scores = nt_dot(qkv[q, 3], qkv[q, 4]) * within
        uu[q] = jnp.dot(scores.astype(BF16), qkv[q, 5], preferred_element_type=F32)

    sequence = lax.rem(z + 4 - x, 4)
    head = 4 * high + f
    key_blocks = 11 + 5 * side
    first_block = 11 * side
    kv_buffers = (lambda i: kk.at[i], lambda i: vv.at[i, :, pl.ds(0, 128)])

    def forward_copy(c, i):
        return remote(kv_buffers[c](i), kv_buffers[c](i), f_s.at[i], f_r.at[i], partner)

    for c in range(2):
        @pl.when(t == c)
        def _():
            @pl.loop(0, key_blocks)
            def _(i):
                @pl.when(jnp.logical_not((i == s) & (high == t)))
                def _():
                    arrival(kv_buffers[c](i), kv_r.at[i])
                forward_copy(c, i).start()

    arrival(gl.at[1 - t], g_r.at[0])

    @pl.loop(first_block, key_blocks)
    def _(i):
        @pl.when(jnp.logical_not((i == s) & (high == t)))
        def _():
            arrival(qb.at[i], q_r.at[i])

    @pl.loop(0, key_blocks)
    def _(i):
        arrival(qb.at[pl.ds(0, 2)], f_r.at[i])

    lam = gl[high, pl.ds(1, 1), :]
    att_gain = gl[high, pl.ds(0, 1), :] * branch_scale
    lane = lax.broadcasted_iota(jnp.int32, (128, 128), 1)
    join_cols = pl.ds(pl.multiple_of(head * 128, 128), 128)

    def att_out(i):
        return remote(
            ob.at[i], join.at[:, join_cols], ja_s.at[i], j_r.at[head], (i // 4, lax.rem(i, 4), sequence, t)
        )

    def att_self(i):
        return (i == s) & (sequence == f)

    def attention(first, count, m):
        for b in range(count):
            query = qb[first + b].astype(F32) * 0.125
            qs[b * 256 : b * 256 + 128] = jnp.where(lane < 64, query, 0.0).astype(BF16)
            qs[b * 256 + 128 : b * 256 + 256] = jnp.where(lane >= 64, query, 0.0).astype(BF16)
            peaks[b * 256 : b * 256 + 256] = jnp.full((256, 128), masked_score, F32)
            sums[b * 256 : b * 256 + 256] = jnp.zeros((256, 256), F32)

        def absorb(c, masked):
            keys = kk[pl.ds(2 * c, 2)].reshape(512, 128)
            values = vv[pl.ds(2 * c, 2)].reshape(512, 256)
            for b in range(count):
                span = slice(b * 256, b * 256 + 256)
                scores = nt_dot(qs[span], keys)
                if masked:
                    row = lax.rem(lax.broadcasted_iota(jnp.int32, (256, 512), 0), 128)
                    row = row + (128 * t + 256 * (first + b - 2 * m))
                    column = lax.broadcasted_iota(jnp.int32, (256, 512), 1)
                    scores = jnp.where(column <= row, scores, masked_score)
                peak = peaks[span]
                new_peak = jnp.maximum(peak, jnp.max(scores, axis=-1, keepdims=True))
                weights = jnp.exp(scores - jnp.concatenate([new_peak] * 4, axis=1)).astype(BF16)
                factor = jnp.exp(peak - new_peak)
                sums[span] = sums[span] * jnp.concatenate([factor] * 2, axis=1) + jnp.dot(
                    weights, values, preferred_element_type=F32
                )
                peaks[span] = new_peak

        @pl.loop(0, m)
        def _(c):
            absorb(c, False)

        absorb(m, True)
        for b in range(count):
            i = first + b
            averaged = sums[b * 256 : b * 256 + 256, 0:128] / sums[b * 256 : b * 256 + 256, 128:256]
            differ = averaged[0:128] - lam * averaged[128:256]
            normed = differ * lax.rsqrt(jnp.mean(differ * differ, axis=-1, keepdims=True) + epsilon)
            result = (normed * att_gain).astype(BF16)
            ob[i] = result

            @pl.when(jnp.logical_not(att_self(i)))
            def _():
                att_out(i).start()

            @pl.when(att_self(i))
            def _():
                join[:, join_cols] = result

    attention(10 + side, 1, 5)

    @pl.loop(0, 16)
    def _(i):
        @pl.when(i != s)
        def _():
            arrival(rs.at[i], st_r.at[i])

    block_decay = jnp.exp(-decay * 256.0)
    carry = jnp.zeros((32, 128), F32)
    for i in range(16):
        ps[i] = carry.astype(BF16)
        if i < 15:
            carry = carry * block_decay + rs[i].astype(F32)

    @pl.loop(0, 16)
    def _(i):
        @pl.when(i != s)
        def _():
            pt_copy(i).start()

    sin[srow, :] = ps[s]

    @pl.loop(6 * side, 5 + 3 * side)
    def _(m):
        attention(2 * m, 2, m)

    @pl.loop(0, 16)
    def _(i):
        @pl.when(i != s)
        def _():
            arrival(sin.at[pl.ds(pl.multiple_of(i * 32, 32), 32), :], pt_r.at[i])

    ret_head = 8 + 4 * t + f
    ret_cols = pl.ds(pl.multiple_of(ret_head * 128, 128), 128)
    query_decay = jnp.exp(-decay * (place_rows + 1.0))
    ret_gain = rows[2:3, :]

    def ret_out(q, c):
        return remote(
            rb.at[q, pl.ds(c * 128, 128), :], join.at[:, ret_cols], jr_s.at[q, c], j_r.at[ret_head], (z, x, q, c)
        )

    def ret_self(q, c):
        return (q == f) & (t == c)

    @pl.loop(0, 4)
    def _(q):
        state = sin[pl.ds(pl.multiple_of(q * 128, 128), 128), :]
        u = uu[q] + jnp.dot(qkv[q, 3], state, preferred_element_type=F32) * query_decay
        normed = u * lax.rsqrt(jnp.mean(u * u, axis=-1, keepdims=True) + epsilon)
        rb[q] = (normed * ret_gain).astype(BF16)
        for c in range(2):
            @pl.when(jnp.logical_not(ret_self(q, c)))
            def _():
                ret_out(q, c).start()

            @pl.when(ret_self(q, c))
            def _():
                join[:, ret_cols] = rb[q, c * 128 : (c + 1) * 128, :]

    @pl.loop(0, 8)
    def _(h):
        @pl.when(jnp.logical_not((lax.rem(h, 4) == f) & (sequence == f) & (x == 2 * (h // 4) + late)))
        def _():
            arrival(ob.at[0], j_r.at[h])

        @pl.when(h != 4 * t + f)
        def _():
            arrival(ob.at[0], j_r.at[8 + h])

    for g in range(2):
        arrival(share(g, 0, 0), w1_s.at[g])
    for c in sends:
        c.wait_send()
    for half in range(2):
        remote(xref(2, half), xref(2, half), p_s.at[2, half], p_r.at[2, half], partner).wait_send()

    @pl.loop(0, 4)
    def _(q):
        for copy, condition in att_copies(q):
            @pl.when(condition)
            def _():
                copy.wait_send()
        for c in range(2):
            @pl.when(jnp.logical_not(ret_self(q, c)))
            def _():
                ret_out(q, c).wait_send()

    @pl.loop(0, 16)
    def _(i):
        @pl.when(i != s)
        def _():
            st_copy(i).wait_send()
            pt_copy(i).wait_send()

    @pl.loop(0, key_blocks)
    def _(i):
        remote(qb.at[pl.ds(0, 2)], qb.at[pl.ds(0, 2)], f_s.at[i], f_r.at[i], partner).wait_send()

    @pl.loop(first_block, key_blocks)
    def _(i):
        @pl.when(jnp.logical_not(att_self(i)))
        def _():
            att_out(i).wait_send()


def body(
    tokens, norm_gain, query_weight, key_weight, value_weight, state_query, state_key, state_value,
    map_lambda, diff_gain, decay_rate, state_gain, out_weight,
):
    hbm = pl.BlockSpec(memory_space=pltpu.HBM)
    vmem = pl.BlockSpec(memory_space=pltpu.VMEM)
    joined = pl.pallas_call(
        kernel,
        out_shape=jax.ShapeDtypeStruct((128, FEATURES), BF16),
        in_specs=[hbm] * 12,
        out_specs=vmem,
        scratch_shapes=[
            pltpu.SMEM((4,), F32),
            pltpu.SMEM((4,), F32),
            pltpu.VMEM((256, 1024), BF16),
            pltpu.VMEM((1, 1024), F32),
            pltpu.VMEM((8, 128), F32),
            pltpu.VMEM((2, 256, 128), F32),
            pltpu.VMEM((2, 8, 128), F32),
            pltpu.VMEM((4, 4, 256, 512), BF16),
            pltpu.VMEM((4, 512, 384), BF16),
            pltpu.VMEM((4, 512, 384), BF16),
            pltpu.VMEM((4, 6, 256, 128), BF16),
            pltpu.VMEM((16, 256, 128), BF16),
            pltpu.VMEM((16, 256, 256), BF16),
            pltpu.VMEM((16, 128, 128), BF16),
            pltpu.VMEM((512, 128), BF16),
            pltpu.VMEM((512, 128), F32),
            pltpu.VMEM((512, 256), F32),
            pltpu.VMEM((16, 128, 128), BF16),
            pltpu.VMEM((512, 128), BF16),
            pltpu.VMEM((16, 32, 128), BF16),
            pltpu.VMEM((16, 32, 128), BF16),
            pltpu.VMEM((512, 128), BF16),
            pltpu.VMEM((4, 256, 128), F32),
            pltpu.VMEM((4, 256, 128), BF16),
            DMA((8,)), DMA((2,)), DMA((2,)), DMA((2,)), DMA((2,)),
            DMA((2, 2)), DMA((2, 2)), DMA((2, 2)), DMA((2, 2)),
            DMA((2, 4, 2)), DMA((2, 4, 2)), DMA((2, 4, 2)), DMA((2, 4, 2)),
            DMA((2, 2)), DMA((2, 2)), DMA((2,)), DMA((2,)), DMA((4, 2)), DMA((4, 2)),
            DMA((4, 4)), DMA((4, 2)), DMA((16,)), DMA((16,)), DMA((16,)), DMA((16,)),
            DMA((16,)), DMA((16,)), DMA((16,)), DMA((16,)),
            DMA((16,)), DMA((4, 2)), DMA((16,)),
        ],
        compiler_params=pltpu.CompilerParams(
            collective_id=0, has_side_effects=True, vmem_limit_bytes=32 * 1024 * 1024
        ),
        cost_estimate=pl.CostEstimate(flops=40_000_000_000, bytes_accessed=8_000_000, transcendentals=8_000_000),
        name="layer",
    )(
        *(
            pltpu.with_memory_space_constraint(a, pltpu.HBM)
            for a in (
                tokens, norm_gain, diff_gain, state_gain, map_lambda, decay_rate,
                query_weight, key_weight, value_weight, state_query, state_key, state_value,
            )
        )
    )
    return jnp.dot(joined, out_weight, preferred_element_type=F32).astype(BF16)[None]


def solution(mesh):
    torus = Mesh(
        mesh.devices.reshape(4, 4, mesh.shape["fs"], mesh.shape["tp"]), ("sp_0", "sp_1", "fs", "tp")
    )
    return jax.shard_map(
        body,
        mesh=torus,
        in_specs=(
            P("fs", SP, "tp"), P(), P("fs", "tp"), P("fs", "tp"), P("fs", "tp"), P("fs", "tp"), P("fs", "tp"),
            P("fs", "tp"), P("tp"), P("tp"), P("tp"), P("tp"), P(),
        ),
        out_specs=P("fs", SP_TP, None),
        check_vma=False,
    )
```

```python
import jax
import jax.numpy as jnp
from jax import lax
from jax.experimental import pallas as pl
from jax.experimental.pallas import tpu as pltpu
from jax.sharding import Mesh
from jax.sharding import PartitionSpec as P

BF16 = jnp.bfloat16
F32 = jnp.float32
MESH = pl.DeviceIdType.MESH
SP = ("sp_0", "sp_1")
SP_TP = ("sp_0", "sp_1", "tp")
FEATURES = 2048
epsilon = 1e-05
branch_scale = 0.8
masked_score = -1e30

DMA = pltpu.SemaphoreType.DMA


def nt_dot(a, b):
    return lax.dot_general(a, b, (((1,), (1,)), ((), ())), preferred_element_type=F32)


def tn_dot(a, b):
    return lax.dot_general(a, b, (((0,), (0,)), ((), ())), preferred_element_type=F32)


def remote(src, dst, send, recv, device):
    return pltpu.make_async_remote_copy(
        src_ref=src, dst_ref=dst, send_sem=send, recv_sem=recv, device_id=device, device_id_type=MESH
    )


def arrival(ref, sem):
    pltpu.make_async_copy(ref, ref, sem).wait()


def kernel(
    tok_hbm, norm_gain, diff_gain, state_gain, lambda_hbm, decay_hbm, wq, wk, wv, sq, sk, sv, join,
    map_lambda, decay_rate, tok, gain, rows, ss, gl, xs, ws, qkv, kk, vv, qb, qs, sums, ob, stat, rs, ps, sin, uu, rb,
    loc, g_s, g_r, w1_s, w1_r, s1_s, s1_r, s1f_s, s1f_r, s2_s, s2_r, s2f_s, s2f_r,
    x_s, x_r, xf_s, xf_r, p_s, p_r, a_s, q_s, kv_r, q_r, f_s, f_r,
    st_s, st_r, pt_s, pt_r, ja_s, jr_s, j_r,
):
    z, x, f, t = (lax.axis_index(a) for a in ("sp_0", "sp_1", "fs", "tp"))
    s = z * 4 + x
    partner = (z, x, f, 1 - t)
    up, down = lax.rem(f + 1, 4), lax.rem(f + 3, 4)
    side = lax.rem(x, 2)
    high = x // 2

    barrier = pltpu.get_barrier_semaphore()
    peers = [partner]
    for k in (1, 3):
        peers += [(z, lax.rem(x + k, 4), f, t), (lax.rem(z + k, 4), x, f, t)]
    for k in (1, 2, 3):
        peers.append((z, x, lax.rem(f + k, 4), t))
    for peer in peers:
        pl.semaphore_signal(barrier, inc=1, device_id=peer, device_id_type=MESH)

    tok_copy = pltpu.make_async_copy(tok_hbm.at[0], tok, loc.at[0])
    tok_copy.start()
    cols = pl.ds(pl.multiple_of(f * 128, 128), 128)
    small = [
        pltpu.make_async_copy(norm_gain.at[pl.ds(pl.multiple_of(t * 1024, 1024), 1024)], gain.at[0], loc.at[3]),
        pltpu.make_async_copy(diff_gain.at[cols], rows.at[0], loc.at[4]),
        pltpu.make_async_copy(state_gain.at[cols], rows.at[2], loc.at[5]),
        pltpu.make_async_copy(lambda_hbm, map_lambda, loc.at[6]),
        pltpu.make_async_copy(decay_hbm, decay_rate, loc.at[7]),
    ]
    for c in small:
        c.start()
    groups = tuple(enumerate(((wq, wk, wv), (sq, sk, sv))))
    for g, group in groups:
        for i, source in enumerate(group):
            pltpu.make_async_copy(
                source.at[:, cols], ws.at[0, :, pl.ds((3 * g + i) * 128, 128)], loc.at[1 + g]
            ).start()

    tok_copy.wait()

    @pl.loop(0, 8)
    def _(b):
        block = pl.ds(pl.multiple_of(b * 32, 32), 32)
        v = tok[block, :].astype(F32)
        v = v * v
        total = v[:, 0:128]
        for k in range(1, 8):
            total = total + v[:, k * 128 : (k + 1) * 128]
        ss[0, block, :] = total

    for c in small:
        c.wait()
    rows[1] = jnp.full((128,), map_lambda[f], F32)

    pl.semaphore_wait(barrier, len(peers))

    ss_copy = remote(ss.at[0], ss.at[1], g_s.at[1], g_r.at[1], partner)
    ss_copy.start()

    srow = pl.ds(pl.multiple_of(s * 32, 32), 32)
    for g, group in groups:
        for k in range(1, 4):
            fd = lax.rem(f + k, 4)
            for i, source in enumerate(group):
                remote(
                    source.at[srow, pl.ds(pl.multiple_of(fd * 128, 128), 128)],
                    ws.at[4 - k, srow, pl.ds((3 * g + i) * 128, 128)],
                    w1_s.at[g], w1_r.at[g], (z, x, fd, t),
                ).start()

    gl_copy = remote(rows, gl.at[t], g_s.at[0], g_r.at[0], partner)
    gl_copy.start()
    gl[t] = rows[...]
    vv[:, :, 128:256] = jnp.ones((16, 256, 128), BF16)

    @pl.when(side == 0)
    def _():
        kk[11] = jnp.zeros((256, 128), BF16)
        vv[11, :, 0:128] = jnp.zeros((256, 128), BF16)

    ss_copy.wait_recv()

    @pl.loop(0, 8)
    def _(b):
        block = pl.ds(pl.multiple_of(b * 32, 32), 32)
        total = jnp.sum(ss[0, block, :] + ss[1, block, :], axis=-1, keepdims=True)
        r = lax.rsqrt(total * (1.0 / FEATURES) + epsilon)
        v = tok[block, :].astype(F32) * r * gain[...]
        v = v.astype(BF16)
        xs[f, 2 * t, block, :] = v[:, 0:512]
        xs[f, 2 * t + 1, block, :] = v[:, 512:1024]

    sends = [gl_copy, ss_copy]

    def xref(e, half):
        return xs.at[lax.rem(f + e, 4), pl.ds(2 * t, 2), pl.ds(half * 128, 128), :]

    def xsend(e, half, target, send, recv):
        c = remote(xref(e, half), xref(e, half), send, recv, (z, x, target, t))
        c.start()
        sends.append(c)

    def xpair(e, half):
        c = remote(xref(e, half), xref(e, half), p_s.at[e, half], p_r.at[e, half], partner)
        c.start()
        sends.append(c)

    xsend(0, 0, up, x_s.at[0, 0], x_r.at[0, 0])
    xsend(0, 1, down, x_s.at[1, 1], x_r.at[1, 1])
    xsend(0, 1, up, x_s.at[0, 1], x_r.at[0, 1])
    xsend(0, 0, down, x_s.at[1, 0], x_r.at[1, 0])
    xpair(0, 0)
    xpair(0, 1)

    def place(g, c1, c2):
        return (c2, c1) if g == 0 else (c1, c2)

    def coords(g):
        return (x, z) if g == 0 else (z, x)

    def share(g, e1, e2, half=None):
        c1, c2 = coords(g)
        pz, px = place(g, lax.rem(c1 + e1, 4), lax.rem(c2 + e2, 4))
        start = (pz * 4 + px) * 32
        if half is None:
            return ws.at[pl.ds(1, 3), pl.ds(pl.multiple_of(start, 32), 32), pl.ds(g * 384, 384)]
        return ws.at[pl.ds(1, 3), pl.ds(pl.multiple_of(start + half * 16, 16), 16), pl.ds(g * 384, 384)]

    def wsend(g, ref, d1, d2, send, recv):
        c1, c2 = coords(g)
        pz, px = place(g, lax.rem(c1 + d1, 4), lax.rem(c2 + d2, 4))
        c = remote(ref, ref, send, recv, (pz, px, f, t))
        c.start()
        sends.append(c)

    step = (1, 3)
    origin = (3, 1)

    def second(g, j):
        for d in range(2):
            wsend(g, share(g, j, 0), 0, step[d], s2_s.at[g, j, d], s2_r.at[g, j, d])

    def second_forward(g, j):
        for d in range(2):
            arrival(share(g, j, origin[d]), s2_r.at[g, j, d])
            wsend(g, share(g, j, origin[d], d), 0, step[d], s2f_s.at[g, j, d], s2f_r.at[g, j, d])

    for g in range(2):
        arrival(share(g, 0, 0), w1_r.at[g])
        for d in range(2):
            wsend(g, share(g, 0, 0), step[d], 0, s1_s.at[g, d], s1_r.at[g, d])
        second(g, 0)
    for g in range(2):
        for d in range(2):
            arrival(share(g, origin[d], 0), s1_r.at[g, d])
            wsend(g, share(g, origin[d], 0, d), step[d], 0, s1f_s.at[g, d], s1f_r.at[g, d])
            second(g, origin[d])
    for g in range(2):
        second_forward(g, 0)

    arrival(xref(3, 0), x_r.at[0, 0])
    xsend(3, 0, up, xf_s.at[0], xf_r.at[0])
    xpair(3, 0)
    arrival(xref(1, 1), x_r.at[1, 1])
    xsend(1, 1, down, xf_s.at[1], xf_r.at[1])
    xpair(1, 1)

    for g in range(2):
        for d in range(2):
            arrival(share(g, 2, 0, d), s1f_r.at[g, d])
        second(g, 2)
    for j in (3, 1):
        for g in range(2):
            second_forward(g, j)
    arrival(xref(3, 1), x_r.at[0, 1])
    xpair(3, 1)
    arrival(xref(1, 0), x_r.at[1, 0])
    xpair(1, 0)
    for g in range(2):
        second_forward(g, 2)
    for j in (0, 3, 1, 2):
        for g in range(2):
            for d in range(2):
                arrival(share(g, j, 2, d), s2f_r.at[g, j, d])
    for g in range(2):
        arrival(ws.at[0, :, pl.ds(g * 384, 384)], loc.at[1 + g])

    def arrived_from_partner(e, half):
        q = lax.rem(f + e, 4)
        arrival(xs.at[q, pl.ds(2 * (1 - t), 2), pl.ds(half * 128, 128), :], p_r.at[e, half])

    for half, target in ((0, up), (1, down)):
        arrival(xref(2, half), xf_r.at[half])
        xpair(2, half)
    for e in range(4):
        for half in range(2):
            arrived_from_partner(e, half)

    late = jnp.where(s >= 11, 1, 0)

    def owner(q, u, c):
        return (lax.rem(q + u, 4), u, f, c)

    def att_copies(q):
        my_sequence = q == lax.rem(z + 4 - x, 4)
        found = []
        for h in (1, 0):
            u = 2 * t + h
            for c in range(2):
                target = kk.at[s] if c == 0 else vv.at[s, :, pl.ds(0, 128)]
                copy = remote(qkv.at[q, 1 + c], target, a_s.at[q, 2 * c + h], kv_r.at[s], owner(q, u, c))
                elsewhere = jnp.logical_not(my_sequence & (x == u) & (t == c))
                found.append((copy, elsewhere if h == 1 else elsewhere & (s <= 10)))
        u = 2 * t + late
        for c in range(2):
            copy = remote(
                qkv.at[q, 0, pl.ds(c * 128, 128), :], qb.at[s], q_s.at[q, c], q_r.at[s], owner(q, u, c)
            )
            found.append((copy, jnp.logical_not(my_sequence & (x == u) & (t == c))))
        return found

    decay = jnp.full((1, 128), decay_rate[f], F32)
    place_rows = lax.broadcasted_iota(jnp.int32, (256, 128), 0).astype(F32)
    key_decay = jnp.exp(-decay * (255.0 - place_rows))

    @pl.loop(0, 4)
    def _(k):
        q = lax.rem(z + x + k, 4)
        features = jnp.concatenate([xs[q, lax.rem(f + d, 4)] for d in range(4)], axis=1)
        total = jnp.dot(features, ws[...].reshape(FEATURES, 768), preferred_element_type=F32).astype(BF16)
        for i in range(6):
            qkv[q, i] = total[:, i * 128 : (i + 1) * 128]

        for copy, condition in att_copies(q):
            @pl.when(condition)
            def _():
                copy.start()

        kept = (q == lax.rem(z + 4 - x, 4)) & (high == t)

        @pl.when(kept & ((side == 1) | (s <= 10)))
        def _():
            @pl.when(t == 0)
            def _():
                kk[s] = qkv[q, 1]

            @pl.when(t == 1)
            def _():
                vv[s, :, 0:128] = qkv[q, 2]

        @pl.when(kept & (side == late))
        def _():
            qb[s] = qkv[q, 0, pl.ds(pl.multiple_of(t * 128, 128), 128), :]

        decayed = (qkv[q, 4].astype(F32) * key_decay).astype(BF16)
        stat[pl.ds(pl.multiple_of(q * 128, 128), 128), :] = tn_dot(decayed, qkv[q, 5]).astype(BF16)

    def st_copy(i):
        return remote(
            stat.at[pl.ds(pl.multiple_of(i * 32, 32), 32), :], rs.at[s], st_s.at[i], st_r.at[s],
            (i // 4, lax.rem(i, 4), f, t),
        )

    def pt_copy(i):
        return remote(
            ps.at[i], sin.at[pl.ds(pl.multiple_of(s * 32, 32), 32), :], pt_s.at[i], pt_r.at[s],
            (i // 4, lax.rem(i, 4), f, t),
        )

    @pl.loop(0, 16)
    def _(i):
        @pl.when(i != s)
        def _():
            st_copy(i).start()

    rs[s] = stat[srow, :]

    decay_square = jnp.broadcast_to(decay[:, 0:1], (256, 256))
    apart = (
        lax.broadcasted_iota(jnp.int32, (256, 256), 0) - lax.broadcasted_iota(jnp.int32, (256, 256), 1)
    ).astype(F32)
    within = jnp.where(apart >= 0, jnp.exp(-decay_square * jnp.maximum(apart, 0.0)), 0.0)

    @pl.loop(0, 4)
    def _(q):
        scores = nt_dot(qkv[q, 3], qkv[q, 4]) * within
        uu[q] = jnp.dot(scores.astype(BF16), qkv[q, 5], preferred_element_type=F32)

    sequence = lax.rem(z + 4 - x, 4)
    head = 4 * high + f
    key_blocks = 11 + 5 * side
    first_block = 11 * side
    kv_buffers = (lambda i: kk.at[i], lambda i: vv.at[i, :, pl.ds(0, 128)])

    def forward_copy(c, i):
        return remote(kv_buffers[c](i), kv_buffers[c](i), f_s.at[i], f_r.at[i], partner)

    for c in range(2):
        @pl.when(t == c)
        def _():
            @pl.loop(0, key_blocks)
            def _(i):
                @pl.when(jnp.logical_not((i == s) & (high == t)))
                def _():
                    arrival(kv_buffers[c](i), kv_r.at[i])
                forward_copy(c, i).start()

    arrival(gl.at[1 - t], g_r.at[0])

    @pl.loop(first_block, key_blocks)
    def _(i):
        @pl.when(jnp.logical_not((i == s) & (high == t)))
        def _():
            arrival(qb.at[i], q_r.at[i])

    @pl.loop(0, key_blocks)
    def _(i):
        arrival(qb.at[pl.ds(0, 2)], f_r.at[i])

    lam = gl[high, pl.ds(1, 1), :]
    att_gain = gl[high, pl.ds(0, 1), :] * branch_scale
    lane = lax.broadcasted_iota(jnp.int32, (128, 128), 1)
    join_cols = pl.ds(pl.multiple_of(head * 128, 128), 128)

    def att_out(i):
        return remote(
            ob.at[i], join.at[:, join_cols], ja_s.at[i], j_r.at[head], (i // 4, lax.rem(i, 4), sequence, t)
        )

    def att_self(i):
        return (i == s) & (sequence == f)

    def attention(first, count, m, height):
        for b in range(count):
            query = qb[first + b].astype(F32) * 0.125
            qs[b * 256 : b * 256 + 128] = jnp.where(lane < 64, query, 0.0).astype(BF16)
            qs[b * 256 + 128 : b * 256 + 256] = jnp.where(lane >= 64, query, 0.0).astype(BF16)
        keys = kk[0 : 2 * m + 2].reshape(512 * m + 512, 128)
        values = vv[0 : 2 * m + 2].reshape(512 * m + 512, 256)
        for b in range(256 * count // height):
            span = slice(b * height, b * height + height)
            scores = nt_dot(qs[span], keys)
            row = lax.broadcasted_iota(jnp.int32, (height, 512), 0) + b * height
            row = lax.rem(row, 128) + 256 * (row // 256) + (128 * t + 256 * (first - 2 * m))
            column = lax.broadcasted_iota(jnp.int32, (height, 512), 1)
            last = jnp.where(column <= row, scores[:, 512 * m :], masked_score)
            scores = jnp.concatenate([scores[:, : 512 * m], last], axis=1) if m else last
            weights = jnp.exp(scores - jnp.max(scores, axis=-1, keepdims=True))
            sums[span] = jnp.dot(weights.astype(BF16), values, preferred_element_type=F32)
        for b in range(count):
            i = first + b
            averaged = sums[b * 256 : b * 256 + 256, 0:128] / sums[b * 256 : b * 256 + 256, 128:256]
            differ = averaged[0:128] - lam * averaged[128:256]
            normed = differ * lax.rsqrt(jnp.mean(differ * differ, axis=-1, keepdims=True) + epsilon)
            result = (normed * att_gain).astype(BF16)
            ob[i] = result

            @pl.when(jnp.logical_not(att_self(i)))
            def _():
                att_out(i).start()

            @pl.when(att_self(i))
            def _():
                join[:, join_cols] = result

    attention(10 + side, 1, 5, 128)

    @pl.loop(0, 16)
    def _(i):
        @pl.when(i != s)
        def _():
            arrival(rs.at[i], st_r.at[i])

    block_decay = jnp.exp(-decay * 256.0)
    carry = jnp.zeros((32, 128), F32)
    for i in range(16):
        ps[i] = carry.astype(BF16)
        if i < 15:
            carry = carry * block_decay + rs[i].astype(F32)

    @pl.loop(0, 16)
    def _(i):
        @pl.when(i != s)
        def _():
            pt_copy(i).start()

    sin[srow, :] = ps[s]

    @pl.when(side == 0)
    def _():
        for m in range(5):
            attention(2 * m, 2, m, 256)

    @pl.when(side == 1)
    def _():
        for m in (6, 7):
            attention(2 * m, 2, m, 256)

    @pl.loop(0, 16)
    def _(i):
        @pl.when(i != s)
        def _():
            arrival(sin.at[pl.ds(pl.multiple_of(i * 32, 32), 32), :], pt_r.at[i])

    ret_head = 8 + 4 * t + f
    ret_cols = pl.ds(pl.multiple_of(ret_head * 128, 128), 128)
    query_decay = jnp.exp(-decay * (place_rows + 1.0))
    ret_gain = rows[2:3, :]

    def ret_out(q, c):
        return remote(
            rb.at[q, pl.ds(c * 128, 128), :], join.at[:, ret_cols], jr_s.at[q, c], j_r.at[ret_head], (z, x, q, c)
        )

    def ret_self(q, c):
        return (q == f) & (t == c)

    @pl.loop(0, 4)
    def _(q):
        state = sin[pl.ds(pl.multiple_of(q * 128, 128), 128), :]
        u = uu[q] + jnp.dot(qkv[q, 3], state, preferred_element_type=F32) * query_decay
        normed = u * lax.rsqrt(jnp.mean(u * u, axis=-1, keepdims=True) + epsilon)
        rb[q] = (normed * ret_gain).astype(BF16)
        for c in range(2):
            @pl.when(jnp.logical_not(ret_self(q, c)))
            def _():
                ret_out(q, c).start()

            @pl.when(ret_self(q, c))
            def _():
                join[:, ret_cols] = rb[q, c * 128 : (c + 1) * 128, :]

    @pl.loop(0, 8)
    def _(h):
        @pl.when(jnp.logical_not((lax.rem(h, 4) == f) & (sequence == f) & (x == 2 * (h // 4) + late)))
        def _():
            arrival(ob.at[0], j_r.at[h])

        @pl.when(h != 4 * t + f)
        def _():
            arrival(ob.at[0], j_r.at[8 + h])

    for g in range(2):
        arrival(share(g, 0, 0), w1_s.at[g])
    for c in sends:
        c.wait_send()

    @pl.loop(0, 4)
    def _(q):
        for copy, condition in att_copies(q):
            @pl.when(condition)
            def _():
                copy.wait_send()
        for c in range(2):
            @pl.when(jnp.logical_not(ret_self(q, c)))
            def _():
                ret_out(q, c).wait_send()

    @pl.loop(0, 16)
    def _(i):
        @pl.when(i != s)
        def _():
            st_copy(i).wait_send()
            pt_copy(i).wait_send()

    @pl.loop(0, key_blocks)
    def _(i):
        remote(qb.at[pl.ds(0, 2)], qb.at[pl.ds(0, 2)], f_s.at[i], f_r.at[i], partner).wait_send()

    @pl.loop(first_block, key_blocks)
    def _(i):
        @pl.when(jnp.logical_not(att_self(i)))
        def _():
            att_out(i).wait_send()


def body(
    tokens, norm_gain, query_weight, key_weight, value_weight, state_query, state_key, state_value,
    map_lambda, diff_gain, decay_rate, state_gain, out_weight,
):
    hbm = pl.BlockSpec(memory_space=pltpu.HBM)
    vmem = pl.BlockSpec(memory_space=pltpu.VMEM)
    joined = pl.pallas_call(
        kernel,
        out_shape=jax.ShapeDtypeStruct((128, FEATURES), BF16),
        in_specs=[hbm] * 12,
        out_specs=vmem,
        scratch_shapes=[
            pltpu.SMEM((4,), F32),
            pltpu.SMEM((4,), F32),
            pltpu.VMEM((256, 1024), BF16),
            pltpu.VMEM((1, 1024), F32),
            pltpu.VMEM((8, 128), F32),
            pltpu.VMEM((2, 256, 128), F32),
            pltpu.VMEM((2, 8, 128), F32),
            pltpu.VMEM((4, 4, 256, 512), BF16),
            pltpu.VMEM((4, 512, 768), BF16),
            pltpu.VMEM((4, 6, 256, 128), BF16),
            pltpu.VMEM((16, 256, 128), BF16),
            pltpu.VMEM((16, 256, 256), BF16),
            pltpu.VMEM((16, 128, 128), BF16),
            pltpu.VMEM((512, 128), BF16),
            pltpu.VMEM((512, 256), F32),
            pltpu.VMEM((16, 128, 128), BF16),
            pltpu.VMEM((512, 128), BF16),
            pltpu.VMEM((16, 32, 128), BF16),
            pltpu.VMEM((16, 32, 128), BF16),
            pltpu.VMEM((512, 128), BF16),
            pltpu.VMEM((4, 256, 128), F32),
            pltpu.VMEM((4, 256, 128), BF16),
            DMA((8,)), DMA((2,)), DMA((2,)), DMA((2,)), DMA((2,)),
            DMA((2, 2)), DMA((2, 2)), DMA((2, 2)), DMA((2, 2)),
            DMA((2, 4, 2)), DMA((2, 4, 2)), DMA((2, 4, 2)), DMA((2, 4, 2)),
            DMA((2, 2)), DMA((2, 2)), DMA((2,)), DMA((2,)), DMA((4, 2)), DMA((4, 2)),
            DMA((4, 4)), DMA((4, 2)), DMA((16,)), DMA((16,)), DMA((16,)), DMA((16,)),
            DMA((16,)), DMA((16,)), DMA((16,)), DMA((16,)),
            DMA((16,)), DMA((4, 2)), DMA((16,)),
        ],
        compiler_params=pltpu.CompilerParams(
            collective_id=0, has_side_effects=True, vmem_limit_bytes=32 * 1024 * 1024
        ),
        cost_estimate=pl.CostEstimate(flops=40_000_000_000, bytes_accessed=8_000_000, transcendentals=8_000_000),
        name="layer",
    )(
        *(
            pltpu.with_memory_space_constraint(a, pltpu.HBM)
            for a in (
                tokens, norm_gain, diff_gain, state_gain, map_lambda, decay_rate,
                query_weight, key_weight, value_weight, state_query, state_key, state_value,
            )
        )
    )
    return jnp.dot(joined, out_weight, preferred_element_type=F32).astype(BF16)[None]


def solution(mesh):
    torus = Mesh(
        mesh.devices.reshape(4, 4, mesh.shape["fs"], mesh.shape["tp"]), ("sp_0", "sp_1", "fs", "tp")
    )
    return jax.shard_map(
        body,
        mesh=torus,
        in_specs=(
            P("fs", SP, "tp"), P(), P("fs", "tp"), P("fs", "tp"), P("fs", "tp"), P("fs", "tp"), P("fs", "tp"),
            P("fs", "tp"), P("tp"), P("tp"), P("tp"), P("tp"), P(),
        ),
        out_specs=P("fs", SP_TP, None),
        check_vma=False,
    )
```

```python
import jax
import jax.numpy as jnp
from jax import lax
from jax.experimental import pallas as pl
from jax.experimental.pallas import tpu as pltpu
from jax.sharding import Mesh
from jax.sharding import PartitionSpec as P

BF16 = jnp.bfloat16
F32 = jnp.float32
MESH = pl.DeviceIdType.MESH
SP = ("sp_0", "sp_1")
SP_TP = ("sp_0", "sp_1", "tp")
FEATURES = 2048
epsilon = 1e-05
branch_scale = 0.8
masked_score = -1e30

DMA = pltpu.SemaphoreType.DMA


def nt_dot(a, b):
    return lax.dot_general(a, b, (((1,), (1,)), ((), ())), preferred_element_type=F32)


def tn_dot(a, b):
    return lax.dot_general(a, b, (((0,), (0,)), ((), ())), preferred_element_type=F32)


def remote(src, dst, send, recv, device):
    return pltpu.make_async_remote_copy(
        src_ref=src, dst_ref=dst, send_sem=send, recv_sem=recv, device_id=device, device_id_type=MESH
    )


def arrival(ref, sem):
    pltpu.make_async_copy(ref, ref, sem).wait()


def kernel(
    tok_hbm, norm_gain, diff_gain, state_gain, lambda_hbm, decay_hbm, wq, wk, wv, sq, sk, sv, ow_hbm, out_hbm,
    map_lambda, decay_rate, tok, gain, rows, ss, gl, xs, ws, stage, qkv, kk, vv, qb, qs, sums, ob, join, ow, summed, rounded, stat, rs, ps, sin, uu, rb,
    loc, once, w1_r, s1_r, s1f_r, s2_r, x_r, xf_r, kv_r, j_r,
):
    (
        ss_s, ss_r, gl_s, gl_r, w1_s, w_s, x_s, p_s, a_s, q_s, f_s, st_s, pt_s, ja_s, jr_s,
        q_r, f_r, st_r, pt_r, jr_r, s2f_r, p_r, p2_r,
    ) = (once.at[i] for i in range(23))
    z, x, f, t = (lax.axis_index(a) for a in ("sp_0", "sp_1", "fs", "tp"))
    s = z * 4 + x
    partner = (z, x, f, 1 - t)
    up, down = lax.rem(f + 1, 4), lax.rem(f + 3, 4)
    side = lax.rem(z, 2)
    high = x // 2

    barrier = pltpu.get_barrier_semaphore()
    peers = [partner]
    for k in (1, 3):
        peers += [(z, lax.rem(x + k, 4), f, t), (lax.rem(z + k, 4), x, f, t)]
    for k in (1, 2, 3):
        peers.append((z, x, lax.rem(f + k, 4), t))
    for peer in peers:
        pl.semaphore_signal(barrier, inc=1, device_id=peer, device_id_type=MESH)

    tok_copy = pltpu.make_async_copy(tok_hbm.at[0], tok, loc.at[0])
    tok_copy.start()
    cols = pl.ds(pl.multiple_of(f * 128, 128), 128)
    small = [
        pltpu.make_async_copy(norm_gain.at[pl.ds(pl.multiple_of(t * 1024, 1024), 1024)], gain.at[0], loc.at[3]),
        pltpu.make_async_copy(diff_gain.at[cols], rows.at[0], loc.at[4]),
        pltpu.make_async_copy(state_gain.at[cols], rows.at[2], loc.at[5]),
        pltpu.make_async_copy(lambda_hbm, map_lambda, loc.at[6]),
        pltpu.make_async_copy(decay_hbm, decay_rate, loc.at[7]),
    ]
    for c in small:
        c.start()
    groups = tuple(enumerate(((wq, wk, wv), (sq, sk, sv))))
    srow = pl.ds(pl.multiple_of(s * 32, 32), 32)
    for g, group in groups:
        for k in range(1, 4):
            theirs = pl.ds(pl.multiple_of(lax.rem(f + k, 4) * 128, 128), 128)
            for i, source in enumerate(group):
                pltpu.make_async_copy(
                    source.at[srow, theirs], stage.at[k - 1, :, pl.ds((3 * g + i) * 128, 128)], loc.at[8 + g]
                ).start()
    for g, group in groups:
        for i, source in enumerate(group):
            pltpu.make_async_copy(
                source.at[:, cols], ws.at[0, :, pl.ds((3 * g + i) * 128, 128)], loc.at[1 + g]
            ).start()

    ow_copy = pltpu.make_async_copy(ow_hbm, ow, loc.at[10])
    ow_copy.start()

    tok_copy.wait()

    @pl.loop(0, 8)
    def _(b):
        block = pl.ds(pl.multiple_of(b * 32, 32), 32)
        v = tok[block, :].astype(F32)
        v = v * v
        total = v[:, 0:128]
        for k in range(1, 8):
            total = total + v[:, k * 128 : (k + 1) * 128]
        ss[0, block, :] = total

    for c in small:
        c.wait()
    rows[1] = jnp.full((128,), map_lambda[f], F32)

    pl.semaphore_wait(barrier, len(peers))

    ss_copy = remote(ss.at[0], ss.at[1], ss_s, ss_r, partner)
    ss_copy.start()

    for g in range(2):
        part = pl.ds(g * 384, 384)
        arrival(stage.at[:, :, part], loc.at[8 + g])
        for k in range(1, 4):
            c = remote(
                stage.at[k - 1, :, part], ws.at[4 - k, srow, part], w1_s, w1_r.at[g],
                (z, x, lax.rem(f + k, 4), t),
            )
            c.start()

    gl_copy = remote(rows, gl.at[t], gl_s, gl_r, partner)
    gl_copy.start()
    gl[t] = rows[...]

    ss_copy.wait_recv()

    @pl.loop(0, 8)
    def _(b):
        block = pl.ds(pl.multiple_of(b * 32, 32), 32)
        total = jnp.sum(ss[0, block, :] + ss[1, block, :], axis=-1, keepdims=True)
        r = lax.rsqrt(total * (1.0 / FEATURES) + epsilon)
        v = tok[block, :].astype(F32) * r * gain[...]
        v = v.astype(BF16)
        xs[f, 2 * t, block, :] = v[:, 0:512]
        xs[f, 2 * t + 1, block, :] = v[:, 512:1024]


    def xref(e, half):
        return xs.at[lax.rem(f + e, 4), pl.ds(2 * t, 2), pl.ds(half * 128, 128), :]

    def xsend(e, half, target, recv):
        remote(xref(e, half), xref(e, half), x_s, recv, (z, x, target, t)).start()

    def xpair(e, half):
        remote(xref(e, half), xref(e, half), p_s, p2_r if e == 2 else p_r, partner).start()

    xsend(0, 0, up, x_r.at[0, 0])
    xsend(0, 1, down, x_r.at[1, 1])
    xsend(0, 1, up, x_r.at[0, 1])
    xsend(0, 0, down, x_r.at[1, 0])
    xpair(0, 0)
    xpair(0, 1)

    vv[:, :, 128:256] = jnp.ones((16, 256, 128), BF16)

    @pl.when(side == 0)
    def _():
        kk[11] = jnp.zeros((256, 128), BF16)
        vv[11, :, 0:128] = jnp.zeros((256, 128), BF16)

    def place(g, c1, c2):
        return (c2, c1) if g == 0 else (c1, c2)

    def coords(g):
        return (x, z) if g == 0 else (z, x)

    def share(g, e1, e2, half=None):
        c1, c2 = coords(g)
        pz, px = place(g, lax.rem(c1 + e1, 4), lax.rem(c2 + e2, 4))
        start = (pz * 4 + px) * 32
        if half is None:
            return ws.at[pl.ds(1, 3), pl.ds(pl.multiple_of(start, 32), 32), pl.ds(g * 384, 384)]
        return ws.at[pl.ds(1, 3), pl.ds(pl.multiple_of(start + half * 16, 16), 16), pl.ds(g * 384, 384)]

    def wsend(g, ref, d1, d2, recv):
        c1, c2 = coords(g)
        pz, px = place(g, lax.rem(c1 + d1, 4), lax.rem(c2 + d2, 4))
        remote(ref, ref, w_s, recv, (pz, px, f, t)).start()

    step = (1, 3)
    origin = (3, 1)

    def second(g, j):
        for d in range(2):
            wsend(g, share(g, j, 0), 0, step[d], s2_r.at[g, j, d])

    def second_forward(g, j):
        for d in range(2):
            arrival(share(g, j, origin[d]), s2_r.at[g, j, d])
            wsend(g, share(g, j, origin[d], d), 0, step[d], s2f_r)

    for g in range(2):
        arrival(share(g, 0, 0), w1_r.at[g])
        for d in range(2):
            wsend(g, share(g, 0, 0), step[d], 0, s1_r.at[g, d])
        second(g, 0)
    for g in range(2):
        for d in range(2):
            arrival(share(g, origin[d], 0), s1_r.at[g, d])
            wsend(g, share(g, origin[d], 0, d), step[d], 0, s1f_r.at[g])
            second(g, origin[d])
    for g in range(2):
        second_forward(g, 0)

    arrival(xref(3, 0), x_r.at[0, 0])
    xsend(3, 0, up, xf_r.at[0])
    xpair(3, 0)
    arrival(xref(1, 1), x_r.at[1, 1])
    xsend(1, 1, down, xf_r.at[1])
    xpair(1, 1)

    for g in range(2):
        arrival(share(g, 2, 0), s1f_r.at[g])
        second(g, 2)
    for j in (3, 1):
        for g in range(2):
            second_forward(g, j)
    arrival(xref(3, 1), x_r.at[0, 1])
    xpair(3, 1)
    arrival(xref(1, 0), x_r.at[1, 0])
    xpair(1, 0)
    for g in range(2):
        second_forward(g, 2)
    arrival(ws.at[0, pl.ds(0, 384), :], s2f_r)
    for g in range(2):
        arrival(ws.at[0, :, pl.ds(g * 384, 384)], loc.at[1 + g])

    arrival(xs.at[pl.ds(0, 3), pl.ds(0, 2)], p_r)

    late = jnp.where(s >= 11, 1, 0)

    def column(q, h):
        return 2 * t + lax.rem(h + q, 2)

    def owner(q, h, c):
        return (lax.rem(q + column(q, h), 4), column(q, h), f, c)

    def att_copies(q):
        my_sequence = q == lax.rem(z + 4 - x, 4)
        found = []
        for h in (1, 0):
            u = column(q, h)
            for c in range(2):
                target = kk.at[s] if c == 0 else vv.at[s, :, pl.ds(0, 128)]
                copy = remote(qkv.at[q, 1 + c], target, a_s, kv_r.at[s], owner(q, h, c))
                elsewhere = jnp.logical_not(my_sequence & (x == u) & (t == c))
                found.append((copy, elsewhere if h == 1 else elsewhere & (s <= 10), h))
        u = column(q, late)
        for c in range(2):
            copy = remote(
                qkv.at[q, 0, pl.ds(c * 128, 128), :], qb.at[s], q_s, q_r, owner(q, late, c)
            )
            found.append((copy, jnp.logical_not(my_sequence & (x == u) & (t == c)), 2))
        return found

    decay = jnp.full((1, 128), decay_rate[f], F32)
    place_rows = lax.broadcasted_iota(jnp.int32, (256, 128), 0).astype(F32)
    key_decay = jnp.exp(-decay * (255.0 - place_rows))

    def project(q, group):
        features = jnp.concatenate([xs[q, lax.rem(f + d, 4)] for d in range(4)], axis=1)
        weights = ws[:, :, group * 384 : group * 384 + 384].reshape(FEATURES, 384)
        total = jnp.dot(features, weights, preferred_element_type=F32).astype(BF16)
        for i in range(3):
            qkv[q, 3 * group + i] = total[:, i * 128 : (i + 1) * 128]

    turn = lax.rem(z + x, 3)

    @pl.loop(0, 4)
    def _(k):
        near = lax.rem(k + turn, 3)
        e = (near + near // 2) * (1 - k // 3) + 2 * (k // 3)
        q = lax.rem(f + e, 4)

        @pl.when(k == 3)
        def _():
            for half in range(2):
                arrival(xref(2, half), xf_r.at[half])
                xpair(2, half)
            arrival(xs.at[0, pl.ds(0, 2)], p2_r)

        project(q, 0)
        for copy, condition, kind in att_copies(q):
            @pl.when(condition if kind else condition & ((k == 0) | (k == 3)))
            def _():
                copy.start()

        kept = (q == lax.rem(z + 4 - x, 4)) & (high == t)

        @pl.when(kept & ((side == 1) | (s <= 10)))
        def _():
            @pl.when(t == 0)
            def _():
                kk[s] = qkv[q, 1]

            @pl.when(t == 1)
            def _():
                vv[s, :, 0:128] = qkv[q, 2]

        @pl.when(kept & (side == late))
        def _():
            qb[s] = qkv[q, 0, pl.ds(pl.multiple_of(t * 128, 128), 128), :]

    @pl.loop(1, 3)
    def _(k):
        near = lax.rem(k + turn, 3)
        for copy, condition, kind in att_copies(lax.rem(f + near + near // 2, 4)):
            if kind == 0:
                @pl.when(condition)
                def _():
                    copy.start()

    @pl.loop(0, 4)
    def _(q):
        project(q, 1)
        decayed = (qkv[q, 4].astype(F32) * key_decay).astype(BF16)
        stat[pl.ds(pl.multiple_of(q * 128, 128), 128), :] = tn_dot(decayed, qkv[q, 5]).astype(BF16)

    def st_copy(i):
        return remote(
            stat.at[pl.ds(pl.multiple_of(i * 32, 32), 32), :], rs.at[s], st_s, st_r,
            (i // 4, lax.rem(i, 4), f, t),
        )

    def pt_copy(i):
        return remote(
            ps.at[i], sin.at[pl.ds(pl.multiple_of(s * 32, 32), 32), :], pt_s, pt_r,
            (i // 4, lax.rem(i, 4), f, t),
        )

    @pl.loop(0, 16)
    def _(i):
        @pl.when(i != s)
        def _():
            st_copy(i).start()

    rs[s] = stat[srow, :]

    decay_square = jnp.broadcast_to(decay[:, 0:1], (256, 256))
    apart = (
        lax.broadcasted_iota(jnp.int32, (256, 256), 0) - lax.broadcasted_iota(jnp.int32, (256, 256), 1)
    ).astype(F32)
    within = jnp.where(apart >= 0, jnp.exp(-decay_square * jnp.maximum(apart, 0.0)), 0.0)

    @pl.loop(0, 4)
    def _(q):
        scores = nt_dot(qkv[q, 3], qkv[q, 4]) * within
        uu[q] = jnp.dot(scores.astype(BF16), qkv[q, 5], preferred_element_type=F32)

    sequence = lax.rem(z + 4 - x, 4)
    head = 4 * high + f
    key_blocks = 11 + 5 * side
    first_block = 11 * side
    kv_buffers = (lambda i: kk.at[i], lambda i: vv.at[i, :, pl.ds(0, 128)])

    def forward_copy(c, i):
        return remote(kv_buffers[c](i), kv_buffers[c](i), f_s, f_r, partner)

    for c in range(2):
        @pl.when(t == c)
        def _():
            @pl.loop(0, key_blocks)
            def _(i):
                @pl.when(jnp.logical_not((i == s) & (high == t)))
                def _():
                    arrival(kv_buffers[c](i), kv_r.at[i])
                forward_copy(c, i).start()

    arrival(gl.at[1 - t], gl_r)

    def one_if(condition):
        return jnp.where(condition, 1, 0)

    def counted(ref, sem, n, *values):
        for k in values:
            @pl.when(n == k)
            def _():
                arrival(ref.at[pl.ds(0, k)], sem)

    queries = 11 - 6 * side
    counted(qb, q_r, queries - one_if((high == t) & (side == late)), 11, 10, 5, 4)
    counted(kk, f_r, key_blocks, 11, 16)

    lam = gl[high, pl.ds(1, 1), :]
    att_gain = gl[high, pl.ds(0, 1), :] * branch_scale
    lane = lax.broadcasted_iota(jnp.int32, (128, 128), 1)
    join_cols = pl.ds(pl.multiple_of(head * 128, 128), 128)

    def att_out(i):
        return remote(
            ob.at[i], join.at[:, join_cols], ja_s, j_r.at[head], (i // 4, lax.rem(i, 4), sequence, t)
        )

    def att_self(i):
        return (i == s) & (sequence == f)

    def attention(first, count, m, height):
        for b in range(count):
            query = qb[first + b].astype(F32) * 0.125
            qs[b * 256 : b * 256 + 128] = jnp.where(lane < 64, query, 0.0).astype(BF16)
            qs[b * 256 + 128 : b * 256 + 256] = jnp.where(lane >= 64, query, 0.0).astype(BF16)
        keys = kk[0 : 2 * m + 2].reshape(512 * m + 512, 128)
        values = vv[0 : 2 * m + 2].reshape(512 * m + 512, 256)
        for b in range(256 * count // height):
            span = slice(b * height, b * height + height)
            scores = nt_dot(qs[span], keys)
            row = lax.broadcasted_iota(jnp.int32, (height, 512), 0) + b * height
            row = lax.rem(row, 128) + 256 * (row // 256) + (128 * t + 256 * (first - 2 * m))
            column = lax.broadcasted_iota(jnp.int32, (height, 512), 1)
            last = jnp.where(column <= row, scores[:, 512 * m :], masked_score)
            scores = jnp.concatenate([scores[:, : 512 * m], last], axis=1) if m else last
            weights = jnp.exp(scores - jnp.max(scores, axis=-1, keepdims=True))
            sums[span] = jnp.dot(weights.astype(BF16), values, preferred_element_type=F32)
        for b in range(count):
            i = first + b
            averaged = sums[b * 256 : b * 256 + 256, 0:128] / sums[b * 256 : b * 256 + 256, 128:256]
            differ = averaged[0:128] - lam * averaged[128:256]
            normed = differ * lax.rsqrt(jnp.mean(differ * differ, axis=-1, keepdims=True) + epsilon)
            result = (normed * att_gain).astype(BF16)
            ob[i] = result

            @pl.when(jnp.logical_not(att_self(i)))
            def _():
                att_out(i).start()

            @pl.when(att_self(i))
            def _():
                join[:, join_cols] = result

    attention(10 + side, 1, 5, 128)

    arrival(rs.at[pl.ds(0, 15)], st_r)

    block_decay = jnp.exp(-decay * 256.0)
    carry = jnp.zeros((32, 128), F32)
    for i in range(16):
        ps[i] = carry.astype(BF16)
        if i < 15:
            carry = carry * block_decay + rs[i].astype(F32)

    @pl.loop(0, 16)
    def _(i):
        @pl.when(i != s)
        def _():
            pt_copy(i).start()

    sin[srow, :] = ps[s]

    @pl.when(side == 0)
    def _():
        for m in range(5):
            attention(2 * m, 2, m, 256)

    @pl.when(side == 1)
    def _():
        for m in (6, 7):
            attention(2 * m, 2, m, 256)

    arrival(sin.at[pl.ds(0, 480), :], pt_r)

    ret_head = 8 + 4 * t + f
    ret_cols = pl.ds(pl.multiple_of(ret_head * 128, 128), 128)
    query_decay = jnp.exp(-decay * (place_rows + 1.0))
    ret_gain = rows[2:3, :]

    def ret_out(q, c):
        return remote(
            rb.at[q, pl.ds(c * 128, 128), :], join.at[:, ret_cols], jr_s, jr_r, (z, x, q, c)
        )

    def ret_self(q, c):
        return (q == f) & (t == c)

    @pl.loop(0, 4)
    def _(q):
        state = sin[pl.ds(pl.multiple_of(q * 128, 128), 128), :]
        u = uu[q] + jnp.dot(qkv[q, 3], state, preferred_element_type=F32) * query_decay
        normed = u * lax.rsqrt(jnp.mean(u * u, axis=-1, keepdims=True) + epsilon)
        rb[q] = (normed * ret_gain).astype(BF16)
        for c in range(2):
            @pl.when(jnp.logical_not(ret_self(q, c)))
            def _():
                ret_out(q, c).start()

            @pl.when(ret_self(q, c))
            def _():
                join[:, ret_cols] = rb[q, c * 128 : (c + 1) * 128, :]

    gl_copy.wait_send()
    ss_copy.wait_send()
    arrival(stage, w1_s)
    arrival(ws.at[pl.ds(0, 3), pl.ds(0, 480), :], w_s)
    arrival(xs.at[pl.ds(0, 3), pl.ds(0, 2)], x_s)
    arrival(xs.at[pl.ds(0, 2)], p_s)
    arrival(rs.at[pl.ds(0, 15)], st_s)
    arrival(ps.at[pl.ds(0, 15)], pt_s)
    kept_kv = one_if((high == t) & ((side == 1) | (s <= 10)))
    counted(kk, a_s, 16 - 8 * late - kept_kv, 16, 15, 8, 7)
    counted(qb, q_s, 8 - one_if((high == t) & (side == late)), 8, 7)
    counted(kk, f_s, key_blocks, 11, 16)

    ow_copy.wait()
    for h in (0, 2, 4, 6):
        for k in (h, h + 1):
            @pl.when(jnp.logical_not((k % 4 == f) & (sequence == f) & (high == k // 4) & (side == late)))
            def _():
                arrival(ob.at[0], j_r.at[k])

        heads = slice(h * 128, h * 128 + 256)
        piece = jnp.dot(join[:, heads], ow[heads, :], preferred_element_type=F32)
        if h == 0:
            summed[...] = piece
        else:
            summed[...] += piece

    arrival(qb.at[pl.ds(0, 7)], jr_r)
    for n in range(4):
        span = slice(n * 512, n * 512 + 512)
        piece = jnp.dot(join[:, 1024:], ow[1024:, span], preferred_element_type=F32)
        rounded[:, span] = (summed[:, span] + piece).astype(BF16)
    out_copy = pltpu.make_async_copy(rounded, out_hbm, loc.at[11])
    out_copy.start()

    counted(ob, ja_s, queries - one_if((sequence == f) & (side == late)), 11, 10, 5, 4)
    arrival(qb.at[pl.ds(0, 7)], jr_s)
    out_copy.wait()


def body(
    tokens, norm_gain, query_weight, key_weight, value_weight, state_query, state_key, state_value,
    map_lambda, diff_gain, decay_rate, state_gain, out_weight,
):
    hbm = pl.BlockSpec(memory_space=pltpu.HBM)
    out = pl.pallas_call(
        kernel,
        out_shape=jax.ShapeDtypeStruct((128, FEATURES), BF16),
        in_specs=[hbm] * 13,
        out_specs=hbm,
        scratch_shapes=[
            pltpu.SMEM((4,), F32),
            pltpu.SMEM((4,), F32),
            pltpu.VMEM((256, 1024), BF16),
            pltpu.VMEM((1, 1024), F32),
            pltpu.VMEM((8, 128), F32),
            pltpu.VMEM((2, 256, 128), F32),
            pltpu.VMEM((2, 8, 128), F32),
            pltpu.VMEM((4, 4, 256, 512), BF16),
            pltpu.VMEM((4, 512, 768), BF16),
            pltpu.VMEM((3, 32, 768), BF16),
            pltpu.VMEM((4, 6, 256, 128), BF16),
            pltpu.VMEM((16, 256, 128), BF16),
            pltpu.VMEM((16, 256, 256), BF16),
            pltpu.VMEM((16, 128, 128), BF16),
            pltpu.VMEM((512, 128), BF16),
            pltpu.VMEM((512, 256), F32),
            pltpu.VMEM((16, 128, 128), BF16),
            pltpu.VMEM((128, FEATURES), BF16),
            pltpu.VMEM((FEATURES, FEATURES), BF16),
            pltpu.VMEM((128, FEATURES), F32),
            pltpu.VMEM((128, FEATURES), BF16),
            pltpu.VMEM((512, 128), BF16),
            pltpu.VMEM((16, 32, 128), BF16),
            pltpu.VMEM((16, 32, 128), BF16),
            pltpu.VMEM((512, 128), BF16),
            pltpu.VMEM((4, 256, 128), F32),
            pltpu.VMEM((4, 256, 128), BF16),
            DMA((12,)), DMA((23,)), DMA((2,)), DMA((2, 2)), DMA((2,)), DMA((2, 4, 2)),
            DMA((2, 2)), DMA((2,)), DMA((16,)), DMA((8,)),
        ],
        compiler_params=pltpu.CompilerParams(
            collective_id=0, has_side_effects=True, vmem_limit_bytes=48 * 1024 * 1024
        ),
        cost_estimate=pl.CostEstimate(flops=40_000_000_000, bytes_accessed=8_000_000, transcendentals=8_000_000),
        name="layer",
    )(
        *(
            pltpu.with_memory_space_constraint(a, pltpu.HBM)
            for a in (
                tokens, norm_gain, diff_gain, state_gain, map_lambda, decay_rate,
                query_weight, key_weight, value_weight, state_query, state_key, state_value, out_weight,
            )
        )
    )
    return out[None]


def solution(mesh):
    torus = Mesh(
        mesh.devices.reshape(4, 4, mesh.shape["fs"], mesh.shape["tp"]), ("sp_0", "sp_1", "fs", "tp")
    )
    return jax.shard_map(
        body,
        mesh=torus,
        in_specs=(
            P("fs", SP, "tp"), P(), P("fs", "tp"), P("fs", "tp"), P("fs", "tp"), P("fs", "tp"), P("fs", "tp"),
            P("fs", "tp"), P("tp"), P("tp"), P("tp"), P("tp"), P(),
        ),
        out_specs=P("fs", SP_TP, None),
        check_vma=False,
    )
```

```python
import jax
import jax.numpy as jnp
from jax import lax
from jax.experimental import pallas as pl
from jax.experimental.pallas import tpu as pltpu
from jax.sharding import Mesh
from jax.sharding import PartitionSpec as P

BF16 = jnp.bfloat16
F32 = jnp.float32
MESH = pl.DeviceIdType.MESH
SP = ("sp_0", "sp_1")
SP_TP = ("sp_0", "sp_1", "tp")
FEATURES = 2048
epsilon = 1e-05
branch_scale = 0.8
masked_score = -1e30

DMA = pltpu.SemaphoreType.DMA


def nt_dot(a, b):
    return lax.dot_general(a, b, (((1,), (1,)), ((), ())), preferred_element_type=F32)


def tn_dot(a, b):
    return lax.dot_general(a, b, (((0,), (0,)), ((), ())), preferred_element_type=F32)


def remote(src, dst, send, recv, device):
    return pltpu.make_async_remote_copy(
        src_ref=src, dst_ref=dst, send_sem=send, recv_sem=recv, device_id=device, device_id_type=MESH
    )


def arrival(ref, sem):
    pltpu.make_async_copy(ref, ref, sem).wait()


def kernel(
    tok_hbm, norm_gain, diff_gain, state_gain, lambda_hbm, decay_hbm, wq, wk, wv, sq, sk, sv, ow_hbm, out_hbm,
    map_lambda, decay_rate, tok, gain, rows, ss, gl, xs, ws, stage, qkv, kk, vv, qb, qs, sums, ob, join, ow, summed, rounded, stat, rs, ps, sin, uu, rb,
    loc, once, w1_r, s1_r, s1f_r, s2_r, x_r, xf_r, kv_r, j_r,
):
    (
        ss_s, ss_r, gl_s, gl_r, w1_s, w_s, x_s, p_s, a_s, q_s, f_s, st_s, pt_s, ja_s, jr_s,
        q_r, f_r, st_r, pt_r, jr_r, s2f_r, p_r, p2_r,
    ) = (once.at[i] for i in range(23))
    z, x, f, t = (lax.axis_index(a) for a in ("sp_0", "sp_1", "fs", "tp"))
    s = z * 4 + x
    partner = (z, x, f, 1 - t)
    up, down = lax.rem(f + 1, 4), lax.rem(f + 3, 4)
    side = lax.rem(z, 2)
    high = x // 2

    barrier = pltpu.get_barrier_semaphore()
    peers = [partner]
    for k in (1, 3):
        peers += [(z, lax.rem(x + k, 4), f, t), (lax.rem(z + k, 4), x, f, t)]
    for k in (1, 2, 3):
        peers.append((z, x, lax.rem(f + k, 4), t))
    for peer in peers:
        pl.semaphore_signal(barrier, inc=1, device_id=peer, device_id_type=MESH)

    tok_copy = pltpu.make_async_copy(tok_hbm.at[0], tok, loc.at[0])
    tok_copy.start()
    cols = pl.ds(pl.multiple_of(f * 128, 128), 128)
    small = [
        pltpu.make_async_copy(norm_gain.at[pl.ds(pl.multiple_of(t * 1024, 1024), 1024)], gain.at[0], loc.at[3]),
        pltpu.make_async_copy(diff_gain.at[cols], rows.at[0], loc.at[4]),
        pltpu.make_async_copy(state_gain.at[cols], rows.at[2], loc.at[5]),
        pltpu.make_async_copy(lambda_hbm, map_lambda, loc.at[6]),
        pltpu.make_async_copy(decay_hbm, decay_rate, loc.at[7]),
    ]
    for c in small:
        c.start()
    groups = tuple(enumerate(((wq, wk, wv), (sq, sk, sv))))
    srow = pl.ds(pl.multiple_of(s * 32, 32), 32)
    for g, group in groups:
        for k in range(1, 4):
            theirs = pl.ds(pl.multiple_of(lax.rem(f + k, 4) * 128, 128), 128)
            for i, source in enumerate(group):
                pltpu.make_async_copy(
                    source.at[srow, theirs], stage.at[k - 1, :, pl.ds((3 * g + i) * 128, 128)], loc.at[8 + g]
                ).start()
    for g, group in groups:
        for i, source in enumerate(group):
            pltpu.make_async_copy(
                source.at[:, cols], ws.at[0, :, pl.ds((3 * g + i) * 128, 128)], loc.at[1 + g]
            ).start()

    ow_copy = pltpu.make_async_copy(ow_hbm, ow, loc.at[10])
    ow_copy.start()

    tok_copy.wait()

    @pl.loop(0, 8)
    def _(b):
        block = pl.ds(pl.multiple_of(b * 32, 32), 32)
        v = tok[block, :].astype(F32)
        v = v * v
        total = v[:, 0:128]
        for k in range(1, 8):
            total = total + v[:, k * 128 : (k + 1) * 128]
        ss[0, block, :] = total

    for c in small:
        c.wait()
    rows[1] = jnp.full((128,), map_lambda[f], F32)

    pl.semaphore_wait(barrier, len(peers))

    ss_copy = remote(ss.at[0], ss.at[1], ss_s, ss_r, partner)
    ss_copy.start()

    for g in range(2):
        part = pl.ds(g * 384, 384)
        arrival(stage.at[:, :, part], loc.at[8 + g])
        for k in range(1, 4):
            c = remote(
                stage.at[k - 1, :, part], ws.at[4 - k, srow, part], w1_s, w1_r.at[g],
                (z, x, lax.rem(f + k, 4), t),
            )
            c.start()

    gl_copy = remote(rows, gl.at[t], gl_s, gl_r, partner)
    gl_copy.start()
    gl[t] = rows[...]

    ss_copy.wait_recv()

    @pl.loop(0, 8)
    def _(b):
        block = pl.ds(pl.multiple_of(b * 32, 32), 32)
        total = jnp.sum(ss[0, block, :] + ss[1, block, :], axis=-1, keepdims=True)
        r = lax.rsqrt(total * (1.0 / FEATURES) + epsilon)
        v = tok[block, :].astype(F32) * r * gain[...]
        v = v.astype(BF16)
        xs[f, 2 * t, block, :] = v[:, 0:512]
        xs[f, 2 * t + 1, block, :] = v[:, 512:1024]


    def xref(e, half):
        return xs.at[lax.rem(f + e, 4), pl.ds(2 * t, 2), pl.ds(half * 128, 128), :]

    def xsend(e, half, target, recv):
        remote(xref(e, half), xref(e, half), x_s, recv, (z, x, target, t)).start()

    def xpair(e, half):
        remote(xref(e, half), xref(e, half), p_s, p2_r if e == 2 else p_r, partner).start()

    xsend(0, 0, up, x_r.at[0, 0])
    xsend(0, 1, down, x_r.at[1, 1])
    xsend(0, 1, up, x_r.at[0, 1])
    xsend(0, 0, down, x_r.at[1, 0])
    xpair(0, 0)
    xpair(0, 1)

    vv[:, :, 128:256] = jnp.ones((16, 256, 128), BF16)

    @pl.when(side == 0)
    def _():
        kk[11] = jnp.zeros((256, 128), BF16)
        vv[11, :, 0:128] = jnp.zeros((256, 128), BF16)

    def place(g, c1, c2):
        return (c2, c1) if g == 0 else (c1, c2)

    def coords(g):
        return (x, z) if g == 0 else (z, x)

    def share(g, e1, e2, half=None):
        c1, c2 = coords(g)
        pz, px = place(g, lax.rem(c1 + e1, 4), lax.rem(c2 + e2, 4))
        start = (pz * 4 + px) * 32
        if half is None:
            return ws.at[pl.ds(1, 3), pl.ds(pl.multiple_of(start, 32), 32), pl.ds(g * 384, 384)]
        return ws.at[pl.ds(1, 3), pl.ds(pl.multiple_of(start + half * 16, 16), 16), pl.ds(g * 384, 384)]

    def wsend(g, ref, d1, d2, recv):
        c1, c2 = coords(g)
        pz, px = place(g, lax.rem(c1 + d1, 4), lax.rem(c2 + d2, 4))
        remote(ref, ref, w_s, recv, (pz, px, f, t)).start()

    step = (1, 3)
    origin = (3, 1)

    def second(g, j):
        for d in range(2):
            wsend(g, share(g, j, 0), 0, step[d], s2_r.at[g, j, d])

    def second_forward(g, j):
        for d in range(2):
            arrival(share(g, j, origin[d]), s2_r.at[g, j, d])
            wsend(g, share(g, j, origin[d], d), 0, step[d], s2f_r)

    for g in range(2):
        arrival(share(g, 0, 0), w1_r.at[g])
        for d in range(2):
            wsend(g, share(g, 0, 0), step[d], 0, s1_r.at[g, d])
        second(g, 0)
    for g in range(2):
        for d in range(2):
            arrival(share(g, origin[d], 0), s1_r.at[g, d])
            wsend(g, share(g, origin[d], 0, d), step[d], 0, s1f_r.at[g])
            second(g, origin[d])
    for g in range(2):
        second_forward(g, 0)

    arrival(xref(3, 0), x_r.at[0, 0])
    xsend(3, 0, up, xf_r.at[0])
    xpair(3, 0)
    arrival(xref(1, 1), x_r.at[1, 1])
    xsend(1, 1, down, xf_r.at[1])
    xpair(1, 1)

    for g in range(2):
        arrival(share(g, 2, 0), s1f_r.at[g])
        second(g, 2)
    for j in (3, 1):
        for g in range(2):
            second_forward(g, j)
    for g in range(2):
        second_forward(g, 2)
    arrival(xref(3, 1), x_r.at[0, 1])
    xpair(3, 1)
    arrival(xref(1, 0), x_r.at[1, 0])
    xpair(1, 0)
    arrival(ws.at[0, pl.ds(0, 384), :], s2f_r)
    for g in range(2):
        arrival(ws.at[0, :, pl.ds(g * 384, 384)], loc.at[1 + g])

    arrival(xs.at[pl.ds(0, 3), pl.ds(0, 2)], p_r)

    late = jnp.where(s >= 11, 1, 0)

    def column(q, h):
        return 2 * t + lax.rem(h + q, 2)

    def owner(q, h, c):
        return (lax.rem(q + column(q, h), 4), column(q, h), f, c)

    def att_copies(q):
        my_sequence = q == lax.rem(z + 4 - x, 4)
        found = []
        for h in (1, 0):
            u = column(q, h)
            for c in range(2):
                target = kk.at[s] if c == 0 else vv.at[s, :, pl.ds(0, 128)]
                copy = remote(qkv.at[q, 1 + c], target, a_s, kv_r.at[s], owner(q, h, c))
                elsewhere = jnp.logical_not(my_sequence & (x == u) & (t == c))
                found.append((copy, elsewhere if h == 1 else elsewhere & (s <= 10), h))
        u = column(q, late)
        for c in range(2):
            copy = remote(
                qkv.at[q, 0, pl.ds(c * 128, 128), :], qb.at[s], q_s, q_r, owner(q, late, c)
            )
            found.append((copy, jnp.logical_not(my_sequence & (x == u) & (t == c)), 2))
        return found

    decay = jnp.full((1, 128), decay_rate[f], F32)
    place_rows = lax.broadcasted_iota(jnp.int32, (256, 128), 0).astype(F32)
    key_decay = jnp.exp(-decay * (255.0 - place_rows))

    def project(q, group):
        features = jnp.concatenate([xs[q, lax.rem(f + d, 4)] for d in range(4)], axis=1)
        weights = ws[:, :, group * 384 : group * 384 + 384].reshape(FEATURES, 384)
        total = jnp.dot(features, weights, preferred_element_type=F32).astype(BF16)
        for i in range(3):
            qkv[q, 3 * group + i] = total[:, i * 128 : (i + 1) * 128]

    turn = lax.rem(z + x, 3)

    @pl.loop(0, 4)
    def _(k):
        near = lax.rem(k + turn, 3)
        e = (near + near // 2) * (1 - k // 3) + 2 * (k // 3)
        q = lax.rem(f + e, 4)

        @pl.when(k == 3)
        def _():
            for half in range(2):
                arrival(xref(2, half), xf_r.at[half])
                xpair(2, half)
            arrival(xs.at[0, pl.ds(0, 2)], p2_r)

        project(q, 0)
        for copy, condition, kind in att_copies(q):
            @pl.when(condition if kind else condition & ((k == 0) | (k == 3)))
            def _():
                copy.start()

        kept = (q == lax.rem(z + 4 - x, 4)) & (high == t)

        @pl.when(kept & ((side == 1) | (s <= 10)))
        def _():
            @pl.when(t == 0)
            def _():
                kk[s] = qkv[q, 1]

            @pl.when(t == 1)
            def _():
                vv[s, :, 0:128] = qkv[q, 2]

        @pl.when(kept & (side == late))
        def _():
            qb[s] = qkv[q, 0, pl.ds(pl.multiple_of(t * 128, 128), 128), :]

    @pl.loop(1, 3)
    def _(k):
        near = lax.rem(k + turn, 3)
        for copy, condition, kind in att_copies(lax.rem(f + near + near // 2, 4)):
            if kind == 0:
                @pl.when(condition)
                def _():
                    copy.start()

    @pl.loop(0, 4)
    def _(q):
        project(q, 1)
        decayed = (qkv[q, 4].astype(F32) * key_decay).astype(BF16)
        stat[pl.ds(pl.multiple_of(q * 128, 128), 128), :] = tn_dot(decayed, qkv[q, 5]).astype(BF16)

    def st_copy(i):
        return remote(
            stat.at[pl.ds(pl.multiple_of(i * 32, 32), 32), :], rs.at[s], st_s, st_r,
            (i // 4, lax.rem(i, 4), f, t),
        )

    def pt_copy(i):
        return remote(
            ps.at[i], sin.at[pl.ds(pl.multiple_of(s * 32, 32), 32), :], pt_s, pt_r,
            (i // 4, lax.rem(i, 4), f, t),
        )

    @pl.loop(0, 16)
    def _(i):
        @pl.when(i != s)
        def _():
            st_copy(i).start()

    rs[s] = stat[srow, :]

    decay_square = jnp.broadcast_to(decay[:, 0:1], (256, 256))
    apart = (
        lax.broadcasted_iota(jnp.int32, (256, 256), 0) - lax.broadcasted_iota(jnp.int32, (256, 256), 1)
    ).astype(F32)
    within = jnp.where(apart >= 0, jnp.exp(-decay_square * jnp.maximum(apart, 0.0)), 0.0)

    @pl.loop(0, 4)
    def _(q):
        scores = nt_dot(qkv[q, 3], qkv[q, 4]) * within
        uu[q] = jnp.dot(scores.astype(BF16), qkv[q, 5], preferred_element_type=F32)

    sequence = lax.rem(z + 4 - x, 4)
    head = 4 * high + f
    key_blocks = 11 + 5 * side
    first_block = 11 * side
    kv_buffers = (lambda i: kk.at[i], lambda i: vv.at[i, :, pl.ds(0, 128)])

    def forward_copy(c, i):
        return remote(kv_buffers[c](i), kv_buffers[c](i), f_s, f_r, partner)

    for c in range(2):
        @pl.when(t == c)
        def _():
            @pl.loop(0, key_blocks)
            def _(i):
                @pl.when(jnp.logical_not((i == s) & (high == t)))
                def _():
                    arrival(kv_buffers[c](i), kv_r.at[i])
                forward_copy(c, i).start()

    arrival(gl.at[1 - t], gl_r)

    def one_if(condition):
        return jnp.where(condition, 1, 0)

    def counted(ref, sem, n, *values):
        for k in values:
            @pl.when(n == k)
            def _():
                arrival(ref.at[pl.ds(0, k)], sem)

    queries = 11 - 6 * side
    counted(qb, q_r, queries - one_if((high == t) & (side == late)), 11, 10, 5, 4)
    counted(kk, f_r, key_blocks, 11, 16)

    lam = gl[high, pl.ds(1, 1), :]
    att_gain = gl[high, pl.ds(0, 1), :] * branch_scale
    lane = lax.broadcasted_iota(jnp.int32, (128, 128), 1)
    join_cols = pl.ds(pl.multiple_of(head * 128, 128), 128)

    def att_out(i):
        return remote(
            ob.at[i], join.at[:, join_cols], ja_s, j_r.at[head], (i // 4, lax.rem(i, 4), sequence, t)
        )

    def att_self(i):
        return (i == s) & (sequence == f)

    def attention(first, count, m, height, parity):
        for b in range(count):
            query = qb[first + b].astype(F32) * 0.125
            qs[parity, b * 256 : b * 256 + 128] = jnp.where(lane < 64, query, 0.0).astype(BF16)
            qs[parity, b * 256 + 128 : b * 256 + 256] = jnp.where(lane >= 64, query, 0.0).astype(BF16)
        keys = kk[0 : 2 * m + 2].reshape(512 * m + 512, 128)
        values = vv[0 : 2 * m + 2].reshape(512 * m + 512, 256)
        for b in range(256 * count // height):
            span = slice(b * height, b * height + height)
            scores = nt_dot(qs[parity, span], keys)
            row = lax.broadcasted_iota(jnp.int32, (height, 512), 0) + b * height
            row = lax.rem(row, 128) + 256 * (row // 256) + (128 * t + 256 * (first - 2 * m))
            column = lax.broadcasted_iota(jnp.int32, (height, 512), 1)
            last = jnp.where(column <= row, scores[:, 512 * m :], masked_score)
            scores = jnp.concatenate([scores[:, : 512 * m], last], axis=1) if m else last
            weights = jnp.exp(scores - jnp.max(scores, axis=-1, keepdims=True))
            sums[parity, span] = jnp.dot(weights.astype(BF16), values, preferred_element_type=F32)

    def finish(first, count, parity):
        for b in range(count):
            found = sums[parity, b * 256 : b * 256 + 256, :]
            averaged = found[:, 0:128] / found[:, 128:256]
            differ = averaged[0:128] - lam * averaged[128:256]
            normed = differ * lax.rsqrt(jnp.mean(differ * differ, axis=-1, keepdims=True) + epsilon)
            ob[first + b] = (normed * att_gain).astype(BF16)

    def deliver(first, count):
        for i in (first + b for b in range(count)):
            @pl.when(jnp.logical_not(att_self(i)))
            def _():
                att_out(i).start()

            @pl.when(att_self(i))
            def _():
                join[:, join_cols] = ob[i]

    def attention_pairs(pairs):
        before = None
        for n, m in enumerate(pairs):
            attention(2 * m, 2, m, 256, n % 2)
            if before is not None:
                finish(2 * before, 2, (n + 1) % 2)
                deliver(2 * before, 2)
            before = m
        finish(2 * before, 2, (len(pairs) + 1) % 2)
        deliver(2 * before, 2)

    attention(10 + side, 1, 5, 128, 0)
    finish(10 + side, 1, 0)
    deliver(10 + side, 1)

    arrival(rs.at[pl.ds(0, 15)], st_r)

    block_decay = jnp.exp(-decay * 256.0)
    carry = jnp.zeros((32, 128), F32)
    for i in range(16):
        ps[i] = carry.astype(BF16)
        if i < 15:
            carry = carry * block_decay + rs[i].astype(F32)

    @pl.loop(0, 16)
    def _(i):
        @pl.when(i != s)
        def _():
            pt_copy(i).start()

    sin[srow, :] = ps[s]

    @pl.when(side == 0)
    def _():
        attention_pairs(range(5))

    @pl.when(side == 1)
    def _():
        attention_pairs((6, 7))

    arrival(sin.at[pl.ds(0, 480), :], pt_r)

    ret_head = 8 + 4 * t + f
    ret_cols = pl.ds(pl.multiple_of(ret_head * 128, 128), 128)
    query_decay = jnp.exp(-decay * (place_rows + 1.0))
    ret_gain = rows[2:3, :]

    def ret_out(q, c):
        return remote(
            rb.at[q, pl.ds(c * 128, 128), :], join.at[:, ret_cols], jr_s, jr_r, (z, x, q, c)
        )

    def ret_self(q, c):
        return (q == f) & (t == c)

    @pl.loop(0, 4)
    def _(q):
        state = sin[pl.ds(pl.multiple_of(q * 128, 128), 128), :]
        u = uu[q] + jnp.dot(qkv[q, 3], state, preferred_element_type=F32) * query_decay
        normed = u * lax.rsqrt(jnp.mean(u * u, axis=-1, keepdims=True) + epsilon)
        rb[q] = (normed * ret_gain).astype(BF16)
        for c in range(2):
            @pl.when(jnp.logical_not(ret_self(q, c)))
            def _():
                ret_out(q, c).start()

            @pl.when(ret_self(q, c))
            def _():
                join[:, ret_cols] = rb[q, c * 128 : (c + 1) * 128, :]

    gl_copy.wait_send()
    ss_copy.wait_send()
    arrival(stage, w1_s)
    arrival(ws.at[pl.ds(0, 3), pl.ds(0, 480), :], w_s)
    arrival(xs.at[pl.ds(0, 3), pl.ds(0, 2)], x_s)
    arrival(xs.at[pl.ds(0, 2)], p_s)
    arrival(rs.at[pl.ds(0, 15)], st_s)
    arrival(ps.at[pl.ds(0, 15)], pt_s)
    kept_kv = one_if((high == t) & ((side == 1) | (s <= 10)))
    counted(kk, a_s, 16 - 8 * late - kept_kv, 16, 15, 8, 7)
    counted(qb, q_s, 8 - one_if((high == t) & (side == late)), 8, 7)
    counted(kk, f_s, key_blocks, 11, 16)

    ow_copy.wait()
    for h in (0, 2, 4, 6):
        for k in (h, h + 1):
            @pl.when(jnp.logical_not((k % 4 == f) & (sequence == f) & (high == k // 4) & (side == late)))
            def _():
                arrival(ob.at[0], j_r.at[k])

        heads = slice(h * 128, h * 128 + 256)
        piece = jnp.dot(join[:, heads], ow[heads, :], preferred_element_type=F32)
        if h == 0:
            summed[...] = piece
        else:
            summed[...] += piece

    arrival(qb.at[pl.ds(0, 7)], jr_r)
    for n in range(4):
        span = slice(n * 512, n * 512 + 512)
        piece = jnp.dot(join[:, 1024:], ow[1024:, span], preferred_element_type=F32)
        rounded[:, span] = (summed[:, span] + piece).astype(BF16)
    out_copy = pltpu.make_async_copy(rounded, out_hbm, loc.at[11])
    out_copy.start()

    counted(ob, ja_s, queries - one_if((sequence == f) & (side == late)), 11, 10, 5, 4)
    arrival(qb.at[pl.ds(0, 7)], jr_s)
    out_copy.wait()


def body(
    tokens, norm_gain, query_weight, key_weight, value_weight, state_query, state_key, state_value,
    map_lambda, diff_gain, decay_rate, state_gain, out_weight,
):
    hbm = pl.BlockSpec(memory_space=pltpu.HBM)
    out = pl.pallas_call(
        kernel,
        out_shape=jax.ShapeDtypeStruct((128, FEATURES), BF16),
        in_specs=[hbm] * 13,
        out_specs=hbm,
        scratch_shapes=[
            pltpu.SMEM((4,), F32),
            pltpu.SMEM((4,), F32),
            pltpu.VMEM((256, 1024), BF16),
            pltpu.VMEM((1, 1024), F32),
            pltpu.VMEM((8, 128), F32),
            pltpu.VMEM((2, 256, 128), F32),
            pltpu.VMEM((2, 8, 128), F32),
            pltpu.VMEM((4, 4, 256, 512), BF16),
            pltpu.VMEM((4, 512, 768), BF16),
            pltpu.VMEM((3, 32, 768), BF16),
            pltpu.VMEM((4, 6, 256, 128), BF16),
            pltpu.VMEM((16, 256, 128), BF16),
            pltpu.VMEM((16, 256, 256), BF16),
            pltpu.VMEM((16, 128, 128), BF16),
            pltpu.VMEM((2, 512, 128), BF16),
            pltpu.VMEM((2, 512, 256), F32),
            pltpu.VMEM((16, 128, 128), BF16),
            pltpu.VMEM((128, FEATURES), BF16),
            pltpu.VMEM((FEATURES, FEATURES), BF16),
            pltpu.VMEM((128, FEATURES), F32),
            pltpu.VMEM((128, FEATURES), BF16),
            pltpu.VMEM((512, 128), BF16),
            pltpu.VMEM((16, 32, 128), BF16),
            pltpu.VMEM((16, 32, 128), BF16),
            pltpu.VMEM((512, 128), BF16),
            pltpu.VMEM((4, 256, 128), F32),
            pltpu.VMEM((4, 256, 128), BF16),
            DMA((12,)), DMA((23,)), DMA((2,)), DMA((2, 2)), DMA((2,)), DMA((2, 4, 2)),
            DMA((2, 2)), DMA((2,)), DMA((16,)), DMA((8,)),
        ],
        compiler_params=pltpu.CompilerParams(
            collective_id=0, has_side_effects=True, vmem_limit_bytes=48 * 1024 * 1024
        ),
        cost_estimate=pl.CostEstimate(flops=40_000_000_000, bytes_accessed=8_000_000, transcendentals=8_000_000),
        name="layer",
    )(
        *(
            pltpu.with_memory_space_constraint(a, pltpu.HBM)
            for a in (
                tokens, norm_gain, diff_gain, state_gain, map_lambda, decay_rate,
                query_weight, key_weight, value_weight, state_query, state_key, state_value, out_weight,
            )
        )
    )
    return out[None]


def solution(mesh):
    torus = Mesh(
        mesh.devices.reshape(4, 4, mesh.shape["fs"], mesh.shape["tp"]), ("sp_0", "sp_1", "fs", "tp")
    )
    return jax.shard_map(
        body,
        mesh=torus,
        in_specs=(
            P("fs", SP, "tp"), P(), P("fs", "tp"), P("fs", "tp"), P("fs", "tp"), P("fs", "tp"), P("fs", "tp"),
            P("fs", "tp"), P("tp"), P("tp"), P("tp"), P("tp"), P(),
        ),
        out_specs=P("fs", SP_TP, None),
        check_vma=False,
    )
```

```python
import jax
import jax.numpy as jnp
from jax import lax
from jax.experimental import pallas as pl
from jax.experimental.pallas import tpu as pltpu
from jax.sharding import Mesh
from jax.sharding import PartitionSpec as P

BF16 = jnp.bfloat16
F32 = jnp.float32
MESH = pl.DeviceIdType.MESH
SP = ("sp_0", "sp_1")
SP_TP = ("sp_0", "sp_1", "tp")
FEATURES = 2048
epsilon = 1e-05
branch_scale = 0.8
masked_score = -1e30

DMA = pltpu.SemaphoreType.DMA


def nt_dot(a, b):
    return lax.dot_general(a, b, (((1,), (1,)), ((), ())), preferred_element_type=F32)


def tn_dot(a, b):
    return lax.dot_general(a, b, (((0,), (0,)), ((), ())), preferred_element_type=F32)


def remote(src, dst, send, recv, device):
    return pltpu.make_async_remote_copy(
        src_ref=src, dst_ref=dst, send_sem=send, recv_sem=recv, device_id=device, device_id_type=MESH
    )


def arrival(ref, sem):
    pltpu.make_async_copy(ref, ref, sem).wait()


def kernel(
    tok_hbm, norm_gain, diff_gain, state_gain, lambda_hbm, decay_hbm, wq, wk, wv, sq, sk, sv, ow_hbm, out_hbm,
    map_lambda, decay_rate, tok, gain, rows, ss, gl, xs, ws, stage, qkv, kk, vv, qb, qs, sums, ob, join, ow, summed, rounded, stat, rs, ps, sin, uu, rb,
    loc, once, w1_r, s1_r, s1f_r, s2_r, x_r, xf_r, kv_r, j_r,
):
    (
        ss_s, ss_r, gl_s, gl_r, w1_s, w_s, x_s, p_s, a_s, q_s, f_s, st_s, pt_s, ja_s, jr_s,
        q_r, f_r, st_r, pt_r, jr_r, s2f_r, p_r, p2_r,
    ) = (once.at[i] for i in range(23))
    z, x, f, t = (lax.axis_index(a) for a in ("sp_0", "sp_1", "fs", "tp"))
    s = z * 4 + x
    partner = (z, x, f, 1 - t)
    up, down = lax.rem(f + 1, 4), lax.rem(f + 3, 4)
    side = lax.rem(z, 2)
    high = x // 2

    barrier = pltpu.get_barrier_semaphore()
    peers = [partner]
    for k in (1, 3):
        peers += [(z, lax.rem(x + k, 4), f, t), (lax.rem(z + k, 4), x, f, t)]
    for k in (1, 2, 3):
        peers.append((z, x, lax.rem(f + k, 4), t))
    for peer in peers:
        pl.semaphore_signal(barrier, inc=1, device_id=peer, device_id_type=MESH)

    tok_copy = pltpu.make_async_copy(tok_hbm.at[0], tok, loc.at[0])
    tok_copy.start()
    cols = pl.ds(pl.multiple_of(f * 128, 128), 128)
    small = [
        pltpu.make_async_copy(norm_gain.at[pl.ds(pl.multiple_of(t * 1024, 1024), 1024)], gain.at[0], loc.at[3]),
        pltpu.make_async_copy(diff_gain.at[cols], rows.at[0], loc.at[4]),
        pltpu.make_async_copy(state_gain.at[cols], rows.at[2], loc.at[5]),
        pltpu.make_async_copy(lambda_hbm, map_lambda, loc.at[6]),
        pltpu.make_async_copy(decay_hbm, decay_rate, loc.at[7]),
    ]
    for c in small:
        c.start()
    groups = tuple(enumerate(((wq, wk, wv), (sq, sk, sv))))
    srow = pl.ds(pl.multiple_of(s * 32, 32), 32)
    for g, group in groups:
        for k in range(1, 4):
            theirs = pl.ds(pl.multiple_of(lax.rem(f + k, 4) * 128, 128), 128)
            for i, source in enumerate(group):
                pltpu.make_async_copy(
                    source.at[srow, theirs], stage.at[k - 1, :, pl.ds((3 * g + i) * 128, 128)], loc.at[8 + g]
                ).start()
    for g, group in groups:
        for i, source in enumerate(group):
            pltpu.make_async_copy(
                source.at[:, cols], ws.at[0, :, pl.ds((3 * g + i) * 128, 128)], loc.at[1 + g]
            ).start()

    ow_copy = pltpu.make_async_copy(ow_hbm, ow, loc.at[10])
    ow_copy.start()

    tok_copy.wait()

    @pl.loop(0, 8)
    def _(b):
        block = pl.ds(pl.multiple_of(b * 32, 32), 32)
        v = tok[block, :].astype(F32)
        v = v * v
        total = v[:, 0:128]
        for k in range(1, 8):
            total = total + v[:, k * 128 : (k + 1) * 128]
        ss[0, block, :] = total

    for c in small:
        c.wait()
    rows[1] = jnp.full((128,), map_lambda[f], F32)

    pl.semaphore_wait(barrier, len(peers))

    ss_copy = remote(ss.at[0], ss.at[1], ss_s, ss_r, partner)
    ss_copy.start()

    for g in range(2):
        part = pl.ds(g * 384, 384)
        arrival(stage.at[:, :, part], loc.at[8 + g])
        for k in range(1, 4):
            c = remote(
                stage.at[k - 1, :, part], ws.at[4 - k, srow, part], w1_s, w1_r.at[g],
                (z, x, lax.rem(f + k, 4), t),
            )
            c.start()

    gl_copy = remote(rows, gl.at[t], gl_s, gl_r, partner)
    gl_copy.start()
    gl[t] = rows[...]

    ss_copy.wait_recv()

    @pl.loop(0, 8)
    def _(b):
        block = pl.ds(pl.multiple_of(b * 32, 32), 32)
        total = jnp.sum(ss[0, block, :] + ss[1, block, :], axis=-1, keepdims=True)
        r = lax.rsqrt(total * (1.0 / FEATURES) + epsilon)
        v = tok[block, :].astype(F32) * r * gain[...]
        v = v.astype(BF16)
        xs[f, 2 * t, block, :] = v[:, 0:512]
        xs[f, 2 * t + 1, block, :] = v[:, 512:1024]


    def xref(e, half):
        return xs.at[lax.rem(f + e, 4), pl.ds(2 * t, 2), pl.ds(half * 128, 128), :]

    def xsend(e, half, target, recv):
        remote(xref(e, half), xref(e, half), x_s, recv, (z, x, target, t)).start()

    def xpair(e, half):
        remote(xref(e, half), xref(e, half), p_s, p2_r if e == 2 else p_r, partner).start()

    xsend(0, 0, up, x_r.at[0, 0])
    xsend(0, 1, down, x_r.at[1, 1])
    xsend(0, 1, up, x_r.at[0, 1])
    xsend(0, 0, down, x_r.at[1, 0])
    xpair(0, 0)
    xpair(0, 1)

    vv[:, :, 128:256] = jnp.ones((16, 256, 128), BF16)

    @pl.when(side == 0)
    def _():
        kk[11] = jnp.zeros((256, 128), BF16)
        vv[11, :, 0:128] = jnp.zeros((256, 128), BF16)

    def place(g, c1, c2):
        return (c2, c1) if g == 0 else (c1, c2)

    def coords(g):
        return (x, z) if g == 0 else (z, x)

    def share(g, e1, e2, half=None):
        c1, c2 = coords(g)
        pz, px = place(g, lax.rem(c1 + e1, 4), lax.rem(c2 + e2, 4))
        start = (pz * 4 + px) * 32
        if half is None:
            return ws.at[pl.ds(1, 3), pl.ds(pl.multiple_of(start, 32), 32), pl.ds(g * 384, 384)]
        return ws.at[pl.ds(1, 3), pl.ds(pl.multiple_of(start + half * 16, 16), 16), pl.ds(g * 384, 384)]

    def wsend(g, ref, d1, d2, recv):
        c1, c2 = coords(g)
        pz, px = place(g, lax.rem(c1 + d1, 4), lax.rem(c2 + d2, 4))
        remote(ref, ref, w_s, recv, (pz, px, f, t)).start()

    step = (1, 3)
    origin = (3, 1)

    def second(g, j):
        for d in range(2):
            wsend(g, share(g, j, 0), 0, step[d], s2_r.at[g, j, d])

    def second_forward(g, j):
        for d in range(2):
            arrival(share(g, j, origin[d]), s2_r.at[g, j, d])
            wsend(g, share(g, j, origin[d], d), 0, step[d], s2f_r)

    for g in range(2):
        arrival(share(g, 0, 0), w1_r.at[g])
        for d in range(2):
            wsend(g, share(g, 0, 0), step[d], 0, s1_r.at[g, d])
        second(g, 0)
    for g in range(2):
        for d in range(2):
            arrival(share(g, origin[d], 0), s1_r.at[g, d])
            wsend(g, share(g, origin[d], 0, d), step[d], 0, s1f_r.at[g])
            second(g, origin[d])
    for g in range(2):
        second_forward(g, 0)

    arrival(xref(3, 0), x_r.at[0, 0])
    xsend(3, 0, up, xf_r.at[0])
    xpair(3, 0)
    arrival(xref(1, 1), x_r.at[1, 1])
    xsend(1, 1, down, xf_r.at[1])
    xpair(1, 1)

    for g in range(2):
        arrival(share(g, 2, 0), s1f_r.at[g])
        second(g, 2)
    for j in (3, 1):
        for g in range(2):
            second_forward(g, j)
    for g in range(2):
        second_forward(g, 2)
    arrival(xref(3, 1), x_r.at[0, 1])
    xpair(3, 1)
    arrival(xref(1, 0), x_r.at[1, 0])
    xpair(1, 0)
    arrival(ws.at[0, pl.ds(0, 384), :], s2f_r)
    for g in range(2):
        arrival(ws.at[0, :, pl.ds(g * 384, 384)], loc.at[1 + g])

    arrival(xs.at[pl.ds(0, 3), pl.ds(0, 2)], p_r)

    late = jnp.where(s >= 11, 1, 0)

    def column(q, h):
        return 2 * t + lax.rem(h + q, 2)

    def owner(q, h, c):
        return (lax.rem(q + column(q, h), 4), column(q, h), f, c)

    def att_copies(q):
        my_sequence = q == lax.rem(z + 4 - x, 4)
        found = []
        for h in (1, 0):
            u = column(q, h)
            for c in range(2):
                target = kk.at[s] if c == 0 else vv.at[s, :, pl.ds(0, 128)]
                copy = remote(qkv.at[q, 1 + c], target, a_s, kv_r.at[s], owner(q, h, c))
                elsewhere = jnp.logical_not(my_sequence & (x == u) & (t == c))
                found.append((copy, elsewhere if h == 1 else elsewhere & (s <= 10), h))
        u = column(q, late)
        for c in range(2):
            copy = remote(
                qkv.at[q, 0, pl.ds(c * 128, 128), :], qb.at[s], q_s, q_r, owner(q, late, c)
            )
            found.append((copy, jnp.logical_not(my_sequence & (x == u) & (t == c)), 2))
        return found

    decay = jnp.full((1, 128), decay_rate[f], F32)
    place_rows = lax.broadcasted_iota(jnp.int32, (256, 128), 0).astype(F32)
    key_decay = jnp.exp(-decay * (255.0 - place_rows))

    def project(q, group):
        features = jnp.concatenate([xs[q, lax.rem(f + d, 4)] for d in range(4)], axis=1)
        weights = ws[:, :, group * 384 : group * 384 + 384].reshape(FEATURES, 384)
        total = jnp.dot(features, weights, preferred_element_type=F32).astype(BF16)
        for i in range(3):
            qkv[q, 3 * group + i] = total[:, i * 128 : (i + 1) * 128]

    turn = lax.rem(z + x, 3)

    @pl.loop(0, 4)
    def _(k):
        near = lax.rem(k + turn, 3)
        e = (near + near // 2) * (1 - k // 3) + 2 * (k // 3)
        q = lax.rem(f + e, 4)

        @pl.when(k == 3)
        def _():
            for half in range(2):
                arrival(xref(2, half), xf_r.at[half])
                xpair(2, half)
            arrival(xs.at[0, pl.ds(0, 2)], p2_r)

        project(q, 0)
        for copy, condition, kind in att_copies(q):
            @pl.when(condition)
            def _():
                copy.start()

        kept = (q == lax.rem(z + 4 - x, 4)) & (high == t)

        @pl.when(kept & ((side == 1) | (s <= 10)))
        def _():
            @pl.when(t == 0)
            def _():
                kk[s] = qkv[q, 1]

            @pl.when(t == 1)
            def _():
                vv[s, :, 0:128] = qkv[q, 2]

        @pl.when(kept & (side == late))
        def _():
            qb[s] = qkv[q, 0, pl.ds(pl.multiple_of(t * 128, 128), 128), :]

    @pl.loop(0, 4)
    def _(q):
        project(q, 1)
        decayed = (qkv[q, 4].astype(F32) * key_decay).astype(BF16)
        stat[pl.ds(pl.multiple_of(q * 128, 128), 128), :] = tn_dot(decayed, qkv[q, 5]).astype(BF16)

    def st_copy(i):
        return remote(
            stat.at[pl.ds(pl.multiple_of(i * 32, 32), 32), :], rs.at[s], st_s, st_r,
            (i // 4, lax.rem(i, 4), f, t),
        )

    def pt_copy(i):
        return remote(
            ps.at[i], sin.at[pl.ds(pl.multiple_of(s * 32, 32), 32), :], pt_s, pt_r,
            (i // 4, lax.rem(i, 4), f, t),
        )

    @pl.loop(0, 16)
    def _(i):
        @pl.when(i != s)
        def _():
            st_copy(i).start()

    rs[s] = stat[srow, :]

    decay_square = jnp.broadcast_to(decay[:, 0:1], (256, 256))
    apart = (
        lax.broadcasted_iota(jnp.int32, (256, 256), 0) - lax.broadcasted_iota(jnp.int32, (256, 256), 1)
    ).astype(F32)
    within = jnp.where(apart >= 0, jnp.exp(-decay_square * jnp.maximum(apart, 0.0)), 0.0)

    @pl.loop(0, 4)
    def _(q):
        scores = nt_dot(qkv[q, 3], qkv[q, 4]) * within
        uu[q] = jnp.dot(scores.astype(BF16), qkv[q, 5], preferred_element_type=F32)

    sequence = lax.rem(z + 4 - x, 4)
    head = 4 * high + f
    key_blocks = 11 + 5 * side
    first_block = 11 * side
    kv_buffers = (lambda i: kk.at[i], lambda i: vv.at[i, :, pl.ds(0, 128)])

    def forward_copy(c, i):
        return remote(kv_buffers[c](i), kv_buffers[c](i), f_s, f_r, partner)

    for c in range(2):
        @pl.when(t == c)
        def _():
            @pl.loop(0, key_blocks)
            def _(i):
                @pl.when(jnp.logical_not((i == s) & (high == t)))
                def _():
                    arrival(kv_buffers[c](i), kv_r.at[i])
                forward_copy(c, i).start()

    arrival(gl.at[1 - t], gl_r)

    def one_if(condition):
        return jnp.where(condition, 1, 0)

    def counted(ref, sem, n, *values):
        for k in values:
            @pl.when(n == k)
            def _():
                arrival(ref.at[pl.ds(0, k)], sem)

    queries = 11 - 6 * side
    counted(qb, q_r, queries - one_if((high == t) & (side == late)), 11, 10, 5, 4)
    counted(kk, f_r, key_blocks, 11, 16)

    lam = gl[high, pl.ds(1, 1), :]
    att_gain = gl[high, pl.ds(0, 1), :] * branch_scale
    lane = lax.broadcasted_iota(jnp.int32, (128, 128), 1)
    join_cols = pl.ds(pl.multiple_of(head * 128, 128), 128)

    def att_out(i):
        return remote(
            ob.at[i], join.at[:, join_cols], ja_s, j_r.at[head], (i // 4, lax.rem(i, 4), sequence, t)
        )

    def att_self(i):
        return (i == s) & (sequence == f)

    def attention(first, count, m, height, parity):
        for b in range(count):
            query = qb[first + b].astype(F32) * 0.125
            qs[parity, b * 256 : b * 256 + 128] = jnp.where(lane < 64, query, 0.0).astype(BF16)
            qs[parity, b * 256 + 128 : b * 256 + 256] = jnp.where(lane >= 64, query, 0.0).astype(BF16)
        keys = kk[0 : 2 * m + 2].reshape(512 * m + 512, 128)
        values = vv[0 : 2 * m + 2].reshape(512 * m + 512, 256)
        for b in range(256 * count // height):
            span = slice(b * height, b * height + height)
            scores = nt_dot(qs[parity, span], keys)
            row = lax.broadcasted_iota(jnp.int32, (height, 512), 0) + b * height
            row = lax.rem(row, 128) + 256 * (row // 256) + (128 * t + 256 * (first - 2 * m))
            column = lax.broadcasted_iota(jnp.int32, (height, 512), 1)
            last = jnp.where(column <= row, scores[:, 512 * m :], masked_score)
            scores = jnp.concatenate([scores[:, : 512 * m], last], axis=1) if m else last
            weights = jnp.exp(scores - jnp.max(scores, axis=-1, keepdims=True))
            sums[parity, span] = jnp.dot(weights.astype(BF16), values, preferred_element_type=F32)

    def finish(first, count, parity):
        for b in range(count):
            found = sums[parity, b * 256 : b * 256 + 256, :]
            averaged = found[:, 0:128] / found[:, 128:256]
            differ = averaged[0:128] - lam * averaged[128:256]
            normed = differ * lax.rsqrt(jnp.mean(differ * differ, axis=-1, keepdims=True) + epsilon)
            ob[first + b] = (normed * att_gain).astype(BF16)

    def deliver(first, count):
        for i in (first + b for b in range(count)):
            @pl.when(jnp.logical_not(att_self(i)))
            def _():
                att_out(i).start()

            @pl.when(att_self(i))
            def _():
                join[:, join_cols] = ob[i]

    def attention_pairs(pairs):
        before = None
        for n, m in enumerate(pairs):
            attention(2 * m, 2, m, 256, n % 2)
            if before is not None:
                finish(2 * before, 2, (n + 1) % 2)
                deliver(2 * before, 2)
            before = m
        finish(2 * before, 2, (len(pairs) + 1) % 2)
        deliver(2 * before, 2)

    attention(10 + side, 1, 5, 128, 0)
    finish(10 + side, 1, 0)
    deliver(10 + side, 1)

    arrival(rs.at[pl.ds(0, 15)], st_r)

    block_decay = jnp.exp(-decay * 256.0)
    carry = jnp.zeros((32, 128), F32)
    for i in range(16):
        ps[i] = carry.astype(BF16)
        if i < 15:
            carry = carry * block_decay + rs[i].astype(F32)

    @pl.loop(0, 16)
    def _(i):
        @pl.when(i != s)
        def _():
            pt_copy(i).start()

    sin[srow, :] = ps[s]

    @pl.when(side == 0)
    def _():
        attention_pairs(range(5))

    @pl.when(side == 1)
    def _():
        attention_pairs((6, 7))

    arrival(sin.at[pl.ds(0, 480), :], pt_r)

    ret_head = 8 + 4 * t + f
    ret_cols = pl.ds(pl.multiple_of(ret_head * 128, 128), 128)
    query_decay = jnp.exp(-decay * (place_rows + 1.0))
    ret_gain = rows[2:3, :]

    def ret_out(q, c):
        return remote(
            rb.at[q, pl.ds(c * 128, 128), :], join.at[:, ret_cols], jr_s, jr_r, (z, x, q, c)
        )

    def ret_self(q, c):
        return (q == f) & (t == c)

    @pl.loop(0, 4)
    def _(q):
        state = sin[pl.ds(pl.multiple_of(q * 128, 128), 128), :]
        u = uu[q] + jnp.dot(qkv[q, 3], state, preferred_element_type=F32) * query_decay
        normed = u * lax.rsqrt(jnp.mean(u * u, axis=-1, keepdims=True) + epsilon)
        rb[q] = (normed * ret_gain).astype(BF16)
        for c in range(2):
            @pl.when(jnp.logical_not(ret_self(q, c)))
            def _():
                ret_out(q, c).start()

            @pl.when(ret_self(q, c))
            def _():
                join[:, ret_cols] = rb[q, c * 128 : (c + 1) * 128, :]

    gl_copy.wait_send()
    ss_copy.wait_send()
    arrival(stage, w1_s)
    arrival(ws.at[pl.ds(0, 3), pl.ds(0, 480), :], w_s)
    arrival(xs.at[pl.ds(0, 3), pl.ds(0, 2)], x_s)
    arrival(xs.at[pl.ds(0, 2)], p_s)
    arrival(rs.at[pl.ds(0, 15)], st_s)
    arrival(ps.at[pl.ds(0, 15)], pt_s)
    kept_kv = one_if((high == t) & ((side == 1) | (s <= 10)))
    counted(kk, a_s, 16 - 8 * late - kept_kv, 16, 15, 8, 7)
    counted(qb, q_s, 8 - one_if((high == t) & (side == late)), 8, 7)
    counted(kk, f_s, key_blocks, 11, 16)

    ow_copy.wait()
    for h in (0, 2, 4, 6):
        for k in (h, h + 1):
            @pl.when(jnp.logical_not((k % 4 == f) & (sequence == f) & (high == k // 4) & (side == late)))
            def _():
                arrival(ob.at[0], j_r.at[k])

        heads = slice(h * 128, h * 128 + 256)
        piece = jnp.dot(join[:, heads], ow[heads, :], preferred_element_type=F32)
        if h == 0:
            summed[...] = piece
        else:
            summed[...] += piece

    arrival(qb.at[pl.ds(0, 7)], jr_r)
    for n in range(4):
        span = slice(n * 512, n * 512 + 512)
        piece = jnp.dot(join[:, 1024:], ow[1024:, span], preferred_element_type=F32)
        rounded[:, span] = (summed[:, span] + piece).astype(BF16)
    out_copy = pltpu.make_async_copy(rounded, out_hbm, loc.at[11])
    out_copy.start()

    counted(ob, ja_s, queries - one_if((sequence == f) & (side == late)), 11, 10, 5, 4)
    arrival(qb.at[pl.ds(0, 7)], jr_s)
    out_copy.wait()


def body(
    tokens, norm_gain, query_weight, key_weight, value_weight, state_query, state_key, state_value,
    map_lambda, diff_gain, decay_rate, state_gain, out_weight,
):
    hbm = pl.BlockSpec(memory_space=pltpu.HBM)
    out = pl.pallas_call(
        kernel,
        out_shape=jax.ShapeDtypeStruct((128, FEATURES), BF16),
        in_specs=[hbm] * 13,
        out_specs=hbm,
        scratch_shapes=[
            pltpu.SMEM((4,), F32),
            pltpu.SMEM((4,), F32),
            pltpu.VMEM((256, 1024), BF16),
            pltpu.VMEM((1, 1024), F32),
            pltpu.VMEM((8, 128), F32),
            pltpu.VMEM((2, 256, 128), F32),
            pltpu.VMEM((2, 8, 128), F32),
            pltpu.VMEM((4, 4, 256, 512), BF16),
            pltpu.VMEM((4, 512, 768), BF16),
            pltpu.VMEM((3, 32, 768), BF16),
            pltpu.VMEM((4, 6, 256, 128), BF16),
            pltpu.VMEM((16, 256, 128), BF16),
            pltpu.VMEM((16, 256, 256), BF16),
            pltpu.VMEM((16, 128, 128), BF16),
            pltpu.VMEM((2, 512, 128), BF16),
            pltpu.VMEM((2, 512, 256), F32),
            pltpu.VMEM((16, 128, 128), BF16),
            pltpu.VMEM((128, FEATURES), BF16),
            pltpu.VMEM((FEATURES, FEATURES), BF16),
            pltpu.VMEM((128, FEATURES), F32),
            pltpu.VMEM((128, FEATURES), BF16),
            pltpu.VMEM((512, 128), BF16),
            pltpu.VMEM((16, 32, 128), BF16),
            pltpu.VMEM((16, 32, 128), BF16),
            pltpu.VMEM((512, 128), BF16),
            pltpu.VMEM((4, 256, 128), F32),
            pltpu.VMEM((4, 256, 128), BF16),
            DMA((12,)), DMA((23,)), DMA((2,)), DMA((2, 2)), DMA((2,)), DMA((2, 4, 2)),
            DMA((2, 2)), DMA((2,)), DMA((16,)), DMA((8,)),
        ],
        compiler_params=pltpu.CompilerParams(
            collective_id=0, has_side_effects=True, vmem_limit_bytes=48 * 1024 * 1024
        ),
        cost_estimate=pl.CostEstimate(flops=40_000_000_000, bytes_accessed=8_000_000, transcendentals=8_000_000),
        name="layer",
    )(
        *(
            pltpu.with_memory_space_constraint(a, pltpu.HBM)
            for a in (
                tokens, norm_gain, diff_gain, state_gain, map_lambda, decay_rate,
                query_weight, key_weight, value_weight, state_query, state_key, state_value, out_weight,
            )
        )
    )
    return out[None]


def solution(mesh):
    torus = Mesh(
        mesh.devices.reshape(4, 4, mesh.shape["fs"], mesh.shape["tp"]), ("sp_0", "sp_1", "fs", "tp")
    )
    return jax.shard_map(
        body,
        mesh=torus,
        in_specs=(
            P("fs", SP, "tp"), P(), P("fs", "tp"), P("fs", "tp"), P("fs", "tp"), P("fs", "tp"), P("fs", "tp"),
            P("fs", "tp"), P("tp"), P("tp"), P("tp"), P("tp"), P(),
        ),
        out_specs=P("fs", SP_TP, None),
        check_vma=False,
    )
```

```python
import jax
import jax.numpy as jnp
from jax import lax
from jax.experimental import pallas as pl
from jax.experimental.pallas import tpu as pltpu
from jax.sharding import Mesh
from jax.sharding import PartitionSpec as P

BF16 = jnp.bfloat16
F32 = jnp.float32
MESH = pl.DeviceIdType.MESH
SP = ("sp_0", "sp_1")
SP_TP = ("sp_0", "sp_1", "tp")
FEATURES = 2048
epsilon = 1e-05
branch_scale = 0.8
masked_score = -1e30

DMA = pltpu.SemaphoreType.DMA


def nt_dot(a, b):
    return lax.dot_general(a, b, (((1,), (1,)), ((), ())), preferred_element_type=F32)


def tn_dot(a, b):
    return lax.dot_general(a, b, (((0,), (0,)), ((), ())), preferred_element_type=F32)


def remote(src, dst, send, recv, device):
    return pltpu.make_async_remote_copy(
        src_ref=src, dst_ref=dst, send_sem=send, recv_sem=recv, device_id=device, device_id_type=MESH
    )


def arrival(ref, sem):
    pltpu.make_async_copy(ref, ref, sem).wait()


def kernel(
    tok_hbm, norm_gain, diff_gain, state_gain, lambda_hbm, decay_hbm, wq, wk, wv, sq, sk, sv, ow_hbm, out_hbm,
    map_lambda, decay_rate, tok, gain, rows, ss, gl, xs, ws, stage, qkv, kk, vv, qb, qs, sums, ob, join, ow, summed, rounded, stat, rs, ps, sin, uu, rb,
    loc, once, w1_r, s1_r, s1f_r, s2_r, x_r, xf_r, kv_r, j_r,
):
    (
        ss_s, ss_r, gl_s, gl_r, w1_s, w_s, x_s, p_s, a_s, q_s, f_s, st_s, pt_s, ja_s, jr_s,
        q_r, f_r, st_r, pt_r, jr_r, s2f_r, p_r, p2_r,
    ) = (once.at[i] for i in range(23))
    z, x, f, t = (lax.axis_index(a) for a in ("sp_0", "sp_1", "fs", "tp"))
    s = z * 4 + x
    partner = (z, x, f, 1 - t)
    up, down = lax.rem(f + 1, 4), lax.rem(f + 3, 4)
    side = lax.rem(z, 2)
    high = x // 2

    barrier = pltpu.get_barrier_semaphore()
    peers = [partner]
    for k in (1, 3):
        peers += [(z, lax.rem(x + k, 4), f, t), (lax.rem(z + k, 4), x, f, t)]
    for k in (1, 2, 3):
        peers.append((z, x, lax.rem(f + k, 4), t))
    for peer in peers:
        pl.semaphore_signal(barrier, inc=1, device_id=peer, device_id_type=MESH)

    tok_copy = pltpu.make_async_copy(tok_hbm.at[0], tok, loc.at[0])
    tok_copy.start()
    cols = pl.ds(pl.multiple_of(f * 128, 128), 128)
    small = [
        pltpu.make_async_copy(norm_gain.at[pl.ds(pl.multiple_of(t * 1024, 1024), 1024)], gain.at[0], loc.at[3]),
        pltpu.make_async_copy(diff_gain.at[cols], rows.at[0], loc.at[4]),
        pltpu.make_async_copy(state_gain.at[cols], rows.at[2], loc.at[5]),
        pltpu.make_async_copy(lambda_hbm, map_lambda, loc.at[6]),
        pltpu.make_async_copy(decay_hbm, decay_rate, loc.at[7]),
    ]
    for c in small:
        c.start()
    groups = tuple(enumerate(((wq, wk, wv), (sq, sk, sv))))
    srow = pl.ds(pl.multiple_of(s * 32, 32), 32)
    for g, group in groups:
        for k in range(1, 4):
            theirs = pl.ds(pl.multiple_of(lax.rem(f + k, 4) * 128, 128), 128)
            for i, source in enumerate(group):
                pltpu.make_async_copy(
                    source.at[srow, theirs], stage.at[k - 1, :, pl.ds((3 * g + i) * 128, 128)], loc.at[8 + g]
                ).start()
    for g, group in groups:
        for i, source in enumerate(group):
            pltpu.make_async_copy(
                source.at[:, cols], ws.at[0, :, pl.ds((3 * g + i) * 128, 128)], loc.at[1 + g]
            ).start()

    ow_copy = pltpu.make_async_copy(ow_hbm, ow, loc.at[10])
    ow_copy.start()

    tok_copy.wait()

    @pl.loop(0, 8)
    def _(b):
        block = pl.ds(pl.multiple_of(b * 32, 32), 32)
        v = tok[block, :].astype(F32)
        v = v * v
        total = v[:, 0:128]
        for k in range(1, 8):
            total = total + v[:, k * 128 : (k + 1) * 128]
        ss[0, block, :] = total

    for c in small:
        c.wait()
    rows[1] = jnp.full((128,), map_lambda[f], F32)

    pl.semaphore_wait(barrier, len(peers))

    ss_copy = remote(ss.at[0], ss.at[1], ss_s, ss_r, partner)
    ss_copy.start()

    for g in range(2):
        part = pl.ds(g * 384, 384)
        arrival(stage.at[:, :, part], loc.at[8 + g])
        for k in range(1, 4):
            c = remote(
                stage.at[k - 1, :, part], ws.at[4 - k, srow, part], w1_s, w1_r.at[g],
                (z, x, lax.rem(f + k, 4), t),
            )
            c.start()

    gl_copy = remote(rows, gl.at[t], gl_s, gl_r, partner)
    gl_copy.start()
    gl[t] = rows[...]

    ss_copy.wait_recv()

    @pl.loop(0, 8)
    def _(b):
        block = pl.ds(pl.multiple_of(b * 32, 32), 32)
        total = jnp.sum(ss[0, block, :] + ss[1, block, :], axis=-1, keepdims=True)
        r = lax.rsqrt(total * (1.0 / FEATURES) + epsilon)
        v = tok[block, :].astype(F32) * r * gain[...]
        v = v.astype(BF16)
        xs[f, 2 * t, block, :] = v[:, 0:512]
        xs[f, 2 * t + 1, block, :] = v[:, 512:1024]


    def xref(e, half):
        return xs.at[lax.rem(f + e, 4), pl.ds(2 * t, 2), pl.ds(half * 128, 128), :]

    def xsend(e, half, target, recv):
        remote(xref(e, half), xref(e, half), x_s, recv, (z, x, target, t)).start()

    def xpair(e, half):
        remote(xref(e, half), xref(e, half), p_s, p2_r if e == 2 else p_r, partner).start()

    xsend(0, 0, up, x_r.at[0, 0])
    xsend(0, 1, down, x_r.at[1, 1])
    xsend(0, 1, up, x_r.at[0, 1])
    xsend(0, 0, down, x_r.at[1, 0])
    xpair(0, 0)
    xpair(0, 1)

    vv[:, :, 128:256] = jnp.ones((16, 256, 128), BF16)

    @pl.when(side == 0)
    def _():
        kk[11] = jnp.zeros((256, 128), BF16)
        vv[11, :, 0:128] = jnp.zeros((256, 128), BF16)

    def place(g, c1, c2):
        return (c2, c1) if g == 0 else (c1, c2)

    def coords(g):
        return (x, z) if g == 0 else (z, x)

    def share(g, e1, e2, half=None):
        c1, c2 = coords(g)
        pz, px = place(g, lax.rem(c1 + e1, 4), lax.rem(c2 + e2, 4))
        start = (pz * 4 + px) * 32
        if half is None:
            return ws.at[pl.ds(1, 3), pl.ds(pl.multiple_of(start, 32), 32), pl.ds(g * 384, 384)]
        return ws.at[pl.ds(1, 3), pl.ds(pl.multiple_of(start + half * 16, 16), 16), pl.ds(g * 384, 384)]

    def wsend(g, ref, d1, d2, recv):
        c1, c2 = coords(g)
        pz, px = place(g, lax.rem(c1 + d1, 4), lax.rem(c2 + d2, 4))
        remote(ref, ref, w_s, recv, (pz, px, f, t)).start()

    step = (1, 3)
    origin = (3, 1)

    def second(g, j):
        for d in range(2):
            wsend(g, share(g, j, 0), 0, step[d], s2_r.at[g, j, d])

    def second_forward(g, j):
        for d in range(2):
            arrival(share(g, j, origin[d]), s2_r.at[g, j, d])
            wsend(g, share(g, j, origin[d], d), 0, step[d], s2f_r)

    for g in range(2):
        arrival(share(g, 0, 0), w1_r.at[g])
        for d in range(2):
            wsend(g, share(g, 0, 0), step[d], 0, s1_r.at[g, d])
        second(g, 0)
    for g in range(2):
        for d in range(2):
            arrival(share(g, origin[d], 0), s1_r.at[g, d])
            wsend(g, share(g, origin[d], 0, d), step[d], 0, s1f_r.at[g])
            second(g, origin[d])
    for g in range(2):
        second_forward(g, 0)

    arrival(xref(3, 0), x_r.at[0, 0])
    xsend(3, 0, up, xf_r.at[0])
    xpair(3, 0)
    arrival(xref(1, 1), x_r.at[1, 1])
    xsend(1, 1, down, xf_r.at[1])
    xpair(1, 1)

    for g in range(2):
        arrival(share(g, 2, 0), s1f_r.at[g])
        second(g, 2)
    for j in (3, 1):
        for g in range(2):
            second_forward(g, j)
    for g in range(2):
        second_forward(g, 2)
    arrival(xref(3, 1), x_r.at[0, 1])
    xpair(3, 1)
    arrival(xref(1, 0), x_r.at[1, 0])
    xpair(1, 0)
    arrival(ws.at[0, pl.ds(0, 384), :], s2f_r)
    for g in range(2):
        arrival(ws.at[0, :, pl.ds(g * 384, 384)], loc.at[1 + g])

    arrival(xs.at[pl.ds(0, 3), pl.ds(0, 2)], p_r)

    late = jnp.where(s >= 11, 1, 0)

    def column(q, h):
        return 2 * t + lax.rem(h + q, 2)

    def owner(q, h, c):
        return (lax.rem(q + column(q, h), 4), column(q, h), f, c)

    def att_copies(q):
        my_sequence = q == lax.rem(z + 4 - x, 4)
        found = []
        for h in (1, 0):
            u = column(q, h)
            for c in range(2):
                target = kk.at[s] if c == 0 else vv.at[s, :, pl.ds(0, 128)]
                copy = remote(qkv.at[q, 1 + c], target, a_s, kv_r.at[s], owner(q, h, c))
                elsewhere = jnp.logical_not(my_sequence & (x == u) & (t == c))
                found.append((copy, elsewhere if h == 1 else elsewhere & (s <= 10), h))
        u = column(q, late)
        for c in range(2):
            copy = remote(
                qkv.at[q, 0, pl.ds(c * 128, 128), :], qb.at[s], q_s, q_r, owner(q, late, c)
            )
            found.append((copy, jnp.logical_not(my_sequence & (x == u) & (t == c)), 2))
        return found

    decay = jnp.full((1, 128), decay_rate[f], F32)
    place_rows = lax.broadcasted_iota(jnp.int32, (256, 128), 0).astype(F32)
    key_decay = jnp.exp(-decay * (255.0 - place_rows))

    def project(q, group):
        features = jnp.concatenate([xs[q, lax.rem(f + d, 4)] for d in range(4)], axis=1)
        weights = ws[:, :, group * 384 : group * 384 + 384].reshape(FEATURES, 384)
        total = jnp.dot(features, weights, preferred_element_type=F32).astype(BF16)
        for i in range(3):
            qkv[q, 3 * group + i] = total[:, i * 128 : (i + 1) * 128]

    turn = lax.rem(z + 2 * x, 3)

    @pl.loop(0, 4)
    def _(k):
        near = lax.rem(k + turn, 3)
        e = (near + near // 2) * (1 - k // 3) + 2 * (k // 3)
        q = lax.rem(f + e, 4)

        @pl.when(k == 3)
        def _():
            for half in range(2):
                arrival(xref(2, half), xf_r.at[half])
                xpair(2, half)
            arrival(xs.at[0, pl.ds(0, 2)], p2_r)

        project(q, 0)
        for copy, condition, kind in att_copies(q):
            @pl.when(condition)
            def _():
                copy.start()

        kept = (q == lax.rem(z + 4 - x, 4)) & (high == t)

        @pl.when(kept & ((side == 1) | (s <= 10)))
        def _():
            @pl.when(t == 0)
            def _():
                kk[s] = qkv[q, 1]

            @pl.when(t == 1)
            def _():
                vv[s, :, 0:128] = qkv[q, 2]

        @pl.when(kept & (side == late))
        def _():
            qb[s] = qkv[q, 0, pl.ds(pl.multiple_of(t * 128, 128), 128), :]

    @pl.loop(0, 4)
    def _(q):
        project(q, 1)
        decayed = (qkv[q, 4].astype(F32) * key_decay).astype(BF16)
        stat[pl.ds(pl.multiple_of(q * 128, 128), 128), :] = tn_dot(decayed, qkv[q, 5]).astype(BF16)

    def st_copy(i):
        return remote(
            stat.at[pl.ds(pl.multiple_of(i * 32, 32), 32), :], rs.at[s], st_s, st_r,
            (i // 4, lax.rem(i, 4), f, t),
        )

    def pt_copy(i):
        return remote(
            ps.at[i], sin.at[pl.ds(pl.multiple_of(s * 32, 32), 32), :], pt_s, pt_r,
            (i // 4, lax.rem(i, 4), f, t),
        )

    @pl.loop(0, 16)
    def _(i):
        @pl.when(i != s)
        def _():
            st_copy(i).start()

    rs[s] = stat[srow, :]

    decay_square = jnp.broadcast_to(decay[:, 0:1], (256, 256))
    apart = (
        lax.broadcasted_iota(jnp.int32, (256, 256), 0) - lax.broadcasted_iota(jnp.int32, (256, 256), 1)
    ).astype(F32)
    within = jnp.where(apart >= 0, jnp.exp(-decay_square * jnp.maximum(apart, 0.0)), 0.0)

    @pl.loop(0, 4)
    def _(q):
        scores = nt_dot(qkv[q, 3], qkv[q, 4]) * within
        uu[q] = jnp.dot(scores.astype(BF16), qkv[q, 5], preferred_element_type=F32)

    sequence = lax.rem(z + 4 - x, 4)
    head = 4 * high + f
    key_blocks = 11 + 5 * side
    first_block = 11 * side
    kv_buffers = (lambda i: kk.at[i], lambda i: vv.at[i, :, pl.ds(0, 128)])

    def forward_copy(c, i):
        return remote(kv_buffers[c](i), kv_buffers[c](i), f_s, f_r, partner)

    for c in range(2):
        @pl.when(t == c)
        def _():
            @pl.loop(0, key_blocks)
            def _(i):
                @pl.when(jnp.logical_not((i == s) & (high == t)))
                def _():
                    arrival(kv_buffers[c](i), kv_r.at[i])
                forward_copy(c, i).start()

    arrival(gl.at[1 - t], gl_r)

    def one_if(condition):
        return jnp.where(condition, 1, 0)

    def counted(ref, sem, n, *values):
        for k in values:
            @pl.when(n == k)
            def _():
                arrival(ref.at[pl.ds(0, k)], sem)

    queries = 11 - 6 * side
    counted(qb, q_r, queries - one_if((high == t) & (side == late)), 11, 10, 5, 4)
    counted(kk, f_r, key_blocks, 11, 16)

    lam = gl[high, pl.ds(1, 1), :]
    att_gain = gl[high, pl.ds(0, 1), :] * branch_scale
    lane = lax.broadcasted_iota(jnp.int32, (128, 128), 1)
    join_cols = pl.ds(pl.multiple_of(head * 128, 128), 128)

    def att_out(i):
        return remote(
            ob.at[i], join.at[:, join_cols], ja_s, j_r.at[head], (i // 4, lax.rem(i, 4), sequence, t)
        )

    def att_self(i):
        return (i == s) & (sequence == f)

    def attention(first, count, m, height, parity):
        for b in range(count):
            query = qb[first + b].astype(F32) * 0.125
            qs[parity, b * 256 : b * 256 + 128] = jnp.where(lane < 64, query, 0.0).astype(BF16)
            qs[parity, b * 256 + 128 : b * 256 + 256] = jnp.where(lane >= 64, query, 0.0).astype(BF16)
        keys = kk[0 : 2 * m + 2].reshape(512 * m + 512, 128)
        values = vv[0 : 2 * m + 2].reshape(512 * m + 512, 256)
        for b in range(256 * count // height):
            span = slice(b * height, b * height + height)
            scores = nt_dot(qs[parity, span], keys)
            row = lax.broadcasted_iota(jnp.int32, (height, 512), 0) + b * height
            row = lax.rem(row, 128) + 256 * (row // 256) + (128 * t + 256 * (first - 2 * m))
            column = lax.broadcasted_iota(jnp.int32, (height, 512), 1)
            last = jnp.where(column <= row, scores[:, 512 * m :], masked_score)
            scores = jnp.concatenate([scores[:, : 512 * m], last], axis=1) if m else last
            weights = jnp.exp(scores - jnp.max(scores, axis=-1, keepdims=True))
            sums[parity, span] = jnp.dot(weights.astype(BF16), values, preferred_element_type=F32)

    def finish(first, count, parity):
        for b in range(count):
            found = sums[parity, b * 256 : b * 256 + 256, :]
            averaged = found[:, 0:128] / found[:, 128:256]
            differ = averaged[0:128] - lam * averaged[128:256]
            normed = differ * lax.rsqrt(jnp.mean(differ * differ, axis=-1, keepdims=True) + epsilon)
            ob[first + b] = (normed * att_gain).astype(BF16)

    def deliver(first, count):
        for i in (first + b for b in range(count)):
            @pl.when(jnp.logical_not(att_self(i)))
            def _():
                att_out(i).start()

            @pl.when(att_self(i))
            def _():
                join[:, join_cols] = ob[i]

    def attention_pairs(pairs):
        before = None
        for n, m in enumerate(pairs):
            attention(2 * m, 2, m, 256, n % 2)
            if before is not None:
                finish(2 * before, 2, (n + 1) % 2)
                deliver(2 * before, 2)
            before = m
        finish(2 * before, 2, (len(pairs) + 1) % 2)
        deliver(2 * before, 2)

    attention(10 + side, 1, 5, 128, 0)
    finish(10 + side, 1, 0)
    deliver(10 + side, 1)

    arrival(rs.at[pl.ds(0, 15)], st_r)

    block_decay = jnp.exp(-decay * 256.0)
    carry = jnp.zeros((32, 128), F32)
    for i in range(16):
        ps[i] = carry.astype(BF16)
        if i < 15:
            carry = carry * block_decay + rs[i].astype(F32)

    @pl.loop(0, 16)
    def _(i):
        @pl.when(i != s)
        def _():
            pt_copy(i).start()

    sin[srow, :] = ps[s]

    @pl.when(side == 0)
    def _():
        attention_pairs(range(5))

    @pl.when(side == 1)
    def _():
        attention_pairs((6, 7))

    arrival(sin.at[pl.ds(0, 480), :], pt_r)

    ret_head = 8 + 4 * t + f
    ret_cols = pl.ds(pl.multiple_of(ret_head * 128, 128), 128)
    query_decay = jnp.exp(-decay * (place_rows + 1.0))
    ret_gain = rows[2:3, :]

    def ret_out(q, c):
        return remote(
            rb.at[q, pl.ds(c * 128, 128), :], join.at[:, ret_cols], jr_s, jr_r, (z, x, q, c)
        )

    def ret_self(q, c):
        return (q == f) & (t == c)

    @pl.loop(0, 4)
    def _(q):
        state = sin[pl.ds(pl.multiple_of(q * 128, 128), 128), :]
        u = uu[q] + jnp.dot(qkv[q, 3], state, preferred_element_type=F32) * query_decay
        normed = u * lax.rsqrt(jnp.mean(u * u, axis=-1, keepdims=True) + epsilon)
        rb[q] = (normed * ret_gain).astype(BF16)
        for c in range(2):
            @pl.when(jnp.logical_not(ret_self(q, c)))
            def _():
                ret_out(q, c).start()

            @pl.when(ret_self(q, c))
            def _():
                join[:, ret_cols] = rb[q, c * 128 : (c + 1) * 128, :]

    gl_copy.wait_send()
    ss_copy.wait_send()
    arrival(stage, w1_s)
    arrival(ws.at[pl.ds(0, 3), pl.ds(0, 480), :], w_s)
    arrival(xs.at[pl.ds(0, 3), pl.ds(0, 2)], x_s)
    arrival(xs.at[pl.ds(0, 2)], p_s)
    arrival(rs.at[pl.ds(0, 15)], st_s)
    arrival(ps.at[pl.ds(0, 15)], pt_s)
    kept_kv = one_if((high == t) & ((side == 1) | (s <= 10)))
    counted(kk, a_s, 16 - 8 * late - kept_kv, 16, 15, 8, 7)
    counted(qb, q_s, 8 - one_if((high == t) & (side == late)), 8, 7)
    counted(kk, f_s, key_blocks, 11, 16)

    ow_copy.wait()
    for h in (0, 2, 4, 6):
        for k in (h, h + 1):
            @pl.when(jnp.logical_not((k % 4 == f) & (sequence == f) & (high == k // 4) & (side == late)))
            def _():
                arrival(ob.at[0], j_r.at[k])

        heads = slice(h * 128, h * 128 + 256)
        piece = jnp.dot(join[:, heads], ow[heads, :], preferred_element_type=F32)
        if h == 0:
            summed[...] = piece
        else:
            summed[...] += piece

    arrival(qb.at[pl.ds(0, 7)], jr_r)
    for n in range(4):
        span = slice(n * 512, n * 512 + 512)
        piece = jnp.dot(join[:, 1024:], ow[1024:, span], preferred_element_type=F32)
        rounded[:, span] = (summed[:, span] + piece).astype(BF16)
    out_copy = pltpu.make_async_copy(rounded, out_hbm, loc.at[11])
    out_copy.start()

    counted(ob, ja_s, queries - one_if((sequence == f) & (side == late)), 11, 10, 5, 4)
    arrival(qb.at[pl.ds(0, 7)], jr_s)
    out_copy.wait()


def body(
    tokens, norm_gain, query_weight, key_weight, value_weight, state_query, state_key, state_value,
    map_lambda, diff_gain, decay_rate, state_gain, out_weight,
):
    hbm = pl.BlockSpec(memory_space=pltpu.HBM)
    out = pl.pallas_call(
        kernel,
        out_shape=jax.ShapeDtypeStruct((128, FEATURES), BF16),
        in_specs=[hbm] * 13,
        out_specs=hbm,
        scratch_shapes=[
            pltpu.SMEM((4,), F32),
            pltpu.SMEM((4,), F32),
            pltpu.VMEM((256, 1024), BF16),
            pltpu.VMEM((1, 1024), F32),
            pltpu.VMEM((8, 128), F32),
            pltpu.VMEM((2, 256, 128), F32),
            pltpu.VMEM((2, 8, 128), F32),
            pltpu.VMEM((4, 4, 256, 512), BF16),
            pltpu.VMEM((4, 512, 768), BF16),
            pltpu.VMEM((3, 32, 768), BF16),
            pltpu.VMEM((4, 6, 256, 128), BF16),
            pltpu.VMEM((16, 256, 128), BF16),
            pltpu.VMEM((16, 256, 256), BF16),
            pltpu.VMEM((16, 128, 128), BF16),
            pltpu.VMEM((2, 512, 128), BF16),
            pltpu.VMEM((2, 512, 256), F32),
            pltpu.VMEM((16, 128, 128), BF16),
            pltpu.VMEM((128, FEATURES), BF16),
            pltpu.VMEM((FEATURES, FEATURES), BF16),
            pltpu.VMEM((128, FEATURES), F32),
            pltpu.VMEM((128, FEATURES), BF16),
            pltpu.VMEM((512, 128), BF16),
            pltpu.VMEM((16, 32, 128), BF16),
            pltpu.VMEM((16, 32, 128), BF16),
            pltpu.VMEM((512, 128), BF16),
            pltpu.VMEM((4, 256, 128), F32),
            pltpu.VMEM((4, 256, 128), BF16),
            DMA((12,)), DMA((23,)), DMA((2,)), DMA((2, 2)), DMA((2,)), DMA((2, 4, 2)),
            DMA((2, 2)), DMA((2,)), DMA((16,)), DMA((8,)),
        ],
        compiler_params=pltpu.CompilerParams(
            collective_id=0, has_side_effects=True, vmem_limit_bytes=48 * 1024 * 1024
        ),
        cost_estimate=pl.CostEstimate(flops=40_000_000_000, bytes_accessed=8_000_000, transcendentals=8_000_000),
        name="layer",
    )(
        *(
            pltpu.with_memory_space_constraint(a, pltpu.HBM)
            for a in (
                tokens, norm_gain, diff_gain, state_gain, map_lambda, decay_rate,
                query_weight, key_weight, value_weight, state_query, state_key, state_value, out_weight,
            )
        )
    )
    return out[None]


def solution(mesh):
    torus = Mesh(
        mesh.devices.reshape(4, 4, mesh.shape["fs"], mesh.shape["tp"]), ("sp_0", "sp_1", "fs", "tp")
    )
    return jax.shard_map(
        body,
        mesh=torus,
        in_specs=(
            P("fs", SP, "tp"), P(), P("fs", "tp"), P("fs", "tp"), P("fs", "tp"), P("fs", "tp"), P("fs", "tp"),
            P("fs", "tp"), P("tp"), P("tp"), P("tp"), P("tp"), P(),
        ),
        out_specs=P("fs", SP_TP, None),
        check_vma=False,
    )
```

```python
import jax
import jax.numpy as jnp
from jax import lax
from jax.experimental import pallas as pl
from jax.experimental.pallas import tpu as pltpu
from jax.sharding import Mesh
from jax.sharding import PartitionSpec as P

BF16 = jnp.bfloat16
F32 = jnp.float32
MESH = pl.DeviceIdType.MESH
SP = ("sp_0", "sp_1")
SP_TP = ("sp_0", "sp_1", "tp")
FEATURES = 2048
epsilon = 1e-05
branch_scale = 0.8
masked_score = -1e30

DMA = pltpu.SemaphoreType.DMA


def nt_dot(a, b):
    return lax.dot_general(a, b, (((1,), (1,)), ((), ())), preferred_element_type=F32)


def tn_dot(a, b):
    return lax.dot_general(a, b, (((0,), (0,)), ((), ())), preferred_element_type=F32)


def remote(src, dst, send, recv, device):
    return pltpu.make_async_remote_copy(
        src_ref=src, dst_ref=dst, send_sem=send, recv_sem=recv, device_id=device, device_id_type=MESH
    )


def arrival(ref, sem):
    pltpu.make_async_copy(ref, ref, sem).wait()


def kernel(
    tok_hbm, norm_gain, diff_gain, state_gain, lambda_hbm, decay_hbm, wq, wk, wv, sq, sk, sv, ow_hbm, out,
    map_lambda, decay_rate, tok, gain, rows, ss, gl, xs, ws, stage, qkv, kk, vv, qb, qs, sums, ob, join, ow, summed, stat, rs, ps, sin, uu, rb,
    loc, once, w1_r, s1_r, s1f_r, s2_r, x_r, xf_r, kv_r, j_r,
):
    (
        ss_s, ss_r, gl_s, gl_r, w1_s, w_s, x_s, p_s, a_s, q_s, f_s, st_s, pt_s, ja_s, jr_s,
        q_r, f_r, st_r, pt_r, jr_r, s2f_r, p_r, p2_r,
    ) = (once.at[i] for i in range(23))
    z, x, f, t = (lax.axis_index(a) for a in ("sp_0", "sp_1", "fs", "tp"))
    s = z * 4 + x
    partner = (z, x, f, 1 - t)
    up, down = lax.rem(f + 1, 4), lax.rem(f + 3, 4)
    side = lax.rem(z, 2)
    high = x // 2

    barrier = pltpu.get_barrier_semaphore()
    peers = [partner]
    for k in (1, 3):
        peers += [(z, lax.rem(x + k, 4), f, t), (lax.rem(z + k, 4), x, f, t)]
    for k in (1, 2, 3):
        peers.append((z, x, lax.rem(f + k, 4), t))
    for peer in peers:
        pl.semaphore_signal(barrier, inc=1, device_id=peer, device_id_type=MESH)

    tok_copy = pltpu.make_async_copy(tok_hbm.at[0], tok, loc.at[0])
    tok_copy.start()
    cols = pl.ds(pl.multiple_of(f * 128, 128), 128)
    small = [
        pltpu.make_async_copy(norm_gain.at[pl.ds(pl.multiple_of(t * 1024, 1024), 1024)], gain.at[0], loc.at[3]),
        pltpu.make_async_copy(diff_gain.at[cols], rows.at[0], loc.at[4]),
        pltpu.make_async_copy(state_gain.at[cols], rows.at[2], loc.at[5]),
        pltpu.make_async_copy(lambda_hbm, map_lambda, loc.at[6]),
        pltpu.make_async_copy(decay_hbm, decay_rate, loc.at[7]),
    ]
    for c in small:
        c.start()
    groups = tuple(enumerate(((wq, wk, wv), (sq, sk, sv))))
    srow = pl.ds(pl.multiple_of(s * 32, 32), 32)
    for g, group in groups:
        for k in range(1, 4):
            theirs = pl.ds(pl.multiple_of(lax.rem(f + k, 4) * 128, 128), 128)
            for i, source in enumerate(group):
                pltpu.make_async_copy(
                    source.at[srow, theirs], stage.at[k - 1, :, pl.ds((3 * g + i) * 128, 128)], loc.at[8 + g]
                ).start()
    for g, group in groups:
        for i, source in enumerate(group):
            pltpu.make_async_copy(
                source.at[:, cols], ws.at[0, :, pl.ds((3 * g + i) * 128, 128)], loc.at[1 + g]
            ).start()

    ow_copy = pltpu.make_async_copy(ow_hbm, ow, loc.at[10])
    ow_copy.start()

    tok_copy.wait()

    @pl.loop(0, 8)
    def _(b):
        block = pl.ds(pl.multiple_of(b * 32, 32), 32)
        v = tok[block, :].astype(F32)
        v = v * v
        total = v[:, 0:128]
        for k in range(1, 8):
            total = total + v[:, k * 128 : (k + 1) * 128]
        ss[0, block, :] = total

    for c in small:
        c.wait()
    rows[1] = jnp.full((128,), map_lambda[f], F32)

    pl.semaphore_wait(barrier, len(peers))

    ss_copy = remote(ss.at[0], ss.at[1], ss_s, ss_r, partner)
    ss_copy.start()

    for g in range(2):
        part = pl.ds(g * 384, 384)
        arrival(stage.at[:, :, part], loc.at[8 + g])
        for k in range(1, 4):
            c = remote(
                stage.at[k - 1, :, part], ws.at[4 - k, srow, part], w1_s, w1_r.at[g],
                (z, x, lax.rem(f + k, 4), t),
            )
            c.start()

    gl_copy = remote(rows, gl.at[t], gl_s, gl_r, partner)
    gl_copy.start()
    gl[t] = rows[...]

    ss_copy.wait_recv()

    @pl.loop(0, 8)
    def _(b):
        block = pl.ds(pl.multiple_of(b * 32, 32), 32)
        total = jnp.sum(ss[0, block, :] + ss[1, block, :], axis=-1, keepdims=True)
        r = lax.rsqrt(total * (1.0 / FEATURES) + epsilon)
        v = tok[block, :].astype(F32) * r * gain[...]
        v = v.astype(BF16)
        xs[f, 2 * t, block, :] = v[:, 0:512]
        xs[f, 2 * t + 1, block, :] = v[:, 512:1024]


    def xref(e, half):
        return xs.at[lax.rem(f + e, 4), pl.ds(2 * t, 2), pl.ds(half * 128, 128), :]

    def xsend(e, half, target, recv):
        remote(xref(e, half), xref(e, half), x_s, recv, (z, x, target, t)).start()

    def xpair(e, half):
        remote(xref(e, half), xref(e, half), p_s, p2_r if e == 2 else p_r, partner).start()

    xsend(0, 0, up, x_r.at[0, 0])
    xsend(0, 1, down, x_r.at[1, 1])
    xsend(0, 1, up, x_r.at[0, 1])
    xsend(0, 0, down, x_r.at[1, 0])
    xpair(0, 0)
    xpair(0, 1)

    vv[:, :, 128:256] = jnp.ones((16, 256, 128), BF16)

    @pl.when(side == 0)
    def _():
        kk[11] = jnp.zeros((256, 128), BF16)
        vv[11, :, 0:128] = jnp.zeros((256, 128), BF16)

    def place(g, c1, c2):
        return (c2, c1) if g == 0 else (c1, c2)

    def coords(g):
        return (x, z) if g == 0 else (z, x)

    def share(g, e1, e2, half=None):
        c1, c2 = coords(g)
        pz, px = place(g, lax.rem(c1 + e1, 4), lax.rem(c2 + e2, 4))
        start = (pz * 4 + px) * 32
        if half is None:
            return ws.at[pl.ds(1, 3), pl.ds(pl.multiple_of(start, 32), 32), pl.ds(g * 384, 384)]
        return ws.at[pl.ds(1, 3), pl.ds(pl.multiple_of(start + half * 16, 16), 16), pl.ds(g * 384, 384)]

    def wsend(g, ref, d1, d2, recv):
        c1, c2 = coords(g)
        pz, px = place(g, lax.rem(c1 + d1, 4), lax.rem(c2 + d2, 4))
        remote(ref, ref, w_s, recv, (pz, px, f, t)).start()

    step = (1, 3)
    origin = (3, 1)

    def second(g, j):
        for d in range(2):
            wsend(g, share(g, j, 0), 0, step[d], s2_r.at[g, j, d])

    def second_forward(g, j):
        for d in range(2):
            arrival(share(g, j, origin[d]), s2_r.at[g, j, d])
            wsend(g, share(g, j, origin[d], d), 0, step[d], s2f_r)

    for g in range(2):
        arrival(share(g, 0, 0), w1_r.at[g])
        for d in range(2):
            wsend(g, share(g, 0, 0), step[d], 0, s1_r.at[g, d])
        second(g, 0)
    for g in range(2):
        for d in range(2):
            arrival(share(g, origin[d], 0), s1_r.at[g, d])
            wsend(g, share(g, origin[d], 0, d), step[d], 0, s1f_r.at[g])
            second(g, origin[d])
    for g in range(2):
        second_forward(g, 0)

    arrival(xref(3, 0), x_r.at[0, 0])
    xsend(3, 0, up, xf_r.at[0])
    xpair(3, 0)
    arrival(xref(1, 1), x_r.at[1, 1])
    xsend(1, 1, down, xf_r.at[1])
    xpair(1, 1)

    for g in range(2):
        arrival(share(g, 2, 0), s1f_r.at[g])
        second(g, 2)
    for j in (3, 1):
        for g in range(2):
            second_forward(g, j)
    for g in range(2):
        second_forward(g, 2)
    arrival(xref(3, 1), x_r.at[0, 1])
    xpair(3, 1)
    arrival(xref(1, 0), x_r.at[1, 0])
    xpair(1, 0)
    arrival(ws.at[0, pl.ds(0, 384), :], s2f_r)
    for g in range(2):
        arrival(ws.at[0, :, pl.ds(g * 384, 384)], loc.at[1 + g])

    arrival(xs.at[pl.ds(0, 3), pl.ds(0, 2)], p_r)

    late = jnp.where(s >= 11, 1, 0)

    def column(q, h):
        return 2 * t + lax.rem(h + q, 2)

    def owner(q, h, c):
        return (lax.rem(q + column(q, h), 4), column(q, h), f, c)

    def att_copies(q):
        my_sequence = q == lax.rem(z + 4 - x, 4)
        found = []
        for h in (1, 0):
            u = column(q, h)
            for c in range(2):
                target = kk.at[s] if c == 0 else vv.at[s, :, pl.ds(0, 128)]
                copy = remote(qkv.at[q, 1 + c], target, a_s, kv_r.at[s], owner(q, h, c))
                elsewhere = jnp.logical_not(my_sequence & (x == u) & (t == c))
                found.append((copy, elsewhere if h == 1 else elsewhere & (s <= 10), h))
        u = column(q, late)
        for c in range(2):
            copy = remote(
                qkv.at[q, 0, pl.ds(c * 128, 128), :], qb.at[s], q_s, q_r, owner(q, late, c)
            )
            found.append((copy, jnp.logical_not(my_sequence & (x == u) & (t == c)), 2))
        return found

    decay = jnp.full((1, 128), decay_rate[f], F32)
    place_rows = lax.broadcasted_iota(jnp.int32, (256, 128), 0).astype(F32)
    key_decay = jnp.exp(-decay * (255.0 - place_rows))

    def project(q, group):
        features = jnp.concatenate([xs[q, lax.rem(f + d, 4)] for d in range(4)], axis=1)
        weights = ws[:, :, group * 384 : group * 384 + 384].reshape(FEATURES, 384)
        total = jnp.dot(features, weights, preferred_element_type=F32).astype(BF16)
        for i in range(3):
            qkv[q, 3 * group + i] = total[:, i * 128 : (i + 1) * 128]

    turn = lax.rem(z + 2 * x, 3)

    @pl.loop(0, 4)
    def _(k):
        near = lax.rem(k + turn, 3)
        e = (near + near // 2) * (1 - k // 3) + 2 * (k // 3)
        q = lax.rem(f + e, 4)

        @pl.when(k == 3)
        def _():
            for half in range(2):
                arrival(xref(2, half), xf_r.at[half])
                xpair(2, half)
            arrival(xs.at[0, pl.ds(0, 2)], p2_r)

        project(q, 0)
        for copy, condition, kind in att_copies(q):
            @pl.when(condition)
            def _():
                copy.start()

        kept = (q == lax.rem(z + 4 - x, 4)) & (high == t)

        @pl.when(kept & ((side == 1) | (s <= 10)))
        def _():
            @pl.when(t == 0)
            def _():
                kk[s] = qkv[q, 1]

            @pl.when(t == 1)
            def _():
                vv[s, :, 0:128] = qkv[q, 2]

        @pl.when(kept & (side == late))
        def _():
            qb[s] = qkv[q, 0, pl.ds(pl.multiple_of(t * 128, 128), 128), :]

    @pl.loop(0, 4)
    def _(q):
        project(q, 1)
        decayed = (qkv[q, 4].astype(F32) * key_decay).astype(BF16)
        stat[pl.ds(pl.multiple_of(q * 128, 128), 128), :] = tn_dot(decayed, qkv[q, 5]).astype(BF16)

    def st_copy(i):
        return remote(
            stat.at[pl.ds(pl.multiple_of(i * 32, 32), 32), :], rs.at[s], st_s, st_r,
            (i // 4, lax.rem(i, 4), f, t),
        )

    def pt_copy(i):
        return remote(
            ps.at[i], sin.at[pl.ds(pl.multiple_of(s * 32, 32), 32), :], pt_s, pt_r,
            (i // 4, lax.rem(i, 4), f, t),
        )

    @pl.loop(0, 16)
    def _(i):
        @pl.when(i != s)
        def _():
            st_copy(i).start()

    rs[s] = stat[srow, :]

    decay_square = jnp.broadcast_to(decay[:, 0:1], (256, 256))
    apart = (
        lax.broadcasted_iota(jnp.int32, (256, 256), 0) - lax.broadcasted_iota(jnp.int32, (256, 256), 1)
    ).astype(F32)
    within = jnp.where(apart >= 0, jnp.exp(-decay_square * jnp.maximum(apart, 0.0)), 0.0)

    @pl.loop(0, 4)
    def _(q):
        scores = nt_dot(qkv[q, 3], qkv[q, 4]) * within
        uu[q] = jnp.dot(scores.astype(BF16), qkv[q, 5], preferred_element_type=F32)

    sequence = lax.rem(z + 4 - x, 4)
    head = 4 * high + f
    key_blocks = 11 + 5 * side
    first_block = 11 * side
    kv_buffers = (lambda i: kk.at[i], lambda i: vv.at[i, :, pl.ds(0, 128)])

    def forward_copy(c, i):
        return remote(kv_buffers[c](i), kv_buffers[c](i), f_s, f_r, partner)

    for c in range(2):
        @pl.when(t == c)
        def _():
            @pl.loop(0, key_blocks)
            def _(i):
                @pl.when(jnp.logical_not((i == s) & (high == t)))
                def _():
                    arrival(kv_buffers[c](i), kv_r.at[i])
                forward_copy(c, i).start()

    arrival(gl.at[1 - t], gl_r)

    def one_if(condition):
        return jnp.where(condition, 1, 0)

    def counted(ref, sem, n, *values):
        for k in values:
            @pl.when(n == k)
            def _():
                arrival(ref.at[pl.ds(0, k)], sem)

    queries = 11 - 6 * side
    counted(qb, q_r, queries - one_if((high == t) & (side == late)), 11, 10, 5, 4)
    counted(kk, f_r, key_blocks, 11, 16)

    lam = gl[high, pl.ds(1, 1), :]
    att_gain = gl[high, pl.ds(0, 1), :] * branch_scale
    lane = lax.broadcasted_iota(jnp.int32, (128, 128), 1)
    join_cols = pl.ds(pl.multiple_of(head * 128, 128), 128)

    def att_out(i):
        return remote(
            ob.at[i], join.at[:, join_cols], ja_s, j_r.at[head], (i // 4, lax.rem(i, 4), sequence, t)
        )

    def att_self(i):
        return (i == s) & (sequence == f)

    def attention(first, count, m, height, parity):
        for b in range(count):
            query = qb[first + b].astype(F32) * 0.125
            qs[parity, b * 256 : b * 256 + 128] = jnp.where(lane < 64, query, 0.0).astype(BF16)
            qs[parity, b * 256 + 128 : b * 256 + 256] = jnp.where(lane >= 64, query, 0.0).astype(BF16)
        keys = kk[0 : 2 * m + 2].reshape(512 * m + 512, 128)
        values = vv[0 : 2 * m + 2].reshape(512 * m + 512, 256)
        for b in range(256 * count // height):
            span = slice(b * height, b * height + height)
            scores = nt_dot(qs[parity, span], keys)
            row = lax.broadcasted_iota(jnp.int32, (height, 512), 0) + b * height
            row = lax.rem(row, 128) + 256 * (row // 256) + (128 * t + 256 * (first - 2 * m))
            column = lax.broadcasted_iota(jnp.int32, (height, 512), 1)
            last = jnp.where(column <= row, scores[:, 512 * m :], masked_score)
            scores = jnp.concatenate([scores[:, : 512 * m], last], axis=1) if m else last
            weights = jnp.exp(scores - jnp.max(scores, axis=-1, keepdims=True))
            sums[parity, span] = jnp.dot(weights.astype(BF16), values, preferred_element_type=F32)

    def finish(first, count, parity):
        for b in range(count):
            found = sums[parity, b * 256 : b * 256 + 256, :]
            averaged = found[:, 0:128] / found[:, 128:256]
            differ = averaged[0:128] - lam * averaged[128:256]
            normed = differ * lax.rsqrt(jnp.mean(differ * differ, axis=-1, keepdims=True) + epsilon)
            ob[first + b] = (normed * att_gain).astype(BF16)

    def deliver(first, count):
        for i in (first + b for b in range(count)):
            @pl.when(jnp.logical_not(att_self(i)))
            def _():
                att_out(i).start()

            @pl.when(att_self(i))
            def _():
                join[:, join_cols] = ob[i]

    def attention_pairs(pairs):
        before = None
        for n, m in enumerate(pairs):
            attention(2 * m, 2, m, 256, n % 2)
            if before is not None:
                finish(2 * before, 2, (n + 1) % 2)
                deliver(2 * before, 2)
            before = m
        finish(2 * before, 2, (len(pairs) + 1) % 2)
        deliver(2 * before, 2)

    attention(10 + side, 1, 5, 128, 0)
    finish(10 + side, 1, 0)
    deliver(10 + side, 1)

    arrival(rs.at[pl.ds(0, 15)], st_r)

    block_decay = jnp.exp(-decay * 256.0)
    carry = jnp.zeros((32, 128), F32)
    for i in range(16):
        ps[i] = carry.astype(BF16)
        if i < 15:
            carry = carry * block_decay + rs[i].astype(F32)

    @pl.loop(0, 16)
    def _(i):
        @pl.when(i != s)
        def _():
            pt_copy(i).start()

    sin[srow, :] = ps[s]

    @pl.when(side == 0)
    def _():
        attention_pairs(range(5))

    @pl.when(side == 1)
    def _():
        attention_pairs((6, 7))

    arrival(sin.at[pl.ds(0, 480), :], pt_r)

    ret_head = 8 + 4 * t + f
    ret_cols = pl.ds(pl.multiple_of(ret_head * 128, 128), 128)
    query_decay = jnp.exp(-decay * (place_rows + 1.0))
    ret_gain = rows[2:3, :]

    def ret_out(q, c):
        return remote(
            rb.at[q, pl.ds(c * 128, 128), :], join.at[:, ret_cols], jr_s, jr_r, (z, x, q, c)
        )

    def ret_self(q, c):
        return (q == f) & (t == c)

    @pl.loop(0, 4)
    def _(q):
        state = sin[pl.ds(pl.multiple_of(q * 128, 128), 128), :]
        u = uu[q] + jnp.dot(qkv[q, 3], state, preferred_element_type=F32) * query_decay
        normed = u * lax.rsqrt(jnp.mean(u * u, axis=-1, keepdims=True) + epsilon)
        rb[q] = (normed * ret_gain).astype(BF16)
        for c in range(2):
            @pl.when(jnp.logical_not(ret_self(q, c)))
            def _():
                ret_out(q, c).start()

            @pl.when(ret_self(q, c))
            def _():
                join[:, ret_cols] = rb[q, c * 128 : (c + 1) * 128, :]

    gl_copy.wait_send()
    ss_copy.wait_send()
    arrival(stage, w1_s)
    arrival(ws.at[pl.ds(0, 3), pl.ds(0, 480), :], w_s)
    arrival(xs.at[pl.ds(0, 3), pl.ds(0, 2)], x_s)
    arrival(xs.at[pl.ds(0, 2)], p_s)
    arrival(rs.at[pl.ds(0, 15)], st_s)
    arrival(ps.at[pl.ds(0, 15)], pt_s)
    kept_kv = one_if((high == t) & ((side == 1) | (s <= 10)))
    counted(kk, a_s, 16 - 8 * late - kept_kv, 16, 15, 8, 7)
    counted(qb, q_s, 8 - one_if((high == t) & (side == late)), 8, 7)
    counted(kk, f_s, key_blocks, 11, 16)

    ow_copy.wait()
    for h in (0, 2, 4, 6):
        for k in (h, h + 1):
            @pl.when(jnp.logical_not((k % 4 == f) & (sequence == f) & (high == k // 4) & (side == late)))
            def _():
                arrival(ob.at[0], j_r.at[k])

        heads = slice(h * 128, h * 128 + 256)
        piece = jnp.dot(join[:, heads], ow[heads, :], preferred_element_type=F32)
        if h == 0:
            summed[...] = piece
        else:
            summed[...] += piece

    arrival(qb.at[pl.ds(0, 7)], jr_r)
    for n in range(4):
        span = slice(n * 512, n * 512 + 512)
        piece = jnp.dot(join[:, 1024:], ow[1024:, span], preferred_element_type=F32)
        out[:, span] = (summed[:, span] + piece).astype(BF16)
    counted(ob, ja_s, queries - one_if((sequence == f) & (side == late)), 11, 10, 5, 4)
    arrival(qb.at[pl.ds(0, 7)], jr_s)


def body(
    tokens, norm_gain, query_weight, key_weight, value_weight, state_query, state_key, state_value,
    map_lambda, diff_gain, decay_rate, state_gain, out_weight,
):
    hbm = pl.BlockSpec(memory_space=pltpu.HBM)
    out = pl.pallas_call(
        kernel,
        out_shape=jax.ShapeDtypeStruct((128, FEATURES), BF16),
        in_specs=[hbm] * 13,
        out_specs=pl.BlockSpec(memory_space=pltpu.VMEM),
        scratch_shapes=[
            pltpu.SMEM((4,), F32),
            pltpu.SMEM((4,), F32),
            pltpu.VMEM((256, 1024), BF16),
            pltpu.VMEM((1, 1024), F32),
            pltpu.VMEM((8, 128), F32),
            pltpu.VMEM((2, 256, 128), F32),
            pltpu.VMEM((2, 8, 128), F32),
            pltpu.VMEM((4, 4, 256, 512), BF16),
            pltpu.VMEM((4, 512, 768), BF16),
            pltpu.VMEM((3, 32, 768), BF16),
            pltpu.VMEM((4, 6, 256, 128), BF16),
            pltpu.VMEM((16, 256, 128), BF16),
            pltpu.VMEM((16, 256, 256), BF16),
            pltpu.VMEM((16, 128, 128), BF16),
            pltpu.VMEM((2, 512, 128), BF16),
            pltpu.VMEM((2, 512, 256), F32),
            pltpu.VMEM((16, 128, 128), BF16),
            pltpu.VMEM((128, FEATURES), BF16),
            pltpu.VMEM((FEATURES, FEATURES), BF16),
            pltpu.VMEM((128, FEATURES), F32),
            pltpu.VMEM((512, 128), BF16),
            pltpu.VMEM((16, 32, 128), BF16),
            pltpu.VMEM((16, 32, 128), BF16),
            pltpu.VMEM((512, 128), BF16),
            pltpu.VMEM((4, 256, 128), F32),
            pltpu.VMEM((4, 256, 128), BF16),
            DMA((11,)), DMA((23,)), DMA((2,)), DMA((2, 2)), DMA((2,)), DMA((2, 4, 2)),
            DMA((2, 2)), DMA((2,)), DMA((16,)), DMA((8,)),
        ],
        compiler_params=pltpu.CompilerParams(
            collective_id=0, has_side_effects=True, vmem_limit_bytes=48 * 1024 * 1024
        ),
        cost_estimate=pl.CostEstimate(flops=40_000_000_000, bytes_accessed=8_000_000, transcendentals=8_000_000),
        name="layer",
    )(
        *(
            pltpu.with_memory_space_constraint(a, pltpu.HBM)
            for a in (
                tokens, norm_gain, diff_gain, state_gain, map_lambda, decay_rate,
                query_weight, key_weight, value_weight, state_query, state_key, state_value, out_weight,
            )
        )
    )
    return out[None]


def solution(mesh):
    torus = Mesh(
        mesh.devices.reshape(4, 4, mesh.shape["fs"], mesh.shape["tp"]), ("sp_0", "sp_1", "fs", "tp")
    )
    return jax.shard_map(
        body,
        mesh=torus,
        in_specs=(
            P("fs", SP, "tp"), P(), P("fs", "tp"), P("fs", "tp"), P("fs", "tp"), P("fs", "tp"), P("fs", "tp"),
            P("fs", "tp"), P("tp"), P("tp"), P("tp"), P("tp"), P(),
        ),
        out_specs=P("fs", SP_TP, None),
        check_vma=False,
    )
```
